32 devices in a mesh: sp: 4 (over z), fs: 4 (over y, x), tp: 2 (over core).
Axes of the slice: x: 2, y: 2, z: 4, core: 2. Of those that a mesh axis runs over, the one named last changes fastest.
Arguments:
- tokens: bfloat16 [4, 512, 2048], P('fs', ('sp', 'tp')), may hold values from -6 to 6
- norm_gain: float32 [2048], replicated, may hold values from 0.1 to 1.9
- gla_query_weight: bfloat16 [2048, 512], P('sp', 'tp'), may hold values from -0.125 to 0.125
- gla_key_weight: bfloat16 [2048, 512], P('sp', 'tp'), may hold values from -0.125 to 0.125
- gla_value_weight: bfloat16 [2048, 1024], P('sp', 'tp'), may hold values from -0.125 to 0.125
- decay_down: bfloat16 [2048, 32], P('sp'), may hold values from -0.125 to 0.125
- decay_up: bfloat16 [32, 512], P(None, 'tp'), may hold values from -1 to 1
- decay_bias: float32 [512], P('tp'), may hold values from 0.5 to 12
- head_gain: float32 [128], replicated, may hold values from 0.1 to 1.9
- window_query_weight: bfloat16 [2048, 1024], P('sp', 'tp'), may hold values from -3 to 3
- window_key_weight: bfloat16 [2048, 256], P('sp', 'tp'), may hold values from -3 to 3
- window_value_weight: bfloat16 [2048, 256], P('sp', 'tp'), may hold values from -0.125 to 0.125
- sink_logit: float32 [16], P('tp'), may hold values from 3 to 7
- gla_output_weight: bfloat16 [1024, 2048], P('tp', 'sp'), may hold values from -0.125 to 0.125
- window_output_weight: bfloat16 [1024, 2048], P('tp', 'sp'), may hold values from -0.125 to 0.125
Outputs:
- mixed: bfloat16 [4, 512, 2048], P('fs', ('sp', 'tp'))
The draws below stay inside these ranges and needn't reach their ends.
All inputs are finite; a program needn't handle non-finite values.
Results may differ from the reference program's by a relative error of at most 0.013.
Values may be sent and summed in bfloat16 or wider, within the bound.
A program may use at most 64 MiB of HBM per device.

```python
import jax
import jax.numpy as jnp
from jax import lax

D = 2048
GLA_HEADS = 8
KEY_DIM = 64
VALUE_DIM = 128
RANK = 32
SWA_HEADS = 16
KV_HEADS = 4
HEAD_DIM = 64
WINDOW = 128
SPAN = 64
SEQS = 4
LEN = 512


def gain_values(key):
    normal_draw = jax.random.normal(jax.random.fold_in(key, 11), (D,), jnp.float32)
    return 1.0 + 0.18 * jnp.clip(normal_draw, -5.0, 5.0)


def drawn_weight(key, salt_value, columns):
    raw_draw = jax.random.normal(jax.random.fold_in(key, salt_value), (D, columns), jnp.float32)
    raw_draw = jnp.clip(raw_draw, -6.0, 6.0) / jnp.sqrt(float(D))
    return raw_draw


def draw_window_query_weight(key, part):
    return drawn_weight(key, 16, SWA_HEADS * HEAD_DIM).astype(jnp.bfloat16)


def draw_window_key_weight(key, part):
    return drawn_weight(key, 17, KV_HEADS * HEAD_DIM).astype(jnp.bfloat16)


def draw_norm_gain(key, part):
    return gain_values(key)


def draw_tokens(key, part):
    base_draw = jax.random.normal(jax.random.fold_in(key, 21), (SEQS, LEN, D), jnp.float32)
    base_draw = jnp.clip(base_draw, -6.0, 6.0)
    return base_draw.astype(jnp.bfloat16)


def block_scale(stream_key, extent, split, smallest, high):
    level = 1.0
    for dim, blocks in split:
        steps = jax.random.uniform(jax.random.fold_in(jax.random.fold_in(stream_key, 6), dim), (blocks,), jnp.float32, smallest / len(split), high / len(split))
        level = level * jnp.repeat(jnp.exp(steps), extent[dim] // blocks).reshape((-1,) + (1,) * (len(extent) - 1 - dim))
    return level


def gaussian(own_key, extent, deviation, limit, pieces=(), held_as=jnp.bfloat16):
    values = deviation * jax.random.normal(own_key, extent, jnp.float32)
    if pieces:
        values = values * block_scale(own_key, extent, pieces, -0.22, 0.18)
    return jnp.clip(values, -limit, limit).astype(held_as)


def setup_inputs(seed: int = 0) -> dict:
    streams_of = jax.random.split(jax.random.key(seed), 16)
    tokens = draw_tokens(jax.random.fold_in(streams_of[15], 71), 0)
    norm_gain = draw_norm_gain(jax.random.fold_in(streams_of[15], 71), 0)
    gla_query_weight = gaussian(streams_of[2], (D, GLA_HEADS * KEY_DIM), D ** -0.5, 0.125, ((0, 4), (1, 2)))
    gla_key_weight = gaussian(streams_of[3], (D, GLA_HEADS * KEY_DIM), D ** -0.5, 0.125, ((0, 4), (1, 2)))
    gla_value_weight = gaussian(streams_of[4], (D, GLA_HEADS * VALUE_DIM), D ** -0.5, 0.125, ((0, 4), (1, 2)))
    decay_down = gaussian(streams_of[5], (D, RANK), D ** -0.5, 0.125, ((0, 4),))
    decay_up = gaussian(streams_of[6], (RANK, GLA_HEADS * KEY_DIM), RANK ** -0.5, 1.0, ((1, 2),))
    decay_bias = jnp.clip(0.5 + 11.5 * jax.random.uniform(streams_of[7], (GLA_HEADS * KEY_DIM,), jnp.float32) ** block_scale(streams_of[7], (GLA_HEADS * KEY_DIM,), ((0, 2),), -0.2, 0.2), 0.5, 12.0)
    head_gain = jnp.clip(1.0 + 0.18 * jax.random.normal(streams_of[8], (VALUE_DIM,), jnp.float32), 0.1, 1.9)
    window_query_weight = draw_window_query_weight(jax.random.fold_in(streams_of[15], 71), 0)
    window_key_weight = draw_window_key_weight(jax.random.fold_in(streams_of[15], 71), 0)
    window_value_weight = gaussian(streams_of[11], (D, KV_HEADS * HEAD_DIM), D ** -0.5, 0.125, ((0, 4), (1, 2)))
    sink_logit = jnp.clip(3.0 + 4.0 * jax.random.uniform(streams_of[12], (SWA_HEADS,), jnp.float32) ** block_scale(streams_of[12], (SWA_HEADS,), ((0, 2),), -0.2, 0.2), 3.0, 7.0)
    gla_output_weight = gaussian(streams_of[13], (GLA_HEADS * VALUE_DIM, D), (GLA_HEADS * VALUE_DIM + SWA_HEADS * HEAD_DIM) ** -0.5, 0.125, ((0, 2), (1, 4)))
    window_output_weight = gaussian(streams_of[14], (SWA_HEADS * HEAD_DIM, D), (GLA_HEADS * VALUE_DIM + SWA_HEADS * HEAD_DIM) ** -0.5, 0.125, ((0, 2), (1, 4)))
    return {"tokens": tokens, "norm_gain": norm_gain, "gla_query_weight": gla_query_weight, "gla_key_weight": gla_key_weight, "gla_value_weight": gla_value_weight, "decay_down": decay_down, "decay_up": decay_up, "decay_bias": decay_bias, "head_gain": head_gain, "window_query_weight": window_query_weight, "window_key_weight": window_key_weight, "window_value_weight": window_value_weight, "sink_logit": sink_logit, "gla_output_weight": gla_output_weight, "window_output_weight": window_output_weight}


EPS = 1e-06
SOFTMAX_TEMPER = 16.0
HIGH = lax.Precision.HIGHEST

def rms_rows(values, gain):
    mean_square = lax.optimization_barrier(jnp.mean(values * values, axis=-1, keepdims=True))
    return values * lax.rsqrt(mean_square + EPS) * gain

def block_terms(query_rows, key_rows, value_rows, log_decay_rate, block_len):
    seq_len, head_count, key_width = query_rows.shape
    value_width = value_rows.shape[-1]
    block_count = seq_len // block_len
    q_scaled = query_rows.reshape(block_count, block_len, head_count, key_width) * key_width ** (-0.5)
    k_blocks = key_rows.reshape(block_count, block_len, head_count, key_width)
    v_blocks = value_rows.reshape(block_count, block_len, head_count, value_width)
    within = jnp.cumsum(log_decay_rate.reshape(block_count, block_len, head_count, key_width), axis=1)
    block_total = within[:, -1]
    q_dec = q_scaled * jnp.exp(within)
    k_dec = k_blocks * jnp.exp(-within)
    k_end = k_blocks * jnp.exp(block_total[:, None] - within)
    causal = jnp.tril(jnp.ones((block_len, block_len), dtype=bool))
    scores = jnp.einsum('nihd,njhd->nhij', q_dec, k_dec, precision=HIGH)
    scores = jnp.where(causal, scores, 0.0)
    local_out = jnp.einsum('nhij,njhe->nihe', scores, v_blocks, precision=HIGH)
    update = jnp.einsum('njhd,njhe->nhde', k_end, v_blocks, precision=HIGH)

    def advance(carried, inputs):
        update_in, decay_in = inputs
        return (decay_in[..., None] * carried + update_in, carried)
    start_state = jnp.zeros((head_count, key_width, value_width), jnp.float32)
    last_state, entering = lax.scan(advance, start_state, (update, jnp.exp(block_total)))
    return (q_dec, local_out, entering, last_state, block_total)

def window_band_mask(block_count, block_len, offset):
    query_pos = jnp.arange(block_len)[:, None] + block_len
    key_pos = jnp.arange(2 * block_len)[None, :]
    distance = query_pos - key_pos
    inside = (distance >= 0) & (distance < block_len)
    global_key = offset + jnp.arange(block_count)[:, None, None] * block_len - block_len + key_pos[None]
    return inside[None] & (global_key >= 0)

def window_attend(query_blocks, key_band, value_band, valid, sinks):
    scores = jnp.einsum('nqhgd,nkhd->nhgqk', query_blocks.astype(jnp.float32), key_band.astype(jnp.float32))
    scores = scores * HEAD_DIM ** (-0.5)
    scores = jnp.where(valid[:, None, None], scores, -1e+30)
    sink_term = sinks[None, :, :, None, None]
    top = jnp.maximum(lax.optimization_barrier(jnp.max(scores, axis=-1, keepdims=True)), sink_term)
    expo = jnp.exp(scores - top)
    denom = lax.optimization_barrier(jnp.sum(expo, axis=-1, keepdims=True)) + jnp.exp(sink_term - top)
    weights = (expo / denom).astype(jnp.bfloat16)
    attended = jnp.einsum('nhgqk,nkhd->nqhgd', weights.astype(jnp.float32), value_band.astype(jnp.float32))
    return attended.astype(jnp.bfloat16)

def reference(tokens, norm_gain, gla_query_weight, gla_key_weight, gla_value_weight, decay_down, decay_up, decay_bias, head_gain, window_query_weight, window_key_weight, window_value_weight, sink_logit, gla_output_weight, window_output_weight):

    def one_sequence(seq_rows):
        seq_len = seq_rows.shape[0]
        normed = rms_rows(seq_rows.astype(jnp.float32), norm_gain).astype(jnp.bfloat16)

        def project(weight):
            return jnp.dot(normed, weight, preferred_element_type=jnp.float32).astype(jnp.bfloat16)
        gla_query = project(gla_query_weight)
        gla_key = project(gla_key_weight)
        gla_value = project(gla_value_weight)
        low_rank = project(decay_down)
        gate_logit_values = jnp.dot(low_rank, decay_up, preferred_element_type=jnp.float32) + decay_bias
        log_decay_rate = jax.nn.log_sigmoid(gate_logit_values) / SOFTMAX_TEMPER
        q_dec, local_out, entering, last_state, block_total = block_terms(gla_query.astype(jnp.float32).reshape(seq_len, GLA_HEADS, KEY_DIM), gla_key.astype(jnp.float32).reshape(seq_len, GLA_HEADS, KEY_DIM), gla_value.astype(jnp.float32).reshape(seq_len, GLA_HEADS, VALUE_DIM), log_decay_rate.reshape(seq_len, GLA_HEADS, KEY_DIM), SPAN)
        gla_out = local_out + jnp.einsum('nihd,nhde->nihe', q_dec, entering, precision=HIGH)
        gla_out = gla_out.reshape(seq_len, GLA_HEADS, VALUE_DIM)
        gla_hidden = rms_rows(gla_out, head_gain).astype(jnp.bfloat16).reshape(seq_len, GLA_HEADS * VALUE_DIM)
        window_query = project(window_query_weight)
        sliding_key = project(window_key_weight)
        window_value = project(window_value_weight)
        block_count = seq_len // WINDOW
        group_size = SWA_HEADS // KV_HEADS
        query_blocks = window_query.reshape(block_count, WINDOW, KV_HEADS, group_size, HEAD_DIM)

        def banded(rows):
            blocks = rows.reshape(block_count, WINDOW, KV_HEADS, HEAD_DIM)
            earlier = jnp.concatenate([jnp.zeros_like(blocks[:1]), blocks[:-1]], axis=0)
            return jnp.concatenate([earlier, blocks], axis=1)
        valid = window_band_mask(block_count, WINDOW, 0)
        sinks = sink_logit.reshape(KV_HEADS, group_size)
        window_hidden = window_attend(query_blocks, banded(sliding_key), banded(window_value), valid, sinks)
        window_hidden = window_hidden.reshape(seq_len, SWA_HEADS * HEAD_DIM)
        total = jnp.dot(gla_hidden, gla_output_weight, preferred_element_type=jnp.float32)
        total = total + jnp.dot(window_hidden, window_output_weight, preferred_element_type=jnp.float32)
        return total.astype(jnp.bfloat16)
    return lax.map(one_sequence, tokens)
```

```python
import functools

import jax
import jax.numpy as jnp
from jax import lax
from jax.experimental import pallas as pl
from jax.experimental.pallas import tpu as pltpu
from jax.sharding import PartitionSpec as P

KEY_DIM = 64
VALUE_DIM = 128
SWA_HEADS = 16
KV_HEADS = 4
HEAD_DIM = 64
WINDOW = 128
SPAN = 64

EPS = 1e-06
SOFTMAX_TEMPER = 16.0
BF = jnp.bfloat16
F32 = jnp.float32


def rms_rows(values, gain):
    mean_square = jnp.mean(values * values, axis=-1, keepdims=True)
    return values * lax.rsqrt(mean_square + EPS) * gain


def nt(a, b):
    return lax.dot_general(a, b, (((1,), (1,)), ((), ())), preferred_element_type=F32)


def nn(a, b):
    return lax.dot_general(a, b, (((1,), (0,)), ((), ())), preferred_element_type=F32)


def tn(a, b):
    return lax.dot_general(a, b, (((0,), (0,)), ((), ())), preferred_element_type=F32)


def exact(a, b):
    return lax.dot_general(
        a, b, (((1,), (0,)), ((), ())), precision=lax.Precision.HIGHEST, preferred_element_type=F32
    )


def mixer_kernel(
    sizes,
    tok_ref,
    gv_ref,
    wq_ref,
    gq_ref,
    gk_ref,
    wk_ref,
    wv_ref,
    low_ref,
    go_ref,
    wo_ref,
    ngain_ref,
    up_ref,
    bias_ref,
    hgain_ref,
    sink_ref,
    out_ref,
    x_buf,
    w_buf,
    l_buf,
    o_buf,
    proj,
    edge_out,
    edge_in,
    state_out,
    state_in,
    local_out,
    q_far,
    hidden,
    half_out,
    half_in,
    half_own,
    piece_out,
    piece_in,
    piece_own,
    local_sem,
    tok_send,
    tok_recv,
    w_send,
    w_recv,
    l_send,
    l_recv,
    v_send,
    v_recv,
    vp_send,
    vp_recv,
    lp_send,
    lp_recv,
    o_send,
    o_recv,
    edge_sem,
    state_send,
    state_recv,
    half_send,
    half_recv,
    piece_send,
    piece_recv,
):
    sp, fs, tp = sizes
    me = lax.axis_index("sp")
    f = lax.axis_index("fs")
    c = lax.axis_index("tp")
    plane = fs * tp
    mine = f * tp + c
    own = tok_ref.shape[0]
    rows = own * tp
    kc = gv_ref.shape[0]
    MESH = pl.DeviceIdType.MESH

    def remote(src, dst, ssem, rsem, target):
        return pltpu.make_async_remote_copy(
            src_ref=src, dst_ref=dst, send_sem=ssem, recv_sem=rsem,
            device_id=target, device_id_type=MESH,
        )

    def w_rows(s):
        return w_buf.at[pl.ds(pl.multiple_of(s * kc, kc), kc)]

    def w_copy(s, way, first):
        target = {"sp": me + (1 if way == 0 else -1)}
        return remote(
            w_main(s), w_main(s), w_send.at[way, s], w_recv.at[s], target
        )

    side = f % 2
    part = kc // 2
    lpart = low_ref.shape[0] // 2

    def w_main(s):
        return w_rows(s).at[:, : starts[4]]

    def v_rows(s, h):
        at = pl.multiple_of(s * kc + h * part, part)
        return w_buf.at[pl.ds(at, part), starts[4] : starts[4] + 2 * HEAD_DIM]

    def l_rows(s, h):
        return l_buf.at[s, pl.ds(pl.multiple_of(h * lpart, lpart), lpart)]

    def v_copy(s, way):
        target = {"sp": me + (1 if way == 0 else -1)}
        return remote(v_rows(s, side), v_rows(s, side), v_send.at[way, s], v_recv.at[s], target)

    def lh_copy(s, way):
        target = {"sp": me + (1 if way == 0 else -1)}
        return remote(l_rows(s, side), l_rows(s, side), l_send.at[way, s], l_recv.at[s], target)

    def pair_copies(s, h):
        target = {"fs": f + 1 - 2 * side}
        return (
            remote(v_rows(s, h), v_rows(s, h), vp_send.at[s], vp_recv.at[s], target),
            remote(l_rows(s, h), l_rows(s, h), lp_send.at[s], lp_recv.at[s], target),
        )

    class l_copy:
        def __init__(self, s, way, first):
            self.s = s
            self.both = (v_copy(s, way), lh_copy(s, way))

        def start(self):
            for copy in self.both:
                copy.start()

        def wait_recv(self):
            for copy, onward in zip(self.both, pair_copies(self.s, side)):
                copy.wait_recv()
                onward.start()

        def wait_send(self):
            for copy in self.both:
                copy.wait_send()

    def o_copy(s, way, first):
        target = {"sp": me + (1 if way == 0 else -1)}
        return remote(
            o_buf.at[s], o_buf.at[s], o_send.at[way, s], o_recv.at[s], target
        )

    def tok_rows(i):
        return x_buf.at[pl.ds(pl.multiple_of(i * own, own), own)]

    def tok_copy(d, peer, sender):
        return remote(
            tok_ref, tok_rows(sender), tok_send.at[d - 1], tok_recv.at[d - 1],
            {"fs": peer // tp, "tp": peer % tp},
        )

    def pick(ref, width, which):
        value = ref[:, :width]
        for i in range(1, ref.shape[1] // width):
            value = jnp.where(which == i, ref[:, i * width : (i + 1) * width], value)
        return value

    def lanes(ref, width):
        return ref.at[:, pl.ds(pl.multiple_of(f * width, width), width)]

    def depth(ref, width):
        return ref.at[pl.ds(pl.multiple_of(f * width, width), width)]

    cols = [VALUE_DIM, 2 * HEAD_DIM, KEY_DIM, KEY_DIM, HEAD_DIM, HEAD_DIM]
    starts = [sum(cols[:i]) for i in range(len(cols))]
    gd = go_ref.shape[0] // fs
    wd = wo_ref.shape[0] // fs
    heads = sink_ref.shape[1] // fs
    copies_in = [
        (lanes(gv_ref, cols[0]), w_rows(me).at[:, : cols[0]]),
        (lanes(wq_ref, cols[1]), w_rows(me).at[:, starts[1] : starts[2]]),
        (depth(go_ref, gd), o_buf.at[me, pl.ds(0, gd)]),
        (depth(wo_ref, wd), o_buf.at[me, pl.ds(gd, wd)]),
        (low_ref, l_buf.at[me]),
        (tok_ref, tok_rows(mine)),
    ]
    locals_ = [
        pltpu.make_async_copy(a, b, local_sem.at[i]) for i, (a, b) in enumerate(copies_in)
    ]
    for copy in locals_:
        copy.start()
    for d in range(1, plane):
        tok_copy(d, lax.rem(mine + d, plane), mine).start()
    own_rows = pl.ds(pl.multiple_of(me * kc, kc), kc)
    kv = (f * heads) // (SWA_HEADS // KV_HEADS)
    w_buf[own_rows, starts[2] : starts[4]] = jnp.concatenate(
        [pick(gq_ref, KEY_DIM, f), pick(gk_ref, KEY_DIM, f)], 1
    )
    w_buf[own_rows, starts[4] :] = jnp.concatenate(
        [pick(wk_ref, HEAD_DIM, kv), pick(wv_ref, HEAD_DIM, kv)], 1
    )
    for copy in locals_[:5]:
        copy.wait()

    def sends(k):
        @pl.when((me - k >= 0) & (me + 1 < sp))
        def _():
            l_copy(me - k, 0, k == 0).start()
            w_copy(me - k, 0, k == 0).start()

        @pl.when((me + k < sp) & (me >= 1))
        def _():
            l_copy(me + k, 1, k == 0).start()
            w_copy(me + k, 1, k == 0).start()

        @pl.when((me == k) & (me + 1 < sp))
        def _():
            o_copy(me, 0, True).start()

        @pl.when((sp - 1 - me == k) & (me >= 1))
        def _():
            o_copy(me, 1, True).start()

    for k in range(sp - 1):
        sends(k)

        @pl.when(me - 1 - k >= 0)
        def _():
            l_copy(me - 1 - k, 0, False).wait_recv()
            w_copy(me - 1 - k, 0, False).wait_recv()

        @pl.when(me + 1 + k < sp)
        def _():
            l_copy(me + 1 + k, 1, False).wait_recv()
            w_copy(me + 1 + k, 1, False).wait_recv()

    inner = (me >= 1) & (me + 1 < sp)
    for k in range(1, sp - 1):
        @pl.when(inner & (me - k >= 0))
        def _():
            o_copy(me - k, 0, False).wait_recv()
            o_copy(me - k, 0, False).start()

        @pl.when(inner & (me + k < sp))
        def _():
            o_copy(me + k, 1, False).wait_recv()
            o_copy(me + k, 1, False).start()

    for copy in locals_[5:]:
        copy.wait()
    for i in range(sp):
        @pl.when(i != me)
        def _():
            for copy in pair_copies(i, 1 - side):
                copy.wait_recv()

    for d in range(1, plane):
        tok_copy(d, mine, lax.rem(mine + plane - d, plane)).wait_recv()


    def project(b, _):
        x = x_buf[pl.ds(pl.multiple_of(b * rows, rows), rows)].astype(F32)
        normed = rms_rows(x, ngain_ref[...]).astype(BF)
        p = nn(normed, w_buf[...]).astype(BF)
        proj[b, :, : p.shape[1]] = p
        edge_out[b] = p[rows - WINDOW :, starts[4] : starts[4] + 2 * HEAD_DIM]
        low = nt(normed[:, :kc], l_buf[0])
        for s in range(1, sp):
            low += nt(normed[:, s * kc : (s + 1) * kc], l_buf[s])
        proj[b, :, p.shape[1] : p.shape[1] + low.shape[1]] = low.astype(BF)
        return 0

    lax.fori_loop(0, fs, project, 0)
    edge = remote(edge_out, edge_in, edge_sem.at[0], edge_sem.at[1], {"sp": me + 1})

    @pl.when(me + 1 < sp)
    def _():
        edge.start()

    @pl.when(me == 0)
    def _():
        edge_in[...] = jnp.zeros_like(edge_in)

    nb = rows // SPAN
    low_at = sum(cols)
    lower = (
        lax.broadcasted_iota(jnp.int32, (SPAN, SPAN), 0)
        >= lax.broadcasted_iota(jnp.int32, (SPAN, SPAN), 1)
    )
    tri = lower.astype(F32)
    up = pick(up_ref, KEY_DIM, f)
    bias = pick(bias_ref, KEY_DIM, f)
    sinks = pick(sink_ref, heads, f)
    for b in range(fs):
        low = proj[b, :, low_at : low_at + up_ref.shape[0]]
        z = nn(low, up) + bias
        rate = (jnp.minimum(z, 0.0) - jnp.log1p(jnp.exp(-jnp.abs(z)))) / SOFTMAX_TEMPER
        state = None
        before = jnp.zeros((1, KEY_DIM), F32)
        for n in range(nb):
            r0 = n * SPAN
            within = exact(tri, rate[r0 : r0 + SPAN])
            total = within[SPAN - 1 :]
            v = proj[b, r0 : r0 + SPAN, starts[0] : starts[0] + VALUE_DIM]
            q = proj[b, r0 : r0 + SPAN, starts[2] : starts[2] + KEY_DIM].astype(F32)
            k = proj[b, r0 : r0 + SPAN, starts[3] : starts[3] + KEY_DIM].astype(F32)
            q_dec = q * KEY_DIM**-0.5 * jnp.exp(within)
            k_dec = (k * jnp.exp(-within)).astype(BF)
            k_end = (k * jnp.exp(total - within)).astype(BF)
            scores = jnp.where(lower, nt(q_dec.astype(BF), k_dec), 0.0)
            o = nn(scores.astype(BF), v)
            if state is not None:
                o += nt(q_dec.astype(BF), state.astype(BF))
            local_out[b, r0 : r0 + SPAN] = o
            q_far[b, r0 : r0 + SPAN] = (q_dec * jnp.exp(before)).astype(BF)
            update = tn(v, k_end)
            state = update if state is None else jnp.exp(total) * state + update
            before = before + total
        half = (b % 2) * KEY_DIM
        state_out[b // 2, :VALUE_DIM, half : half + KEY_DIM] = state.astype(BF)
        state_out[b // 2, VALUE_DIM:, half : half + KEY_DIM] = jnp.broadcast_to(
            jnp.exp(before), (16, KEY_DIM)
        ).astype(BF)

    def state_copy(d, sender):
        return remote(
            state_out, state_in.at[sender], state_send.at[d - 1], state_recv.at[sender],
            {"sp": me + d},
        )

    for d in range(1, sp):
        @pl.when(me + d < sp)
        def _():
            state_copy(d, me).start()

    @pl.when(me >= 1)
    def _():
        edge.wait_recv()

    qi = lax.broadcasted_iota(jnp.int32, (WINDOW, 2 * WINDOW), 0)
    ki = lax.broadcasted_iota(jnp.int32, (WINDOW, 2 * WINDOW), 1)
    distance = qi + WINDOW - ki
    inside = (distance >= 0) & (distance < WINDOW)
    for b in range(fs):
        for w in range(rows // WINDOW):
            r0 = w * WINDOW
            here = proj[b, r0 : r0 + WINDOW, starts[4] : starts[4] + 2 * HEAD_DIM]
            if w == 0:
                past = edge_in[b]
                valid = inside & ((ki >= WINDOW) | (me >= 1))
            else:
                past = proj[b, r0 - WINDOW : r0, starts[4] : starts[4] + 2 * HEAD_DIM]
                valid = inside
            band = jnp.concatenate([past, here], 0)
            bk = band[:, :HEAD_DIM]
            bv = band[:, HEAD_DIM:]
            for h in range(heads):
                q0 = starts[1] + h * HEAD_DIM
                q = proj[b, r0 : r0 + WINDOW, q0 : q0 + HEAD_DIM]
                s = jnp.where(valid, nt(q, bk) * HEAD_DIM**-0.5, -1e30)
                sink = sinks[:, h : h + 1]
                top = jnp.maximum(jnp.max(s, -1, keepdims=True), sink)
                e = jnp.exp(s - top)
                den = jnp.sum(e, -1, keepdims=True) + jnp.exp(sink - top)
                a = nn((e / den).astype(BF), bv).astype(BF)
                h0 = VALUE_DIM + h * HEAD_DIM
                hidden[b, r0 : r0 + WINDOW, h0 : h0 + HEAD_DIM] = a

    for i in range(sp - 1):
        @pl.when(i < me)
        def _():
            state_copy(1, i).wait_recv()

        @pl.when(i >= me)
        def _():
            state_in[i] = jnp.zeros(state_in.shape[1:], BF)

    for b in range(fs):
        half = (b % 2) * KEY_DIM
        incoming = jnp.zeros((VALUE_DIM, KEY_DIM), F32)
        for i in range(sp - 1):
            got = state_in[i, b // 2, :VALUE_DIM, half : half + KEY_DIM].astype(F32)
            kept = state_in[i, b // 2, VALUE_DIM : VALUE_DIM + 1, half : half + KEY_DIM].astype(F32)
            incoming = jnp.where(i < me, kept * incoming + got, incoming)
        o = local_out[b] + nt(q_far[b], incoming.astype(BF))
        hidden[b, :, :VALUE_DIM] = rms_rows(o, hgain_ref[...]).astype(BF)

    forward = 2 * me < sp
    nc = o_buf.shape[2]

    def chunk(t):
        return lax.rem(jnp.where(forward, me + t, me - t) + sp, sp)

    def half_copy(s):
        return remote(half_out.at[s], half_in.at[s], half_send.at[s], half_recv.at[s], {"tp": 1 - c})

    def piece_copy(s, d, target):
        return remote(
            piece_out.at[s, d - 1], piece_in.at[s, d - 1],
            piece_send.at[s, d - 1], piece_recv.at[s, d - 1], {"fs": target},
        )

    def produce(t):
        s = chunk(t)

        @pl.when(jnp.logical_not(inner) & (t > 0))
        def _():
            o_copy(s, 0, False).wait_recv()

        w = o_buf[s]
        for b in range(fs):
            part = nn(hidden[b], w)
            lo, hi = part[:own], part[own:]
            half_out[s, b] = jnp.where(c == 0, hi, lo).astype(BF)
            half_own[s, b] = jnp.where(c == 0, lo, hi)
        half_copy(s).start()

    def combine(t):
        s = chunk(t)
        half_copy(s).wait_recv()
        for d in range(1, fs):
            to = lax.rem(f + d, fs)
            piece_out[s, d - 1] = (half_own[s, to] + half_in[s, to].astype(F32)).astype(BF)
            piece_copy(s, d, to).start()
        piece_own[s] = half_own[s, f] + half_in[s, f].astype(F32)

    def finish(t):
        s = chunk(t)
        total = piece_own[s]
        for d in range(1, fs):
            piece_copy(s, d, f).wait_recv()
            total += piece_in[s, d - 1].astype(F32)
        if len(out_ref.shape) == 2:
            out_ref[:, pl.ds(pl.multiple_of(s * nc, nc), nc)] = total.astype(BF)
        else:
            out_ref[s] = total.astype(BF)

    produce(0)

    def steady(t, _):
        produce(t)
        combine(t - 1)
        return 0

    lax.fori_loop(1, sp, steady, 0)
    combine(sp - 1)

    def close(t, _):
        finish(t)
        s = chunk(t)
        half_copy(s).wait_send()
        for d in range(1, fs):
            piece_copy(s, d, f).wait_send()
        return 0

    lax.fori_loop(0, sp, close, 0)

    for k in range(sp - 1):
        @pl.when((me - k >= 0) & (me + 1 < sp))
        def _():
            l_copy(me - k, 0, False).wait_send()
            w_copy(me - k, 0, False).wait_send()
            o_copy(me - k, 0, False).wait_send()

        @pl.when((me + k < sp) & (me >= 1))
        def _():
            l_copy(me + k, 1, False).wait_send()
            w_copy(me + k, 1, False).wait_send()
            o_copy(me + k, 1, False).wait_send()

    for i in range(sp):
        @pl.when(i != me)
        def _():
            for copy in pair_copies(i, side):
                copy.wait_send()

    for d in range(1, plane):
        tok_copy(d, mine, mine).wait_send()

    @pl.when(me + 1 < sp)
    def _():
        edge.wait_send()

    for d in range(1, sp):
        @pl.when(me + d < sp)
        def _():
            state_copy(d, me).wait_send()


def roll_half(a):
    return jnp.concatenate([a[:, a.shape[1] // 2 :], a[:, : a.shape[1] // 2]], 1)


def fold_kernel(
    sizes,
    tok_ref,
    gv_ref,
    wq_ref,
    gq_ref,
    gk_ref,
    wk_ref,
    wv_ref,
    low_ref,
    go_ref,
    wo_ref,
    ngain_ref,
    up_ref,
    bias_ref,
    hgain_ref,
    sink_ref,
    out_ref,
    x_buf,
    ww,
    wg,
    wl,
    o_buf,
    tiles,
    qw,
    kvb,
    gvb,
    qkb,
    lowb,
    decays,
    totals,
    states,
    state_out,
    state_in,
    local_out,
    q_far,
    hidden,
    half_out,
    half_in,
    half_own,
    piece_out,
    piece_in,
    piece_own,
    local_sem,
    x_send,
    x_recv,
    w_send,
    w_recv,
    p_send,
    p_recv,
    o_send,
    o_recv,
    edge_sem,
    state_sem,
    hid_send,
    hid_recv,
    half_send,
    half_recv,
    piece_send,
    piece_recv,
):
    sp, fs, tp = sizes
    me = lax.axis_index("sp")
    f = lax.axis_index("fs")
    c = lax.axis_index("tp")
    own = tok_ref.shape[0]
    rows = own * tp
    kc = gv_ref.shape[0]
    part = kc // 2
    lpart = low_ref.shape[0] // 2
    MESH = pl.DeviceIdType.MESH
    pair = 2 * KEY_DIM
    wide = VALUE_DIM + pair

    slot = lax.rem(me, 2)
    far_slot = 1 - slot
    inner = (me >= 1) & (me + 1 < sp)
    outer = jnp.logical_not(inner)
    middle = 1 + slot
    outside = (sp - 1) * (me - 1)
    buddy = me + 1 - 2 * slot
    third = 2 - me // 2
    fourth = third + 1 - 2 * lax.rem(third, 2)
    chunks = [me, buddy, third, fourth]
    side = lax.rem(f, 2)
    xn = f + 1 - 2 * side
    yn = lax.rem(f + 2, fs)
    n1 = xn * (1 - c) + yn * c
    n2 = xn * c + yn * (1 - c)

    def remote(src, dst, ssem, rsem, target):
        return pltpu.make_async_remote_copy(
            src_ref=src, dst_ref=dst, send_sem=ssem, recv_sem=rsem,
            device_id=target, device_id_type=MESH,
        )

    barrier = pltpu.get_barrier_semaphore()

    def greet(target):
        pl.semaphore_signal(barrier, inc=1, device_id=target, device_id_type=MESH)

    greet({"tp": 1 - c})
    for d in range(1, fs):
        greet({"fs": lax.rem(f + d, fs)})

    @pl.when(me + 1 < sp)
    def _():
        greet({"sp": me + 1})

    @pl.when(me >= 1)
    def _():
        greet({"sp": me - 1})

    def lanes(ref, at, width):
        return ref.at[:, pl.ds(pl.multiple_of(at * width, width), width)]

    def depth(ref, width):
        return ref.at[pl.ds(pl.multiple_of(f * width, width), width)]

    def slice_rows(ref, s):
        return ref.at[pl.ds(pl.multiple_of(s * kc, kc), kc)]

    gd = go_ref.shape[0] // fs
    wd = wo_ref.shape[0] // fs
    heads = sink_ref.shape[1] // fs
    wq_cols = heads * HEAD_DIM
    kv = (f * heads) // (SWA_HEADS // KV_HEADS)
    copies_in = [
        (lanes(gq_ref, f // 2, pair), tiles.at[0]),
        (lanes(gk_ref, f // 2, pair), tiles.at[1]),
        (wk_ref, tiles.at[2]),
        (wv_ref, tiles.at[3]),
        (lanes(wq_ref, f, wq_cols), slice_rows(ww, me).at[:, :wq_cols]),
        (lanes(gv_ref, f, VALUE_DIM), slice_rows(wg, me).at[:, :VALUE_DIM]),
        (low_ref, wl.at[me]),
        (depth(go_ref, gd), o_buf.at[me, pl.ds(0, gd)]),
        (depth(wo_ref, wd), o_buf.at[me, pl.ds(gd, wd)]),
    ]
    locals_ = [
        pltpu.make_async_copy(a, b, local_sem.at[i]) for i, (a, b) in enumerate(copies_in)
    ]
    for copy in locals_:
        copy.start()

    def block(s, i):
        return x_buf.at[s, pl.ds(pl.multiple_of(i * own, own), own)]

    mine = f * tp + c
    b1, b2, b3 = n1 * tp + c, n2 * tp + c, (fs - 1 - f) * tp + c

    normed = rms_rows(tok_ref[...].astype(F32), ngain_ref[...]).astype(BF)
    x_buf[slot, pl.ds(pl.multiple_of(mine * own, own), own)] = normed

    def x_copy(s, i, k, target):
        return remote(block(s, i), block(s, i), x_send.at[s, k], x_recv.at[s, i], target)

    SIB = {"tp": 1 - c}

    def x_first(s):
        return [
            x_copy(s, mine, 0, {"fs": n1}),
            x_copy(s, mine, 1, {"fs": n2}),
            x_copy(s, mine, 2, SIB),
        ]

    def x_from1(s):
        return [x_copy(s, b1, 3, {"fs": n2}), x_copy(s, b1, 4, SIB)]

    def x_from2(s):
        return [x_copy(s, b2, 5, SIB)]

    def x_from3(s):
        return [x_copy(s, b3, 6, SIB)]

    def x_all(s):
        return x_first(s) + x_from1(s) + x_from2(s) + x_from3(s)

    def x_out():
        return x_copy(slot, mine, 0, {"sp": middle})

    def kv_rows(s, h):
        at = pl.multiple_of(s * kc + h * part, part)
        return ww.at[pl.ds(at, part), wq_cols:]

    def low_rows(s, h):
        return wl.at[s, pl.ds(pl.multiple_of(h * lpart, lpart), lpart)]

    def w_copy(kind, s):
        ref = (
            lambda: slice_rows(ww, s).at[:, :wq_cols],
            lambda: kv_rows(s, side),
            lambda: low_rows(s, c),
            lambda: slice_rows(wg, s),
        )[kind]()
        return remote(ref, ref, w_send.at[kind, s], w_recv.at[kind, s], {"sp": middle})

    def kv_share(s, h):
        return remote(
            kv_rows(s, h), kv_rows(s, h), p_send.at[0, s], p_recv.at[0, s], {"fs": xn}
        )

    def low_share(s, h):
        return remote(low_rows(s, h), low_rows(s, h), p_send.at[1, s], p_recv.at[1, s], SIB)

    def o_copy(way, s):
        target = {"sp": middle if way == 0 else outside}
        return remote(o_buf.at[s], o_buf.at[s], o_send.at[way, s], o_recv.at[s], target)

    def start(copies):
        for copy in copies:
            copy.start()

    pl.semaphore_wait(barrier, fs + jnp.where(inner, 2, 1))

    @pl.when(outer)
    def _():
        x_out().start()

    @pl.when(inner)
    def _():
        start(x_first(slot))

    for copy in locals_[:7]:
        copy.wait()
    own_rows = pl.ds(pl.multiple_of(me * kc, kc), kc)

    def half_of(i, width, which):
        return jnp.where(which == 0, tiles[i, :, :width], tiles[i, :, width:])

    ww[own_rows, wq_cols:] = jnp.concatenate(
        [half_of(2, HEAD_DIM, kv), half_of(3, HEAD_DIM, kv)], 1
    )
    for kind in range(3):
        w_copy(kind, me).start()
    wg[own_rows, VALUE_DIM:] = jnp.concatenate(
        [half_of(0, KEY_DIM, side), half_of(1, KEY_DIM, side)], 1
    )
    w_copy(3, me).start()
    for copy in locals_[7:]:
        copy.wait()

    @pl.when(outer)
    def _():
        o_copy(0, me).start()

    lane = lax.broadcasted_iota(jnp.int32, (rows, pair), 1)
    row = lax.broadcasted_iota(jnp.int32, (rows, pair), 0)
    left = lane < KEY_DIM
    early = row < SPAN
    same = (row < SPAN) == (lane < SPAN)
    diagonal = same & (row >= lane)
    below = (row >= SPAN) & (lane < SPAN)

    edge = remote(kvb.at[2], kvb.at[0], edge_sem.at[0], edge_sem.at[1], {"sp": me + 1})
    state = remote(state_out, state_in, state_sem.at[0], state_sem.at[1], {"sp": me + 1})

    def hid_part(s, i):
        return hidden.at[s, :, i * VALUE_DIM : (i + 1) * VALUE_DIM]

    def hid_copy(i, s):
        return remote(
            hid_part(s, i), hid_part(s, i), hid_send.at[i], hid_recv.at[i], {"sp": outside}
        )

    def seq(b):
        if isinstance(b, int):
            return pl.ds(b * rows, rows)
        return pl.ds(pl.multiple_of(b * rows, rows), rows)

    @pl.when(inner)
    def _():
        o_copy(1, me).start()
        x_copy(far_slot, mine, 0, SIB).wait_recv()
        start(x_first(far_slot))

        def got_first(s, onward):
            for kind in range(3):
                w_copy(kind, s).wait_recv()
                if onward:
                    w_copy(kind, s).start()
            kv_share(s, side).start()
            low_share(s, c).start()

        def neighbours(s):
            x_copy(s, b1, 0, SIB).wait_recv()
            start(x_from1(s))
            x_copy(s, b2, 0, SIB).wait_recv()
            start(x_from2(s))

        def corner(s):
            x_copy(s, b3, 0, SIB).wait_recv()
            start(x_from3(s))

        got_first(third, False)
        neighbours(slot)
        corner(slot)
        got_first(buddy, True)
        neighbours(far_slot)
        w_copy(3, buddy).wait_recv()
        w_copy(3, buddy).start()
        o_copy(0, me).start()
        corner(far_slot)
        got_first(fourth, False)
        for s in chunks[1:]:
            kv_share(s, 1 - side).wait_recv()
            low_share(s, 1 - c).wait_recv()
        for s in range(2):
            for g in range(fs):
                x_copy(s, g * tp + 1 - c, 0, SIB).wait_recv()

        def first_maps(i, _):
            s = i // fs
            b = lax.rem(i, fs)
            x = x_buf[s, seq(b)]
            p = nn(x, ww[...])
            qw[s, seq(b)] = (p[:, :wq_cols].astype(BF).astype(F32) * HEAD_DIM**-0.5).astype(BF)
            kvb[s + 1, seq(b)] = p[:, wq_cols:].astype(BF)
            low = nt(x[:, :kc], wl[0])
            for j in range(1, sp):
                low += nt(x[:, j * kc : (j + 1) * kc], wl[j])
            lowb[s, seq(b)] = low.astype(BF)
            return 0

        lax.fori_loop(0, 2 * fs, first_maps, 0)

        @pl.when(me == 1)
        def _():
            edge.start()
            kvb[0] = jnp.zeros(kvb.shape[1:], BF)
            state_in[...] = jnp.zeros_like(state_in)

        up = jnp.where(side == 0, up_ref[:, :KEY_DIM], up_ref[:, KEY_DIM:pair])
        up1 = jnp.where(side == 0, up_ref[:, pair : pair + KEY_DIM], up_ref[:, pair + KEY_DIM :])
        up = jnp.where(f // 2 == 0, up, up1)
        bs = [bias_ref[:, i * KEY_DIM : (i + 1) * KEY_DIM] for i in range(fs)]
        bias = bs[0]
        for i in range(1, fs):
            bias = jnp.where(f == i, bs[i], bias)
        up_l = jnp.concatenate([up, jnp.zeros_like(up)], 1)
        up_r = jnp.concatenate([jnp.zeros_like(up), up], 1)
        bias2 = jnp.concatenate([bias, bias], 1)
        tri = diagonal.astype(F32)
        for s in range(2):
            for p in range(fs // 2):
                z = nn(lowb[s, seq(2 * p)], up_l) + nn(lowb[s, seq(2 * p + 1)], up_r) + bias2
                rate = (jnp.minimum(z, 0.0) - jnp.log1p(jnp.exp(-jnp.abs(z)))) / SOFTMAX_TEMPER
                within = exact(tri, rate)
                t0, t1 = within[SPAN - 1 : SPAN], within[rows - 1 :]
                grow = jnp.exp(within) * KEY_DIM**-0.5
                end = jnp.exp(jnp.where(early, t0, t1) - within)
                decays[s, p, 0] = grow
                decays[s, p, 1] = jnp.exp(-within)
                decays[s, p, 2] = end
                decays[s, p, 3] = grow * jnp.where(early, 1.0, jnp.exp(t0))
                decays[s, p, 4] = end * jnp.where(early, jnp.exp(t1), 1.0)
                totals[s, p] = jnp.broadcast_to(jnp.exp(t0 + t1), totals.shape[2:])

        qi = lax.broadcasted_iota(jnp.int32, (WINDOW, 2 * WINDOW), 0)
        ki = lax.broadcasted_iota(jnp.int32, (WINDOW, 2 * WINDOW), 1)
        distance = qi + WINDOW - ki
        inside = (distance >= 0) & (distance < WINDOW)
        sinks = sink_ref[:, :heads]
        for i in range(1, fs):
            sinks = jnp.where(f == i, sink_ref[:, i * heads : (i + 1) * heads], sinks)

        def window(s):
            valid = inside & ((ki >= WINDOW) | (me > 1) | (s > 0))

            def one(b, _):
                band = jnp.concatenate([kvb[s, seq(b)], kvb[s + 1, seq(b)]], 0)
                q = qw[s, seq(b)].astype(F32)
                outs = []
                for h in range(heads):
                    qh = jnp.where(left, q if h == 0 else roll_half(q), 0.0).astype(BF)
                    sc = jnp.where(valid, nt(qh, band), -1e30)
                    sink = sinks[:, h : h + 1]
                    top = jnp.maximum(jnp.max(sc, -1, keepdims=True), sink)
                    e = jnp.exp(sc - top)
                    den = jnp.sum(e, -1, keepdims=True) + jnp.exp(sink - top)
                    outs.append(nn((e * (1.0 / den)).astype(BF), band))
                hidden[s, seq(b), VALUE_DIM:] = jnp.where(left, roll_half(outs[0]), outs[1]).astype(BF)
                return 0

            for b in range(fs):
                one(b, 0)

        window(far_slot)
        hid_copy(1, far_slot).start()
        w_copy(3, third).wait_recv()
        w_copy(3, fourth).wait_recv()

        def second_maps(i, _):
            s = i // fs
            b = lax.rem(i, fs)
            p = nn(x_buf[s, seq(b)], wg[...]).astype(BF)
            gvb[s, seq(b)] = p[:, :VALUE_DIM]
            qkb[s, seq(b)] = p[:, VALUE_DIM:].astype(F32)
            return 0

        lax.fori_loop(0, 2 * fs, second_maps, 0)

        def keys(s, p):
            return jnp.where(left, roll_half(qkb[s, seq(2 * p)]), qkb[s, seq(2 * p + 1)])

        def queries(s, p):
            return jnp.where(left, qkb[s, seq(2 * p)], roll_half(qkb[s, seq(2 * p + 1)]))

        for s in range(2):
            for p in range(fs // 2):
                k_far = (keys(s, p) * decays[s, p, 4]).astype(BF)
                states[s, p] = jnp.where(
                    left, tn(gvb[s, seq(2 * p)], k_far), tn(gvb[s, seq(2 * p + 1)], k_far)
                )
        for p in range(fs // 2):
            state_out[p] = (totals[1, p, :1] * states[0, p] + states[1, p]).astype(BF)

        @pl.when(me == 1)
        def _():
            state.start()

        o_copy(0, buddy).wait_recv()
        o_copy(0, buddy).start()

        for s in range(2):
            for p in range(fs // 2):
                k = keys(s, p)
                q = queries(s, p)
                qd = q * decays[s, p, 0]
                qf = q * decays[s, p, 3]
                kd = (k * decays[s, p, 1]).astype(BF)
                ke = (k * decays[s, p, 2]).astype(BF)
                for j in range(2):
                    here = left if j == 0 else jnp.logical_not(left)
                    qj = jnp.where(here, qd, 0.0).astype(BF)
                    scores = jnp.where(
                        diagonal, nt(qj, kd), jnp.where(below, nt(qj, ke), 0.0)
                    ).astype(BF)
                    local_out[s, seq(2 * p + j)] = nn(scores, gvb[s, seq(2 * p + j)])
                    q_far[s, seq(2 * p + j)] = jnp.where(here, qf, 0.0).astype(BF)

        @pl.when(me > 1)
        def _():
            state.wait_recv()

        def finish_state(s):
            for p in range(fs // 2):
                arrived = state_in[p].astype(F32)
                entering = jnp.where(s == 0, arrived, totals[0, p, :1] * arrived + states[0, p])
                entering = entering.astype(BF)
                for j in range(2):
                    b = 2 * p + j
                    o = local_out[s, seq(b)] + nt(q_far[s, seq(b)], entering)
                    hidden[s, seq(b), :VALUE_DIM] = rms_rows(o, hgain_ref[...]).astype(BF)

        finish_state(far_slot)
        hid_copy(0, far_slot).start()
        finish_state(slot)

        @pl.when(me > 1)
        def _():
            edge.wait_recv()

        window(slot)

    @pl.when(outer)
    def _():
        hid_copy(1, slot).wait_recv()
        hid_copy(0, slot).wait_recv()

    nc = o_buf.shape[2]

    def half_copy(s):
        return remote(half_out.at[s], half_in.at[s], half_send.at[s], half_recv.at[s], SIB)

    def piece_copy(s, d, target):
        return remote(
            piece_out.at[s, d - 1], piece_in.at[s, d - 1],
            piece_send.at[s, d - 1], piece_recv.at[s, d - 1], {"fs": target},
        )

    def produce(t):
        s = chunks[t]
        if t == 1:
            @pl.when(outer)
            def _():
                o_copy(0, s).wait_recv()
        if t > 1:
            o_copy(0, s).wait_recv()

            @pl.when(inner)
            def _():
                o_copy(1, s).start()

        w = o_buf[s]
        for b in range(fs):
            partial = nn(hidden[slot, seq(b)], w)
            lo, hi = partial[:own], partial[own:]
            half_out[s, b] = jnp.where(c == 0, hi, lo).astype(BF)
            half_own[s, b] = jnp.where(c == 0, lo, hi)
        half_copy(s).start()

    def combine(t):
        s = chunks[t]
        half_copy(s).wait_recv()
        for d in range(1, fs):
            to = lax.rem(f + d, fs)
            piece_out[s, d - 1] = (half_own[s, to] + half_in[s, to].astype(F32)).astype(BF)
            piece_copy(s, d, to).start()
        piece_own[s] = half_own[s, f] + half_in[s, f].astype(F32)

    def finish(t):
        s = chunks[t]
        total = piece_own[s]
        for d in range(1, fs):
            piece_copy(s, d, f).wait_recv()
            total += piece_in[s, d - 1].astype(F32)
        out_ref[:, pl.ds(pl.multiple_of(s * nc, nc), nc)] = total.astype(BF)

    produce(0)
    for t in range(1, sp):
        produce(t)
        combine(t - 1)
    combine(sp - 1)
    for t in range(sp):
        finish(t)
    for t in range(sp):
        s = chunks[t]
        half_copy(s).wait_send()
        for d in range(1, fs):
            piece_copy(s, d, f).wait_send()

    for kind in range(4):
        w_copy(kind, me).wait_send()
    o_copy(0, me).wait_send()

    @pl.when(outer)
    def _():
        x_out().wait_send()

    @pl.when(inner)
    def _():
        for s in range(2):
            for copy in x_all(s):
                copy.wait_send()
        for kind in range(4):
            w_copy(kind, buddy).wait_send()
        for s in chunks[1:]:
            kv_share(s, side).wait_send()
            low_share(s, c).wait_send()
        o_copy(0, buddy).wait_send()
        for s in (me, third, fourth):
            o_copy(1, s).wait_send()
        for i in range(2):
            hid_copy(i, far_slot).wait_send()

        @pl.when(me == 1)
        def _():
            edge.wait_send()
            state.wait_send()


def fold_call(sizes, operands):
    sp, fs, tp = sizes
    own, d = operands[0].shape
    rows = own * tp
    kc = operands[1].shape[0]
    rank = operands[7].shape[0]
    depth = (operands[8].shape[0] + operands[9].shape[0]) // fs
    nc = operands[8].shape[1]
    pair = 2 * KEY_DIM
    all_rows = fs * rows
    pairs = fs // 2
    vm = pltpu.VMEM
    dma = pltpu.SemaphoreType.DMA
    scratch = [
        vm((2, all_rows, d), BF),
        vm((d, 2 * pair), BF),
        vm((d, VALUE_DIM + pair), BF),
        vm((sp, rank, kc), BF),
        vm((sp, depth, nc), BF),
        vm((4, kc, pair), BF),
        vm((2, all_rows, pair), BF),
        vm((3, all_rows, pair), BF),
        vm((2, all_rows, VALUE_DIM), BF),
        vm((2, all_rows, pair), F32),
        vm((2, all_rows, rank), BF),
        vm((2, pairs, 5, rows, pair), F32),
        vm((2, pairs, 8, pair), F32),
        vm((2, pairs, VALUE_DIM, pair), F32),
        vm((pairs, VALUE_DIM, pair), BF),
        vm((pairs, VALUE_DIM, pair), BF),
        vm((2, all_rows, VALUE_DIM), F32),
        vm((2, all_rows, pair), BF),
        vm((2, all_rows, depth), BF),
        vm((sp, fs, own, nc), BF),
        vm((sp, fs, own, nc), BF),
        vm((sp, fs, own, nc), F32),
        vm((sp, fs - 1, own, nc), BF),
        vm((sp, fs - 1, own, nc), BF),
        vm((sp, own, nc), F32),
        dma((9,)),
        dma((2, 7)),
        dma((2, fs * tp)),
        dma((4, sp)),
        dma((4, sp)),
        dma((2, sp)),
        dma((2, sp)),
        dma((2, sp)),
        dma((sp,)),
        dma((2,)),
        dma((2,)),
        dma((2,)),
        dma((2,)),
        dma((sp,)),
        dma((sp,)),
        dma((sp, fs - 1)),
        dma((sp, fs - 1)),
    ]
    spec = pl.BlockSpec(memory_space=pltpu.VMEM)
    anywhere = pl.BlockSpec(memory_space=pl.ANY)
    return pl.pallas_call(
        functools.partial(fold_kernel, sizes),
        out_shape=jax.ShapeDtypeStruct((own, sp * nc), BF),
        in_specs=[anywhere if i in (1, 2, 3, 4, 5, 6, 8, 9) else spec for i in range(15)],
        out_specs=spec,
        scratch_shapes=scratch,
        compiler_params=pltpu.CompilerParams(
            has_side_effects=True, vmem_limit_bytes=60 * 1024 * 1024, collective_id=0
        ),
    )(*operands)


def folds(sp, fs, tp, shape, rows, kc, width, rank, nc, depth):
    whole_rows = rows == WINDOW == 2 * SPAN
    lanes_fit = nc % 128 == 0 and kc % 128 == 0 and depth == 2 * VALUE_DIM
    return sp == 4 and fs == 4 and tp == 2 and whole_rows and lanes_fit and rank % 32 == 0


def per_device(
    tokens,
    norm_gain,
    gla_query_weight,
    gla_key_weight,
    gla_value_weight,
    decay_down,
    decay_up,
    decay_bias,
    head_gain,
    window_query_weight,
    window_key_weight,
    window_value_weight,
    sink_logit,
    gla_output_weight,
    window_output_weight,
):
    fs, tp, sp = (lax.axis_size(n) for n in ("fs", "tp", "sp"))
    low = decay_down.T
    own = tokens.shape[1]
    rows = own * tp
    kc = decay_down.shape[0]
    width = VALUE_DIM + 4 * HEAD_DIM + 2 * KEY_DIM
    rank = low.shape[0]
    depth = (gla_output_weight.shape[0] + window_output_weight.shape[0]) // fs
    nc = gla_output_weight.shape[1]
    flat = nc % 128 == 0
    operands = (
        tokens[0],
        gla_value_weight,
        window_query_weight,
        gla_query_weight,
        gla_key_weight,
        window_key_weight,
        window_value_weight,
        low,
        gla_output_weight,
        window_output_weight,
        norm_gain[None],
        decay_up,
        decay_bias[None],
        head_gain[None],
        sink_logit[None],
    )
    if folds(sp, fs, tp, tokens.shape, rows, kc, width, rank, nc, depth):
        return fold_call((sp, fs, tp), operands).reshape(1, own, sp * nc)
    vm = pltpu.VMEM
    dma = pltpu.SemaphoreType.DMA
    scratch = [
        vm((fs * rows, tokens.shape[2]), BF),
        vm((sp * kc, width), BF),
        vm((sp, rank, kc), BF),
        vm((sp, depth, nc), BF),
        vm((fs, rows, width + 128), BF),
        vm((fs, WINDOW, 2 * HEAD_DIM), BF),
        vm((fs, WINDOW, 2 * HEAD_DIM), BF),
        vm((fs // 2, VALUE_DIM + 16, 2 * KEY_DIM), BF),
        vm((sp, fs // 2, VALUE_DIM + 16, 2 * KEY_DIM), BF),
        vm((fs, rows, VALUE_DIM), F32),
        vm((fs, rows, KEY_DIM), BF),
        vm((fs, rows, depth), BF),
        vm((sp, fs, own, nc), BF),
        vm((sp, fs, own, nc), BF),
        vm((sp, fs, own, nc), F32),
        vm((sp, fs - 1, own, nc), BF),
        vm((sp, fs - 1, own, nc), BF),
        vm((sp, own, nc), F32),
        dma((6,)),
        dma((fs * tp - 1,)),
        dma((fs * tp - 1,)),
        dma((2, sp)),
        dma((sp,)),
        dma((2, sp)),
        dma((sp,)),
        dma((2, sp)),
        dma((sp,)),
        dma((sp,)),
        dma((sp,)),
        dma((sp,)),
        dma((sp,)),
        dma((2, sp)),
        dma((sp,)),
        dma((2,)),
        dma((sp,)),
        dma((sp,)),
        dma((sp,)),
        dma((sp,)),
        dma((sp, fs - 1)),
        dma((sp, fs - 1)),
    ]
    spec = pl.BlockSpec(memory_space=pltpu.VMEM)
    anywhere = pl.BlockSpec(memory_space=pl.ANY)
    mixed = pl.pallas_call(
        functools.partial(mixer_kernel, (sp, fs, tp)),
        out_shape=jax.ShapeDtypeStruct((own, sp * nc) if flat else (sp, own, nc), BF),
        in_specs=[
            anywhere if i in (1, 2, 8, 9) else spec for i in range(15)
        ],
        out_specs=spec,
        scratch_shapes=scratch,
        compiler_params=pltpu.CompilerParams(
            has_side_effects=True, vmem_limit_bytes=60 * 1024 * 1024
        ),
    )(*operands)
    return (mixed if flat else mixed.transpose(1, 0, 2)).reshape(1, own, sp * nc)


def solution(mesh):
    in_specs = (
        P("fs", ("sp", "tp"), None),
        P(),
        P("sp", "tp"),
        P("sp", "tp"),
        P("sp", "tp"),
        P("sp", None),
        P(None, "tp"),
        P("tp"),
        P(),
        P("sp", "tp"),
        P("sp", "tp"),
        P("sp", "tp"),
        P("tp"),
        P("tp", "sp"),
        P("tp", "sp"),
    )
    out_specs = P("fs", ("sp", "tp"), None)
    return jax.shard_map(
        per_device, mesh=mesh, in_specs=in_specs, out_specs=out_specs, check_vma=False
    )
```

```python
import functools

import jax
import jax.numpy as jnp
from jax import lax
from jax.experimental import pallas as pl
from jax.experimental.pallas import tpu as pltpu
from jax.sharding import PartitionSpec as P

KEY_DIM = 64
VALUE_DIM = 128
SWA_HEADS = 16
KV_HEADS = 4
HEAD_DIM = 64
WINDOW = 128
SPAN = 64

EPS = 1e-06
SOFTMAX_TEMPER = 16.0
BF = jnp.bfloat16
F32 = jnp.float32


def rms_rows(values, gain):
    mean_square = jnp.mean(values * values, axis=-1, keepdims=True)
    return values * lax.rsqrt(mean_square + EPS) * gain


def nt(a, b):
    return lax.dot_general(a, b, (((1,), (1,)), ((), ())), preferred_element_type=F32)


def nn(a, b):
    return lax.dot_general(a, b, (((1,), (0,)), ((), ())), preferred_element_type=F32)


def tn(a, b):
    return lax.dot_general(a, b, (((0,), (0,)), ((), ())), preferred_element_type=F32)


def exact(a, b):
    return lax.dot_general(
        a, b, (((1,), (0,)), ((), ())), precision=lax.Precision.HIGHEST, preferred_element_type=F32
    )


def mixer_kernel(
    sizes,
    tok_ref,
    gv_ref,
    wq_ref,
    gq_ref,
    gk_ref,
    wk_ref,
    wv_ref,
    low_ref,
    go_ref,
    wo_ref,
    ngain_ref,
    up_ref,
    bias_ref,
    hgain_ref,
    sink_ref,
    out_ref,
    x_buf,
    w_buf,
    l_buf,
    o_buf,
    proj,
    edge_out,
    edge_in,
    state_out,
    state_in,
    local_out,
    q_far,
    hidden,
    half_out,
    half_in,
    half_own,
    piece_out,
    piece_in,
    piece_own,
    local_sem,
    tok_send,
    tok_recv,
    w_send,
    w_recv,
    l_send,
    l_recv,
    v_send,
    v_recv,
    vp_send,
    vp_recv,
    lp_send,
    lp_recv,
    o_send,
    o_recv,
    edge_sem,
    state_send,
    state_recv,
    half_send,
    half_recv,
    piece_send,
    piece_recv,
):
    sp, fs, tp = sizes
    me = lax.axis_index("sp")
    f = lax.axis_index("fs")
    c = lax.axis_index("tp")
    plane = fs * tp
    mine = f * tp + c
    own = tok_ref.shape[0]
    rows = own * tp
    kc = gv_ref.shape[0]
    MESH = pl.DeviceIdType.MESH

    def remote(src, dst, ssem, rsem, target):
        return pltpu.make_async_remote_copy(
            src_ref=src, dst_ref=dst, send_sem=ssem, recv_sem=rsem,
            device_id=target, device_id_type=MESH,
        )

    def w_rows(s):
        return w_buf.at[pl.ds(pl.multiple_of(s * kc, kc), kc)]

    def w_copy(s, way, first):
        target = {"sp": me + (1 if way == 0 else -1)}
        return remote(
            w_main(s), w_main(s), w_send.at[way, s], w_recv.at[s], target
        )

    side = f % 2
    part = kc // 2
    lpart = low_ref.shape[0] // 2

    def w_main(s):
        return w_rows(s).at[:, : starts[4]]

    def v_rows(s, h):
        at = pl.multiple_of(s * kc + h * part, part)
        return w_buf.at[pl.ds(at, part), starts[4] : starts[4] + 2 * HEAD_DIM]

    def l_rows(s, h):
        return l_buf.at[s, pl.ds(pl.multiple_of(h * lpart, lpart), lpart)]

    def v_copy(s, way):
        target = {"sp": me + (1 if way == 0 else -1)}
        return remote(v_rows(s, side), v_rows(s, side), v_send.at[way, s], v_recv.at[s], target)

    def lh_copy(s, way):
        target = {"sp": me + (1 if way == 0 else -1)}
        return remote(l_rows(s, side), l_rows(s, side), l_send.at[way, s], l_recv.at[s], target)

    def pair_copies(s, h):
        target = {"fs": f + 1 - 2 * side}
        return (
            remote(v_rows(s, h), v_rows(s, h), vp_send.at[s], vp_recv.at[s], target),
            remote(l_rows(s, h), l_rows(s, h), lp_send.at[s], lp_recv.at[s], target),
        )

    class l_copy:
        def __init__(self, s, way, first):
            self.s = s
            self.both = (v_copy(s, way), lh_copy(s, way))

        def start(self):
            for copy in self.both:
                copy.start()

        def wait_recv(self):
            for copy, onward in zip(self.both, pair_copies(self.s, side)):
                copy.wait_recv()
                onward.start()

        def wait_send(self):
            for copy in self.both:
                copy.wait_send()

    def o_copy(s, way, first):
        target = {"sp": me + (1 if way == 0 else -1)}
        return remote(
            o_buf.at[s], o_buf.at[s], o_send.at[way, s], o_recv.at[s], target
        )

    def tok_rows(i):
        return x_buf.at[pl.ds(pl.multiple_of(i * own, own), own)]

    def tok_copy(d, peer, sender):
        return remote(
            tok_ref, tok_rows(sender), tok_send.at[d - 1], tok_recv.at[d - 1],
            {"fs": peer // tp, "tp": peer % tp},
        )

    def pick(ref, width, which):
        value = ref[:, :width]
        for i in range(1, ref.shape[1] // width):
            value = jnp.where(which == i, ref[:, i * width : (i + 1) * width], value)
        return value

    def lanes(ref, width):
        return ref.at[:, pl.ds(pl.multiple_of(f * width, width), width)]

    def depth(ref, width):
        return ref.at[pl.ds(pl.multiple_of(f * width, width), width)]

    cols = [VALUE_DIM, 2 * HEAD_DIM, KEY_DIM, KEY_DIM, HEAD_DIM, HEAD_DIM]
    starts = [sum(cols[:i]) for i in range(len(cols))]
    gd = go_ref.shape[0] // fs
    wd = wo_ref.shape[0] // fs
    heads = sink_ref.shape[1] // fs
    copies_in = [
        (lanes(gv_ref, cols[0]), w_rows(me).at[:, : cols[0]]),
        (lanes(wq_ref, cols[1]), w_rows(me).at[:, starts[1] : starts[2]]),
        (depth(go_ref, gd), o_buf.at[me, pl.ds(0, gd)]),
        (depth(wo_ref, wd), o_buf.at[me, pl.ds(gd, wd)]),
        (low_ref, l_buf.at[me]),
        (tok_ref, tok_rows(mine)),
    ]
    locals_ = [
        pltpu.make_async_copy(a, b, local_sem.at[i]) for i, (a, b) in enumerate(copies_in)
    ]
    for copy in locals_:
        copy.start()
    for d in range(1, plane):
        tok_copy(d, lax.rem(mine + d, plane), mine).start()
    own_rows = pl.ds(pl.multiple_of(me * kc, kc), kc)
    kv = (f * heads) // (SWA_HEADS // KV_HEADS)
    w_buf[own_rows, starts[2] : starts[4]] = jnp.concatenate(
        [pick(gq_ref, KEY_DIM, f), pick(gk_ref, KEY_DIM, f)], 1
    )
    w_buf[own_rows, starts[4] :] = jnp.concatenate(
        [pick(wk_ref, HEAD_DIM, kv), pick(wv_ref, HEAD_DIM, kv)], 1
    )
    for copy in locals_[:5]:
        copy.wait()

    def sends(k):
        @pl.when((me - k >= 0) & (me + 1 < sp))
        def _():
            l_copy(me - k, 0, k == 0).start()
            w_copy(me - k, 0, k == 0).start()

        @pl.when((me + k < sp) & (me >= 1))
        def _():
            l_copy(me + k, 1, k == 0).start()
            w_copy(me + k, 1, k == 0).start()

        @pl.when((me == k) & (me + 1 < sp))
        def _():
            o_copy(me, 0, True).start()

        @pl.when((sp - 1 - me == k) & (me >= 1))
        def _():
            o_copy(me, 1, True).start()

    for k in range(sp - 1):
        sends(k)

        @pl.when(me - 1 - k >= 0)
        def _():
            l_copy(me - 1 - k, 0, False).wait_recv()
            w_copy(me - 1 - k, 0, False).wait_recv()

        @pl.when(me + 1 + k < sp)
        def _():
            l_copy(me + 1 + k, 1, False).wait_recv()
            w_copy(me + 1 + k, 1, False).wait_recv()

    inner = (me >= 1) & (me + 1 < sp)
    for k in range(1, sp - 1):
        @pl.when(inner & (me - k >= 0))
        def _():
            o_copy(me - k, 0, False).wait_recv()
            o_copy(me - k, 0, False).start()

        @pl.when(inner & (me + k < sp))
        def _():
            o_copy(me + k, 1, False).wait_recv()
            o_copy(me + k, 1, False).start()

    for copy in locals_[5:]:
        copy.wait()
    for i in range(sp):
        @pl.when(i != me)
        def _():
            for copy in pair_copies(i, 1 - side):
                copy.wait_recv()

    for d in range(1, plane):
        tok_copy(d, mine, lax.rem(mine + plane - d, plane)).wait_recv()


    def project(b, _):
        x = x_buf[pl.ds(pl.multiple_of(b * rows, rows), rows)].astype(F32)
        normed = rms_rows(x, ngain_ref[...]).astype(BF)
        p = nn(normed, w_buf[...]).astype(BF)
        proj[b, :, : p.shape[1]] = p
        edge_out[b] = p[rows - WINDOW :, starts[4] : starts[4] + 2 * HEAD_DIM]
        low = nt(normed[:, :kc], l_buf[0])
        for s in range(1, sp):
            low += nt(normed[:, s * kc : (s + 1) * kc], l_buf[s])
        proj[b, :, p.shape[1] : p.shape[1] + low.shape[1]] = low.astype(BF)
        return 0

    lax.fori_loop(0, fs, project, 0)
    edge = remote(edge_out, edge_in, edge_sem.at[0], edge_sem.at[1], {"sp": me + 1})

    @pl.when(me + 1 < sp)
    def _():
        edge.start()

    @pl.when(me == 0)
    def _():
        edge_in[...] = jnp.zeros_like(edge_in)

    nb = rows // SPAN
    low_at = sum(cols)
    lower = (
        lax.broadcasted_iota(jnp.int32, (SPAN, SPAN), 0)
        >= lax.broadcasted_iota(jnp.int32, (SPAN, SPAN), 1)
    )
    tri = lower.astype(F32)
    up = pick(up_ref, KEY_DIM, f)
    bias = pick(bias_ref, KEY_DIM, f)
    sinks = pick(sink_ref, heads, f)
    for b in range(fs):
        low = proj[b, :, low_at : low_at + up_ref.shape[0]]
        z = nn(low, up) + bias
        rate = (jnp.minimum(z, 0.0) - jnp.log1p(jnp.exp(-jnp.abs(z)))) / SOFTMAX_TEMPER
        state = None
        before = jnp.zeros((1, KEY_DIM), F32)
        for n in range(nb):
            r0 = n * SPAN
            within = exact(tri, rate[r0 : r0 + SPAN])
            total = within[SPAN - 1 :]
            v = proj[b, r0 : r0 + SPAN, starts[0] : starts[0] + VALUE_DIM]
            q = proj[b, r0 : r0 + SPAN, starts[2] : starts[2] + KEY_DIM].astype(F32)
            k = proj[b, r0 : r0 + SPAN, starts[3] : starts[3] + KEY_DIM].astype(F32)
            q_dec = q * KEY_DIM**-0.5 * jnp.exp(within)
            k_dec = (k * jnp.exp(-within)).astype(BF)
            k_end = (k * jnp.exp(total - within)).astype(BF)
            scores = jnp.where(lower, nt(q_dec.astype(BF), k_dec), 0.0)
            o = nn(scores.astype(BF), v)
            if state is not None:
                o += nt(q_dec.astype(BF), state.astype(BF))
            local_out[b, r0 : r0 + SPAN] = o
            q_far[b, r0 : r0 + SPAN] = (q_dec * jnp.exp(before)).astype(BF)
            update = tn(v, k_end)
            state = update if state is None else jnp.exp(total) * state + update
            before = before + total
        half = (b % 2) * KEY_DIM
        state_out[b // 2, :VALUE_DIM, half : half + KEY_DIM] = state.astype(BF)
        state_out[b // 2, VALUE_DIM:, half : half + KEY_DIM] = jnp.broadcast_to(
            jnp.exp(before), (16, KEY_DIM)
        ).astype(BF)

    def state_copy(d, sender):
        return remote(
            state_out, state_in.at[sender], state_send.at[d - 1], state_recv.at[sender],
            {"sp": me + d},
        )

    for d in range(1, sp):
        @pl.when(me + d < sp)
        def _():
            state_copy(d, me).start()

    @pl.when(me >= 1)
    def _():
        edge.wait_recv()

    qi = lax.broadcasted_iota(jnp.int32, (WINDOW, 2 * WINDOW), 0)
    ki = lax.broadcasted_iota(jnp.int32, (WINDOW, 2 * WINDOW), 1)
    distance = qi + WINDOW - ki
    inside = (distance >= 0) & (distance < WINDOW)
    for b in range(fs):
        for w in range(rows // WINDOW):
            r0 = w * WINDOW
            here = proj[b, r0 : r0 + WINDOW, starts[4] : starts[4] + 2 * HEAD_DIM]
            if w == 0:
                past = edge_in[b]
                valid = inside & ((ki >= WINDOW) | (me >= 1))
            else:
                past = proj[b, r0 - WINDOW : r0, starts[4] : starts[4] + 2 * HEAD_DIM]
                valid = inside
            band = jnp.concatenate([past, here], 0)
            bk = band[:, :HEAD_DIM]
            bv = band[:, HEAD_DIM:]
            for h in range(heads):
                q0 = starts[1] + h * HEAD_DIM
                q = proj[b, r0 : r0 + WINDOW, q0 : q0 + HEAD_DIM]
                s = jnp.where(valid, nt(q, bk) * HEAD_DIM**-0.5, -1e30)
                sink = sinks[:, h : h + 1]
                top = jnp.maximum(jnp.max(s, -1, keepdims=True), sink)
                e = jnp.exp(s - top)
                den = jnp.sum(e, -1, keepdims=True) + jnp.exp(sink - top)
                a = nn((e / den).astype(BF), bv).astype(BF)
                h0 = VALUE_DIM + h * HEAD_DIM
                hidden[b, r0 : r0 + WINDOW, h0 : h0 + HEAD_DIM] = a

    for i in range(sp - 1):
        @pl.when(i < me)
        def _():
            state_copy(1, i).wait_recv()

        @pl.when(i >= me)
        def _():
            state_in[i] = jnp.zeros(state_in.shape[1:], BF)

    for b in range(fs):
        half = (b % 2) * KEY_DIM
        incoming = jnp.zeros((VALUE_DIM, KEY_DIM), F32)
        for i in range(sp - 1):
            got = state_in[i, b // 2, :VALUE_DIM, half : half + KEY_DIM].astype(F32)
            kept = state_in[i, b // 2, VALUE_DIM : VALUE_DIM + 1, half : half + KEY_DIM].astype(F32)
            incoming = jnp.where(i < me, kept * incoming + got, incoming)
        o = local_out[b] + nt(q_far[b], incoming.astype(BF))
        hidden[b, :, :VALUE_DIM] = rms_rows(o, hgain_ref[...]).astype(BF)

    forward = 2 * me < sp
    nc = o_buf.shape[2]

    def chunk(t):
        return lax.rem(jnp.where(forward, me + t, me - t) + sp, sp)

    def half_copy(s):
        return remote(half_out.at[s], half_in.at[s], half_send.at[s], half_recv.at[s], {"tp": 1 - c})

    def piece_copy(s, d, target):
        return remote(
            piece_out.at[s, d - 1], piece_in.at[s, d - 1],
            piece_send.at[s, d - 1], piece_recv.at[s, d - 1], {"fs": target},
        )

    def produce(t):
        s = chunk(t)

        @pl.when(jnp.logical_not(inner) & (t > 0))
        def _():
            o_copy(s, 0, False).wait_recv()

        w = o_buf[s]
        for b in range(fs):
            part = nn(hidden[b], w)
            lo, hi = part[:own], part[own:]
            half_out[s, b] = jnp.where(c == 0, hi, lo).astype(BF)
            half_own[s, b] = jnp.where(c == 0, lo, hi)
        half_copy(s).start()

    def combine(t):
        s = chunk(t)
        half_copy(s).wait_recv()
        for d in range(1, fs):
            to = lax.rem(f + d, fs)
            piece_out[s, d - 1] = (half_own[s, to] + half_in[s, to].astype(F32)).astype(BF)
            piece_copy(s, d, to).start()
        piece_own[s] = half_own[s, f] + half_in[s, f].astype(F32)

    def finish(t):
        s = chunk(t)
        total = piece_own[s]
        for d in range(1, fs):
            piece_copy(s, d, f).wait_recv()
            total += piece_in[s, d - 1].astype(F32)
        if len(out_ref.shape) == 2:
            out_ref[:, pl.ds(pl.multiple_of(s * nc, nc), nc)] = total.astype(BF)
        else:
            out_ref[s] = total.astype(BF)

    produce(0)

    def steady(t, _):
        produce(t)
        combine(t - 1)
        return 0

    lax.fori_loop(1, sp, steady, 0)
    combine(sp - 1)

    def close(t, _):
        finish(t)
        s = chunk(t)
        half_copy(s).wait_send()
        for d in range(1, fs):
            piece_copy(s, d, f).wait_send()
        return 0

    lax.fori_loop(0, sp, close, 0)

    for k in range(sp - 1):
        @pl.when((me - k >= 0) & (me + 1 < sp))
        def _():
            l_copy(me - k, 0, False).wait_send()
            w_copy(me - k, 0, False).wait_send()
            o_copy(me - k, 0, False).wait_send()

        @pl.when((me + k < sp) & (me >= 1))
        def _():
            l_copy(me + k, 1, False).wait_send()
            w_copy(me + k, 1, False).wait_send()
            o_copy(me + k, 1, False).wait_send()

    for i in range(sp):
        @pl.when(i != me)
        def _():
            for copy in pair_copies(i, side):
                copy.wait_send()

    for d in range(1, plane):
        tok_copy(d, mine, mine).wait_send()

    @pl.when(me + 1 < sp)
    def _():
        edge.wait_send()

    for d in range(1, sp):
        @pl.when(me + d < sp)
        def _():
            state_copy(d, me).wait_send()


def roll_half(a):
    return jnp.concatenate([a[:, a.shape[1] // 2 :], a[:, : a.shape[1] // 2]], 1)


def fold_kernel(
    sizes,
    tok_in,
    gv_ref,
    wq_ref,
    gq_ref,
    gk_ref,
    wk_ref,
    wv_ref,
    low_ref,
    go_ref,
    wo_ref,
    ngain_in,
    up_in,
    bias_in,
    hgain_in,
    sink_in,
    out_hbm,
    tok_ref,
    ngain_ref,
    up_ref,
    bias_ref,
    hgain_ref,
    sink_ref,
    out_ref,
    x_buf,
    ww,
    wg,
    wl,
    o_buf,
    tiles,
    qw,
    kvb,
    gvb,
    qkb,
    acc,
    lowx,
    decays,
    totals,
    states,
    state_out,
    state_in,
    local_out,
    q_far,
    hidden,
    half_out,
    half_in,
    half_own,
    piece_out,
    piece_in,
    piece_own,
    local_sem,
    out_sem,
    l_send,
    l_recv,
    x_send,
    x_recv,
    w_send,
    w_recv,
    p_send,
    p_recv,
    o_send,
    o_recv,
    edge_sem,
    state_sem,
    hid_send,
    hid_recv,
    half_send,
    half_recv,
    piece_send,
    piece_recv,
):
    sp, fs, tp = sizes
    me = lax.axis_index("sp")
    f = lax.axis_index("fs")
    c = lax.axis_index("tp")
    own = tok_in.shape[0]
    rows = own * tp
    kc = gv_ref.shape[0]
    part = kc // 2
    lpart = low_ref.shape[0] // 2
    MESH = pl.DeviceIdType.MESH
    pair = 2 * KEY_DIM
    wide = VALUE_DIM + pair

    slot = lax.rem(me, 2)
    far_slot = 1 - slot
    inner = (me >= 1) & (me + 1 < sp)
    outer = jnp.logical_not(inner)
    middle = 1 + slot
    outside = (sp - 1) * (me - 1)
    buddy = me + 1 - 2 * slot
    third = 2 - me // 2
    fourth = third + 1 - 2 * lax.rem(third, 2)
    chunks = [me, buddy, third, fourth]
    side = lax.rem(f, 2)
    xn = f + 1 - 2 * side
    yn = lax.rem(f + 2, fs)
    n1 = xn * (1 - c) + yn * c
    n2 = xn * c + yn * (1 - c)

    def remote(src, dst, ssem, rsem, target):
        return pltpu.make_async_remote_copy(
            src_ref=src, dst_ref=dst, send_sem=ssem, recv_sem=rsem,
            device_id=target, device_id_type=MESH,
        )

    barrier = pltpu.get_barrier_semaphore()

    def greet(target):
        pl.semaphore_signal(barrier, inc=1, device_id=target, device_id_type=MESH)

    greet({"tp": 1 - c})
    for d in range(1, fs):
        greet({"fs": lax.rem(f + d, fs)})

    @pl.when(me + 1 < sp)
    def _():
        greet({"sp": me + 1})

    @pl.when(me >= 1)
    def _():
        greet({"sp": me - 1})

    def lanes(ref, at, width):
        return ref.at[:, pl.ds(pl.multiple_of(at * width, width), width)]

    def depth(ref, width):
        return ref.at[pl.ds(pl.multiple_of(f * width, width), width)]

    def slice_rows(ref, s):
        return ref.at[pl.ds(pl.multiple_of(s * kc, kc), kc)]

    gd = go_ref.shape[0] // fs
    wd = wo_ref.shape[0] // fs
    heads = sink_in.shape[1] // fs
    wq_cols = heads * HEAD_DIM
    kv = (f * heads) // (SWA_HEADS // KV_HEADS)
    copies_in = [
        (lanes(gq_ref, f // 2, pair), tiles.at[0]),
        (lanes(gk_ref, f // 2, pair), tiles.at[1]),
        (wk_ref, tiles.at[2]),
        (wv_ref, tiles.at[3]),
        (lanes(wq_ref, f, wq_cols), slice_rows(ww, me).at[:, :wq_cols]),
        (lanes(gv_ref, f, VALUE_DIM), slice_rows(wg, me).at[:, :VALUE_DIM]),
        (low_ref, wl.at[me]),
    ]
    nc = o_buf.shape[3]
    for h in range(2):
        cut = pl.ds(h * nc, nc)
        copies_in += [
            (depth(go_ref, gd).at[:, cut], o_buf.at[me, h, pl.ds(0, gd)]),
            (depth(wo_ref, wd).at[:, cut], o_buf.at[me, h, pl.ds(gd, wd)]),
        ]
    copies_in += [
        (ngain_in, ngain_ref),
        (tok_in, tok_ref),
        (up_in, up_ref),
        (bias_in, bias_ref),
        (hgain_in, hgain_ref),
        (sink_in, sink_ref),
    ]
    locals_ = [
        pltpu.make_async_copy(a, b, local_sem.at[i]) for i, (a, b) in enumerate(copies_in)
    ]
    for copy in locals_[11:] + locals_[:11]:
        copy.start()

    def block(s, i):
        return x_buf.at[s, pl.ds(pl.multiple_of(i * own, own), own)]

    mine = f * tp + c
    b1, b2, b3 = n1 * tp + c, n2 * tp + c, (fs - 1 - f) * tp + c

    for copy in locals_[11:]:
        copy.wait()
    normed = rms_rows(tok_ref[...].astype(F32), ngain_ref[...]).astype(BF)
    x_buf[slot, pl.ds(pl.multiple_of(mine * own, own), own)] = normed

    def x_copy(s, i, k, target):
        return remote(block(s, i), block(s, i), x_send.at[s, k], x_recv.at[s, i], target)

    SIB = {"tp": 1 - c}

    def x_first(s):
        return [
            x_copy(s, mine, 0, {"fs": n1}),
            x_copy(s, mine, 1, {"fs": n2}),
            x_copy(s, mine, 2, SIB),
        ]

    def x_from1(s):
        return [x_copy(s, b1, 3, {"fs": n2}), x_copy(s, b1, 4, SIB)]

    def x_from2(s):
        return [x_copy(s, b2, 5, SIB)]

    def x_from3(s):
        return [x_copy(s, b3, 6, SIB)]

    def x_all(s):
        return x_first(s) + x_from1(s) + x_from2(s) + x_from3(s)

    def x_out():
        return x_copy(slot, mine, 0, {"sp": middle})

    def kv_rows(s, h):
        at = pl.multiple_of(s * kc + h * part, part)
        return ww.at[pl.ds(at, part), wq_cols:]

    def low_rows(s, h):
        return wl.at[s, pl.ds(pl.multiple_of(h * lpart, lpart), lpart)]

    def w_copy(kind, s):
        ref = (
            lambda: slice_rows(ww, s).at[:, :wq_cols],
            lambda: kv_rows(s, side),
            lambda: low_rows(s, c),
            lambda: slice_rows(wg, s),
        )[kind]()
        return remote(ref, ref, w_send.at[kind, s], w_recv.at[kind, s], {"sp": middle})

    def kv_share(s, h):
        return remote(
            kv_rows(s, h), kv_rows(s, h), p_send.at[0, s], p_recv.at[0, s], {"fs": xn}
        )

    def low_share(s, h):
        return remote(low_rows(s, h), low_rows(s, h), p_send.at[1, s], p_recv.at[1, s], SIB)

    def o_copy(way, s, h):
        target = {"sp": middle if way == 0 else outside}
        return remote(
            o_buf.at[s, h], o_buf.at[s, h], o_send.at[way, s, h], o_recv.at[s, h], target
        )

    def l_copy(i, k, target):
        return remote(lowx.at[i], lowx.at[i], l_send.at[k], l_recv.at[i], target)

    def l_first():
        peers = [{"fs": n1}, {"fs": n2}, {"fs": fs - 1 - f}, SIB]
        return [l_copy(mine, k, peer) for k, peer in enumerate(peers)]

    def l_onward():
        return [l_copy(i, 4 + k, SIB) for k, i in enumerate((b1, b2, b3))]

    def start(copies):
        for copy in copies:
            copy.start()

    pl.semaphore_wait(barrier, fs + jnp.where(inner, 2, 1))

    LOW, KV, QUERY, STATE = 2, 1, 0, 3
    locals_[6].wait()
    w_copy(LOW, me).start()

    @pl.when(outer)
    def _():
        x_out().start()

    @pl.when(inner)
    def _():
        start(x_first(slot))

    for copy in locals_[:6]:
        copy.wait()
    own_rows = pl.ds(pl.multiple_of(me * kc, kc), kc)

    def half_of(i, width, which):
        return jnp.where(which == 0, tiles[i, :, :width], tiles[i, :, width:])

    ww[own_rows, wq_cols:] = jnp.concatenate(
        [half_of(2, HEAD_DIM, kv), half_of(3, HEAD_DIM, kv)], 1
    )
    w_copy(KV, me).start()
    w_copy(QUERY, me).start()
    wg[own_rows, VALUE_DIM:] = jnp.concatenate(
        [half_of(0, KEY_DIM, side), half_of(1, KEY_DIM, side)], 1
    )
    for copy in locals_[7:11]:
        copy.wait()

    @pl.when(outer)
    def _():
        w_copy(STATE, me).start()
        for h in range(2):
            o_copy(0, me, h).start()

    lane = lax.broadcasted_iota(jnp.int32, (rows, pair), 1)
    row = lax.broadcasted_iota(jnp.int32, (rows, pair), 0)
    left = lane < KEY_DIM
    early = row < SPAN
    same = (row < SPAN) == (lane < SPAN)
    diagonal = same & (row >= lane)
    below = (row >= SPAN) & (lane < SPAN)

    edge = remote(kvb.at[2], kvb.at[0], edge_sem.at[0], edge_sem.at[1], {"sp": me + 1})
    state = remote(state_out, state_in, state_sem.at[0], state_sem.at[1], {"sp": me + 1})

    def hid_part(s, i):
        return hidden.at[s, :, i * VALUE_DIM : (i + 1) * VALUE_DIM]

    def hid_copy(i, s):
        return remote(
            hid_part(s, i), hid_part(s, i), hid_send.at[i], hid_recv.at[i], {"sp": outside}
        )

    def seq(b):
        if isinstance(b, int):
            return pl.ds(b * rows, rows)
        return pl.ds(pl.multiple_of(b * rows, rows), rows)

    @pl.when(inner)
    def _():
        for h in range(2):
            o_copy(1, me, h).start()

        def arrive(kind, s, onward):
            w_copy(kind, s).wait_recv()
            if onward:
                w_copy(kind, s).start()
            if kind == LOW:
                low_share(s, c).start()
            if kind == KV:
                kv_share(s, side).start()

        def neighbours(s):
            x_copy(s, b1, 0, SIB).wait_recv()
            start(x_from1(s))
            x_copy(s, b2, 0, SIB).wait_recv()
            start(x_from2(s))

        def corner(s):
            x_copy(s, b3, 0, SIB).wait_recv()
            start(x_from3(s))

        def siblings(s):
            for g in range(fs):
                x_copy(s, g * tp + 1 - c, 0, SIB).wait_recv()

        def columns(s):
            return pl.ds(pl.multiple_of(s * kc, kc), kc)

        bs = [bias_ref[:, i * KEY_DIM : (i + 1) * KEY_DIM] for i in range(fs)]
        ups = [up_ref[:, i * KEY_DIM : (i + 1) * KEY_DIM] for i in range(fs)]
        bias, up = bs[0], ups[0]
        for i in range(1, fs):
            bias = jnp.where(f == i, bs[i], bias)
            up = jnp.where(f == i, ups[i], up)
        up_l = jnp.concatenate([up, jnp.zeros_like(up)], 1)
        up_r = jnp.concatenate([jnp.zeros_like(up), up], 1)
        bias2 = jnp.concatenate([bias, bias], 1)

        def own_low():
            at = pl.ds(pl.multiple_of(mine * own, own), own)
            x = jnp.concatenate([x_buf[slot, at], x_buf[far_slot, at]], 0)
            low = nt(wl[0], x[:, :kc])
            for j in range(1, sp):
                low += nt(wl[j], x[:, j * kc : (j + 1) * kc])
            lowx[mine] = low.astype(BF)

        def gate(p):
            pre = []
            for i in range(tp):
                z = tn(lowx[2 * p * tp + i], up_l) + tn(lowx[(2 * p + 1) * tp + i], up_r)
                pre.append(z + bias2)
            return [
                jnp.concatenate([z[k * own : (k + 1) * own] for z in pre], 0) for k in range(2)
            ]

        def decay():
            tri = diagonal.astype(F32)
            for p in range(fs // 2):
                for s, z in zip((slot, far_slot), gate(p)):
                    decay_of(s, p, z, tri)

        def decay_of(s, p, z, tri):
            rate = (jnp.minimum(z, 0.0) - jnp.log1p(jnp.exp(-jnp.abs(z)))) / SOFTMAX_TEMPER
            within = exact(tri, rate)
            t0, t1 = within[SPAN - 1 : SPAN], within[rows - 1 :]
            grow = jnp.exp(within) * KEY_DIM**-0.5
            end = jnp.exp(jnp.where(early, t0, t1) - within)
            decays[s, p, 0] = grow
            decays[s, p, 1] = jnp.exp(-within)
            decays[s, p, 2] = end
            decays[s, p, 3] = grow * jnp.where(early, 1.0, jnp.exp(t0))
            decays[s, p, 4] = end * jnp.where(early, jnp.exp(t1), 1.0)
            totals[s, p] = jnp.broadcast_to(jnp.exp(t0 + t1), totals.shape[2:])

        def window_maps(s, slices):
            total = nn(x_buf[s, :, columns(slices[0])], slice_rows(ww, slices[0])[...])
            for j in slices[1:]:
                total += nn(x_buf[s, :, columns(j)], slice_rows(ww, j)[...])
            return total

        arrive(LOW, buddy, True)
        w_copy(STATE, me).start()
        arrive(LOW, third, False)
        arrive(LOW, fourth, False)
        x_copy(far_slot, mine, 0, SIB).wait_recv()
        start(x_first(far_slot))
        for s in chunks[1:]:
            low_share(s, 1 - c).wait_recv()
        own_low()
        start(l_first())
        arrive(KV, third, False)
        neighbours(slot)
        arrive(KV, buddy, True)
        arrive(QUERY, buddy, True)
        for i in (b1, b2, b3):
            l_copy(i, 0, SIB).wait_recv()
        start(l_onward())
        neighbours(far_slot)
        corner(slot)
        for g in range(fs):
            l_copy(g * tp + 1 - c, 0, SIB).wait_recv()
        decay()
        arrive(STATE, buddy, True)
        o_copy(0, me, 0).start()
        arrive(KV, fourth, False)
        siblings(slot)
        arrive(QUERY, third, False)
        for s in chunks[1:3]:
            kv_share(s, 1 - side).wait_recv()
        acc[slot] = window_maps(slot, chunks[:3])
        corner(far_slot)
        siblings(far_slot)
        acc[far_slot] = window_maps(far_slot, chunks[:3])
        arrive(QUERY, fourth, False)
        kv_share(fourth, 1 - side).wait_recv()

        def place(s):
            p = acc[s] + window_maps(s, chunks[3:])
            qw[s] = (p[:, :wq_cols].astype(BF).astype(F32) * HEAD_DIM**-0.5).astype(BF)
            kvb[s + 1] = p[:, wq_cols:].astype(BF)

        place(slot)
        place(far_slot)

        @pl.when(me == 1)
        def _():
            edge.start()
            kvb[0] = jnp.zeros(kvb.shape[1:], BF)
            state_in[...] = jnp.zeros_like(state_in)

        @pl.when(me > 1)
        def _():
            o_copy(0, me, 1).start()

        qi = lax.broadcasted_iota(jnp.int32, (WINDOW, 2 * WINDOW), 0)
        ki = lax.broadcasted_iota(jnp.int32, (WINDOW, 2 * WINDOW), 1)
        distance = qi + WINDOW - ki
        inside = (distance >= 0) & (distance < WINDOW)
        sinks = sink_ref[:, :heads]
        for i in range(1, fs):
            sinks = jnp.where(f == i, sink_ref[:, i * heads : (i + 1) * heads], sinks)

        def window(s):
            valid = inside & ((ki >= WINDOW) | (me > 1) | (s > 0))

            def one(b, _):
                band = jnp.concatenate([kvb[s, seq(b)], kvb[s + 1, seq(b)]], 0)
                q = qw[s, seq(b)].astype(F32)
                outs = []
                for h in range(heads):
                    qh = jnp.where(left, q if h == 0 else roll_half(q), 0.0).astype(BF)
                    sc = jnp.where(valid, nt(qh, band), -1e30)
                    sink = sinks[:, h : h + 1]
                    top = jnp.maximum(jnp.max(sc, -1, keepdims=True), sink)
                    e = jnp.exp(sc - top)
                    den = jnp.sum(e, -1, keepdims=True) + jnp.exp(sink - top)
                    outs.append(nn((e * (1.0 / den)).astype(BF), band))
                hidden[s, seq(b), VALUE_DIM:] = jnp.where(left, roll_half(outs[0]), outs[1]).astype(BF)
                return 0

            for b in range(fs):
                one(b, 0)

        window(far_slot)
        hid_copy(1, far_slot).start()
        w_copy(STATE, third).wait_recv()
        w_copy(STATE, fourth).wait_recv()

        for s in range(2):
            p = nn(x_buf[s], wg[...]).astype(BF)
            gvb[s] = p[:, :VALUE_DIM]
            qkb[s] = p[:, VALUE_DIM:].astype(F32)

        def keys(s, p):
            return jnp.where(left, roll_half(qkb[s, seq(2 * p)]), qkb[s, seq(2 * p + 1)])

        def queries(s, p):
            return jnp.where(left, qkb[s, seq(2 * p)], roll_half(qkb[s, seq(2 * p + 1)]))

        for s in range(2):
            for p in range(fs // 2):
                k_far = (keys(s, p) * decays[s, p, 4]).astype(BF)
                states[s, p] = jnp.where(
                    left, tn(gvb[s, seq(2 * p)], k_far), tn(gvb[s, seq(2 * p + 1)], k_far)
                )
        for p in range(fs // 2):
            state_out[p] = (totals[1, p, :1] * states[0, p] + states[1, p]).astype(BF)

        @pl.when(me == 1)
        def _():
            state.start()
            o_copy(0, me, 1).start()

        for h in range(2):
            o_copy(0, buddy, h).wait_recv()
            o_copy(0, buddy, h).start()

        for s in range(2):
            for p in range(fs // 2):
                k = keys(s, p)
                q = queries(s, p)
                qd = q * decays[s, p, 0]
                qf = q * decays[s, p, 3]
                kd = (k * decays[s, p, 1]).astype(BF)
                ke = (k * decays[s, p, 2]).astype(BF)
                for j in range(2):
                    here = left if j == 0 else jnp.logical_not(left)
                    qj = jnp.where(here, qd, 0.0).astype(BF)
                    scores = jnp.where(
                        diagonal, nt(qj, kd), jnp.where(below, nt(qj, ke), 0.0)
                    ).astype(BF)
                    local_out[s, seq(2 * p + j)] = nn(scores, gvb[s, seq(2 * p + j)])
                    q_far[s, seq(2 * p + j)] = jnp.where(here, qf, 0.0).astype(BF)

        @pl.when(me > 1)
        def _():
            state.wait_recv()

        def finish_state(s):
            for p in range(fs // 2):
                arrived = state_in[p].astype(F32)
                entering = jnp.where(s == 0, arrived, totals[0, p, :1] * arrived + states[0, p])
                entering = entering.astype(BF)
                for j in range(2):
                    b = 2 * p + j
                    o = local_out[s, seq(b)] + nt(q_far[s, seq(b)], entering)
                    hidden[s, seq(b), :VALUE_DIM] = rms_rows(o, hgain_ref[...]).astype(BF)

        finish_state(far_slot)
        hid_copy(0, far_slot).start()
        for h in range(2):
            o_copy(0, third, h).wait_recv()
            o_copy(1, third, h).start()
        finish_state(slot)

        @pl.when(me > 1)
        def _():
            edge.wait_recv()

        window(slot)

    @pl.when(outer)
    def _():
        hid_copy(1, slot).wait_recv()
        hid_copy(0, slot).wait_recv()

    parts = [(s, h) for s in chunks for h in range(2)]

    def half_copy(s, h):
        return remote(
            half_out.at[s, h], half_in.at[s, h], half_send.at[s, h], half_recv.at[s, h], SIB
        )

    def piece_copy(s, h, d, target):
        return remote(
            piece_out.at[s, h, d - 1], piece_in.at[s, h, d - 1],
            piece_send.at[s, h, d - 1], piece_recv.at[s, h, d - 1], {"fs": target},
        )

    def produce(t):
        s, h = parts[t]
        if 2 <= t < 6:
            @pl.when(outer)
            def _():
                o_copy(0, s, h).wait_recv()
        if t >= 6:
            o_copy(0, s, h).wait_recv()

            @pl.when(inner)
            def _():
                o_copy(1, s, h).start()

        w = o_buf[s, h]
        for b in range(fs):
            partial = nn(hidden[slot, seq(b)], w)
            lo, hi = partial[:own], partial[own:]
            half_out[s, h, b] = jnp.where(c == 0, hi, lo).astype(BF)
            half_own[s, h, b] = jnp.where(c == 0, lo, hi)
        half_copy(s, h).start()

    def combine(t):
        s, h = parts[t]
        half_copy(s, h).wait_recv()
        for d in range(1, fs):
            to = lax.rem(f + d, fs)
            piece_out[s, h, d - 1] = (half_own[s, h, to] + half_in[s, h, to].astype(F32)).astype(BF)
            piece_copy(s, h, d, to).start()
        piece_own[s, h] = half_own[s, h, f] + half_in[s, h, f].astype(F32)

    def finish(t):
        s, h = parts[t]
        total = piece_own[s, h]
        for d in range(1, fs):
            piece_copy(s, h, d, f).wait_recv()
            total += piece_in[s, h, d - 1].astype(F32)
        at = pl.ds(pl.multiple_of((2 * s + h) * nc, nc), nc)
        out_ref[:, at] = total.astype(BF)
        pltpu.make_async_copy(out_ref.at[:, at], out_hbm.at[:, at], out_sem.at[t]).start()

    produce(0)
    for t in range(1, 2 * sp):
        produce(t)
        combine(t - 1)
    combine(2 * sp - 1)
    for t in range(2 * sp):
        finish(t)
    for t, (s, h) in enumerate(parts):
        at = pl.ds(pl.multiple_of((2 * s + h) * nc, nc), nc)
        pltpu.make_async_copy(out_ref.at[:, at], out_hbm.at[:, at], out_sem.at[t]).wait()
        half_copy(s, h).wait_send()
        for d in range(1, fs):
            piece_copy(s, h, d, f).wait_send()

    for kind in range(4):
        w_copy(kind, me).wait_send()
    for h in range(2):
        o_copy(0, me, h).wait_send()

    @pl.when(outer)
    def _():
        x_out().wait_send()

    @pl.when(inner)
    def _():
        for s in range(2):
            for copy in x_all(s):
                copy.wait_send()
        for kind in range(4):
            w_copy(kind, buddy).wait_send()
        for copy in l_first() + l_onward():
            copy.wait_send()
        for s in chunks[1:]:
            kv_share(s, side).wait_send()
            low_share(s, c).wait_send()
        for h in range(2):
            o_copy(0, buddy, h).wait_send()
            for s in (me, third, fourth):
                o_copy(1, s, h).wait_send()
        for i in range(2):
            hid_copy(i, far_slot).wait_send()

        @pl.when(me == 1)
        def _():
            edge.wait_send()
            state.wait_send()


def fold_call(sizes, operands):
    sp, fs, tp = sizes
    own, d = operands[0].shape
    rows = own * tp
    kc = operands[1].shape[0]
    rank = operands[7].shape[0]
    depth = (operands[8].shape[0] + operands[9].shape[0]) // fs
    nc = operands[8].shape[1]
    pair = 2 * KEY_DIM
    all_rows = fs * rows
    pairs = fs // 2
    vm = pltpu.VMEM
    dma = pltpu.SemaphoreType.DMA
    small = [(o.shape, o.dtype) for o in operands[10:]]
    scratch = [
        vm((own, d), BF),
        *(vm(shape, dtype) for shape, dtype in small),
        vm((own, sp * nc), BF),
        vm((2, all_rows, d), BF),
        vm((d, 2 * pair), BF),
        vm((d, VALUE_DIM + pair), BF),
        vm((sp, rank, kc), BF),
        vm((sp, 2, depth, nc // 2), BF),
        vm((4, kc, pair), BF),
        vm((2, all_rows, pair), BF),
        vm((3, all_rows, pair), BF),
        vm((2, all_rows, VALUE_DIM), BF),
        vm((2, all_rows, pair), F32),
        vm((2, all_rows, 2 * pair), F32),
        vm((fs * tp, rank, 2 * own), BF),
        vm((2, pairs, 5, rows, pair), F32),
        vm((2, pairs, 8, pair), F32),
        vm((2, pairs, VALUE_DIM, pair), F32),
        vm((pairs, VALUE_DIM, pair), BF),
        vm((pairs, VALUE_DIM, pair), BF),
        vm((2, all_rows, VALUE_DIM), F32),
        vm((2, all_rows, pair), BF),
        vm((2, all_rows, depth), BF),
        vm((sp, 2, fs, own, nc // 2), BF),
        vm((sp, 2, fs, own, nc // 2), BF),
        vm((sp, 2, fs, own, nc // 2), F32),
        vm((sp, 2, fs - 1, own, nc // 2), BF),
        vm((sp, 2, fs - 1, own, nc // 2), BF),
        vm((sp, 2, own, nc // 2), F32),
        dma((17,)),
        dma((2 * sp,)),
        dma((7,)),
        dma((fs * tp,)),
        dma((2, 7)),
        dma((2, fs * tp)),
        dma((4, sp)),
        dma((4, sp)),
        dma((2, sp)),
        dma((2, sp)),
        dma((2, sp, 2)),
        dma((sp, 2)),
        dma((2,)),
        dma((2,)),
        dma((2,)),
        dma((2,)),
        dma((sp, 2)),
        dma((sp, 2)),
        dma((sp, 2, fs - 1)),
        dma((sp, 2, fs - 1)),
    ]
    anywhere = pl.BlockSpec(memory_space=pl.ANY)
    return pl.pallas_call(
        functools.partial(fold_kernel, sizes),
        out_shape=jax.ShapeDtypeStruct((own, sp * nc), BF),
        in_specs=[anywhere] * 15,
        out_specs=anywhere,
        scratch_shapes=scratch,
        compiler_params=pltpu.CompilerParams(
            has_side_effects=True, vmem_limit_bytes=60 * 1024 * 1024, collective_id=0
        ),
    )(*operands)


def folds(sp, fs, tp, shape, rows, kc, width, rank, nc, depth):
    whole_rows = rows == WINDOW == 2 * SPAN
    lanes_fit = nc % 256 == 0 and kc % 128 == 0 and depth == 2 * VALUE_DIM
    return sp == 4 and fs == 4 and tp == 2 and whole_rows and lanes_fit and rank % 32 == 0


def per_device(
    tokens,
    norm_gain,
    gla_query_weight,
    gla_key_weight,
    gla_value_weight,
    decay_down,
    decay_up,
    decay_bias,
    head_gain,
    window_query_weight,
    window_key_weight,
    window_value_weight,
    sink_logit,
    gla_output_weight,
    window_output_weight,
):
    fs, tp, sp = (lax.axis_size(n) for n in ("fs", "tp", "sp"))
    low = decay_down.T
    own = tokens.shape[1]
    rows = own * tp
    kc = decay_down.shape[0]
    width = VALUE_DIM + 4 * HEAD_DIM + 2 * KEY_DIM
    rank = low.shape[0]
    depth = (gla_output_weight.shape[0] + window_output_weight.shape[0]) // fs
    nc = gla_output_weight.shape[1]
    flat = nc % 128 == 0
    operands = (
        tokens[0],
        gla_value_weight,
        window_query_weight,
        gla_query_weight,
        gla_key_weight,
        window_key_weight,
        window_value_weight,
        low,
        gla_output_weight,
        window_output_weight,
        norm_gain[None],
        decay_up,
        decay_bias[None],
        head_gain[None],
        sink_logit[None],
    )
    if folds(sp, fs, tp, tokens.shape, rows, kc, width, rank, nc, depth):
        return fold_call((sp, fs, tp), operands).reshape(1, own, sp * nc)
    vm = pltpu.VMEM
    dma = pltpu.SemaphoreType.DMA
    scratch = [
        vm((fs * rows, tokens.shape[2]), BF),
        vm((sp * kc, width), BF),
        vm((sp, rank, kc), BF),
        vm((sp, depth, nc), BF),
        vm((fs, rows, width + 128), BF),
        vm((fs, WINDOW, 2 * HEAD_DIM), BF),
        vm((fs, WINDOW, 2 * HEAD_DIM), BF),
        vm((fs // 2, VALUE_DIM + 16, 2 * KEY_DIM), BF),
        vm((sp, fs // 2, VALUE_DIM + 16, 2 * KEY_DIM), BF),
        vm((fs, rows, VALUE_DIM), F32),
        vm((fs, rows, KEY_DIM), BF),
        vm((fs, rows, depth), BF),
        vm((sp, fs, own, nc), BF),
        vm((sp, fs, own, nc), BF),
        vm((sp, fs, own, nc), F32),
        vm((sp, fs - 1, own, nc), BF),
        vm((sp, fs - 1, own, nc), BF),
        vm((sp, own, nc), F32),
        dma((6,)),
        dma((fs * tp - 1,)),
        dma((fs * tp - 1,)),
        dma((2, sp)),
        dma((sp,)),
        dma((2, sp)),
        dma((sp,)),
        dma((2, sp)),
        dma((sp,)),
        dma((sp,)),
        dma((sp,)),
        dma((sp,)),
        dma((sp,)),
        dma((2, sp)),
        dma((sp,)),
        dma((2,)),
        dma((sp,)),
        dma((sp,)),
        dma((sp,)),
        dma((sp,)),
        dma((sp, fs - 1)),
        dma((sp, fs - 1)),
    ]
    spec = pl.BlockSpec(memory_space=pltpu.VMEM)
    anywhere = pl.BlockSpec(memory_space=pl.ANY)
    mixed = pl.pallas_call(
        functools.partial(mixer_kernel, (sp, fs, tp)),
        out_shape=jax.ShapeDtypeStruct((own, sp * nc) if flat else (sp, own, nc), BF),
        in_specs=[
            anywhere if i in (1, 2, 8, 9) else spec for i in range(15)
        ],
        out_specs=spec,
        scratch_shapes=scratch,
        compiler_params=pltpu.CompilerParams(
            has_side_effects=True, vmem_limit_bytes=60 * 1024 * 1024
        ),
    )(*operands)
    return (mixed if flat else mixed.transpose(1, 0, 2)).reshape(1, own, sp * nc)


def solution(mesh):
    in_specs = (
        P("fs", ("sp", "tp"), None),
        P(),
        P("sp", "tp"),
        P("sp", "tp"),
        P("sp", "tp"),
        P("sp", None),
        P(None, "tp"),
        P("tp"),
        P(),
        P("sp", "tp"),
        P("sp", "tp"),
        P("sp", "tp"),
        P("tp"),
        P("tp", "sp"),
        P("tp", "sp"),
    )
    out_specs = P("fs", ("sp", "tp"), None)
    return jax.shard_map(
        per_device, mesh=mesh, in_specs=in_specs, out_specs=out_specs, check_vma=False
    )
```

```python
import functools

import jax
import jax.numpy as jnp
from jax import lax
from jax.experimental import pallas as pl
from jax.experimental.pallas import tpu as pltpu
from jax.sharding import PartitionSpec as P

KEY_DIM = 64
VALUE_DIM = 128
SWA_HEADS = 16
KV_HEADS = 4
HEAD_DIM = 64
WINDOW = 128
SPAN = 64

EPS = 1e-06
SOFTMAX_TEMPER = 16.0
BF = jnp.bfloat16
F32 = jnp.float32


def rms_rows(values, gain):
    mean_square = jnp.mean(values * values, axis=-1, keepdims=True)
    return values * lax.rsqrt(mean_square + EPS) * gain


def nt(a, b):
    return lax.dot_general(a, b, (((1,), (1,)), ((), ())), preferred_element_type=F32)


def nn(a, b):
    return lax.dot_general(a, b, (((1,), (0,)), ((), ())), preferred_element_type=F32)


def tn(a, b):
    return lax.dot_general(a, b, (((0,), (0,)), ((), ())), preferred_element_type=F32)


def exact(a, b):
    return lax.dot_general(
        a, b, (((1,), (0,)), ((), ())), precision=lax.Precision.HIGHEST, preferred_element_type=F32
    )


def mixer_kernel(
    sizes,
    tok_ref,
    gv_ref,
    wq_ref,
    gq_ref,
    gk_ref,
    wk_ref,
    wv_ref,
    low_ref,
    go_ref,
    wo_ref,
    ngain_ref,
    up_ref,
    bias_ref,
    hgain_ref,
    sink_ref,
    out_ref,
    x_buf,
    w_buf,
    l_buf,
    o_buf,
    proj,
    edge_out,
    edge_in,
    state_out,
    state_in,
    local_out,
    q_far,
    hidden,
    half_out,
    half_in,
    half_own,
    piece_out,
    piece_in,
    piece_own,
    local_sem,
    tok_send,
    tok_recv,
    w_send,
    w_recv,
    l_send,
    l_recv,
    v_send,
    v_recv,
    vp_send,
    vp_recv,
    lp_send,
    lp_recv,
    o_send,
    o_recv,
    edge_sem,
    state_send,
    state_recv,
    half_send,
    half_recv,
    piece_send,
    piece_recv,
):
    sp, fs, tp = sizes
    me = lax.axis_index("sp")
    f = lax.axis_index("fs")
    c = lax.axis_index("tp")
    plane = fs * tp
    mine = f * tp + c
    own = tok_ref.shape[0]
    rows = own * tp
    kc = gv_ref.shape[0]
    MESH = pl.DeviceIdType.MESH

    def remote(src, dst, ssem, rsem, target):
        return pltpu.make_async_remote_copy(
            src_ref=src, dst_ref=dst, send_sem=ssem, recv_sem=rsem,
            device_id=target, device_id_type=MESH,
        )

    def w_rows(s):
        return w_buf.at[pl.ds(pl.multiple_of(s * kc, kc), kc)]

    def w_copy(s, way, first):
        target = {"sp": me + (1 if way == 0 else -1)}
        return remote(
            w_main(s), w_main(s), w_send.at[way, s], w_recv.at[s], target
        )

    side = f % 2
    part = kc // 2
    lpart = low_ref.shape[0] // 2

    def w_main(s):
        return w_rows(s).at[:, : starts[4]]

    def v_rows(s, h):
        at = pl.multiple_of(s * kc + h * part, part)
        return w_buf.at[pl.ds(at, part), starts[4] : starts[4] + 2 * HEAD_DIM]

    def l_rows(s, h):
        return l_buf.at[s, pl.ds(pl.multiple_of(h * lpart, lpart), lpart)]

    def v_copy(s, way):
        target = {"sp": me + (1 if way == 0 else -1)}
        return remote(v_rows(s, side), v_rows(s, side), v_send.at[way, s], v_recv.at[s], target)

    def lh_copy(s, way):
        target = {"sp": me + (1 if way == 0 else -1)}
        return remote(l_rows(s, side), l_rows(s, side), l_send.at[way, s], l_recv.at[s], target)

    def pair_copies(s, h):
        target = {"fs": f + 1 - 2 * side}
        return (
            remote(v_rows(s, h), v_rows(s, h), vp_send.at[s], vp_recv.at[s], target),
            remote(l_rows(s, h), l_rows(s, h), lp_send.at[s], lp_recv.at[s], target),
        )

    class l_copy:
        def __init__(self, s, way, first):
            self.s = s
            self.both = (v_copy(s, way), lh_copy(s, way))

        def start(self):
            for copy in self.both:
                copy.start()

        def wait_recv(self):
            for copy, onward in zip(self.both, pair_copies(self.s, side)):
                copy.wait_recv()
                onward.start()

        def wait_send(self):
            for copy in self.both:
                copy.wait_send()

    def o_copy(s, way, first):
        target = {"sp": me + (1 if way == 0 else -1)}
        return remote(
            o_buf.at[s], o_buf.at[s], o_send.at[way, s], o_recv.at[s], target
        )

    def tok_rows(i):
        return x_buf.at[pl.ds(pl.multiple_of(i * own, own), own)]

    def tok_copy(d, peer, sender):
        return remote(
            tok_ref, tok_rows(sender), tok_send.at[d - 1], tok_recv.at[d - 1],
            {"fs": peer // tp, "tp": peer % tp},
        )

    def pick(ref, width, which):
        value = ref[:, :width]
        for i in range(1, ref.shape[1] // width):
            value = jnp.where(which == i, ref[:, i * width : (i + 1) * width], value)
        return value

    def lanes(ref, width):
        return ref.at[:, pl.ds(pl.multiple_of(f * width, width), width)]

    def depth(ref, width):
        return ref.at[pl.ds(pl.multiple_of(f * width, width), width)]

    cols = [VALUE_DIM, 2 * HEAD_DIM, KEY_DIM, KEY_DIM, HEAD_DIM, HEAD_DIM]
    starts = [sum(cols[:i]) for i in range(len(cols))]
    gd = go_ref.shape[0] // fs
    wd = wo_ref.shape[0] // fs
    heads = sink_ref.shape[1] // fs
    copies_in = [
        (lanes(gv_ref, cols[0]), w_rows(me).at[:, : cols[0]]),
        (lanes(wq_ref, cols[1]), w_rows(me).at[:, starts[1] : starts[2]]),
        (depth(go_ref, gd), o_buf.at[me, pl.ds(0, gd)]),
        (depth(wo_ref, wd), o_buf.at[me, pl.ds(gd, wd)]),
        (low_ref, l_buf.at[me]),
        (tok_ref, tok_rows(mine)),
    ]
    locals_ = [
        pltpu.make_async_copy(a, b, local_sem.at[i]) for i, (a, b) in enumerate(copies_in)
    ]
    for copy in locals_:
        copy.start()
    for d in range(1, plane):
        tok_copy(d, lax.rem(mine + d, plane), mine).start()
    own_rows = pl.ds(pl.multiple_of(me * kc, kc), kc)
    kv = (f * heads) // (SWA_HEADS // KV_HEADS)
    w_buf[own_rows, starts[2] : starts[4]] = jnp.concatenate(
        [pick(gq_ref, KEY_DIM, f), pick(gk_ref, KEY_DIM, f)], 1
    )
    w_buf[own_rows, starts[4] :] = jnp.concatenate(
        [pick(wk_ref, HEAD_DIM, kv), pick(wv_ref, HEAD_DIM, kv)], 1
    )
    for copy in locals_[:5]:
        copy.wait()

    def sends(k):
        @pl.when((me - k >= 0) & (me + 1 < sp))
        def _():
            l_copy(me - k, 0, k == 0).start()
            w_copy(me - k, 0, k == 0).start()

        @pl.when((me + k < sp) & (me >= 1))
        def _():
            l_copy(me + k, 1, k == 0).start()
            w_copy(me + k, 1, k == 0).start()

        @pl.when((me == k) & (me + 1 < sp))
        def _():
            o_copy(me, 0, True).start()

        @pl.when((sp - 1 - me == k) & (me >= 1))
        def _():
            o_copy(me, 1, True).start()

    for k in range(sp - 1):
        sends(k)

        @pl.when(me - 1 - k >= 0)
        def _():
            l_copy(me - 1 - k, 0, False).wait_recv()
            w_copy(me - 1 - k, 0, False).wait_recv()

        @pl.when(me + 1 + k < sp)
        def _():
            l_copy(me + 1 + k, 1, False).wait_recv()
            w_copy(me + 1 + k, 1, False).wait_recv()

    inner = (me >= 1) & (me + 1 < sp)
    for k in range(1, sp - 1):
        @pl.when(inner & (me - k >= 0))
        def _():
            o_copy(me - k, 0, False).wait_recv()
            o_copy(me - k, 0, False).start()

        @pl.when(inner & (me + k < sp))
        def _():
            o_copy(me + k, 1, False).wait_recv()
            o_copy(me + k, 1, False).start()

    for copy in locals_[5:]:
        copy.wait()
    for i in range(sp):
        @pl.when(i != me)
        def _():
            for copy in pair_copies(i, 1 - side):
                copy.wait_recv()

    for d in range(1, plane):
        tok_copy(d, mine, lax.rem(mine + plane - d, plane)).wait_recv()


    def project(b, _):
        x = x_buf[pl.ds(pl.multiple_of(b * rows, rows), rows)].astype(F32)
        normed = rms_rows(x, ngain_ref[...]).astype(BF)
        p = nn(normed, w_buf[...]).astype(BF)
        proj[b, :, : p.shape[1]] = p
        edge_out[b] = p[rows - WINDOW :, starts[4] : starts[4] + 2 * HEAD_DIM]
        low = nt(normed[:, :kc], l_buf[0])
        for s in range(1, sp):
            low += nt(normed[:, s * kc : (s + 1) * kc], l_buf[s])
        proj[b, :, p.shape[1] : p.shape[1] + low.shape[1]] = low.astype(BF)
        return 0

    lax.fori_loop(0, fs, project, 0)
    edge = remote(edge_out, edge_in, edge_sem.at[0], edge_sem.at[1], {"sp": me + 1})

    @pl.when(me + 1 < sp)
    def _():
        edge.start()

    @pl.when(me == 0)
    def _():
        edge_in[...] = jnp.zeros_like(edge_in)

    nb = rows // SPAN
    low_at = sum(cols)
    lower = (
        lax.broadcasted_iota(jnp.int32, (SPAN, SPAN), 0)
        >= lax.broadcasted_iota(jnp.int32, (SPAN, SPAN), 1)
    )
    tri = lower.astype(F32)
    up = pick(up_ref, KEY_DIM, f)
    bias = pick(bias_ref, KEY_DIM, f)
    sinks = pick(sink_ref, heads, f)
    for b in range(fs):
        low = proj[b, :, low_at : low_at + up_ref.shape[0]]
        z = nn(low, up) + bias
        rate = (jnp.minimum(z, 0.0) - jnp.log1p(jnp.exp(-jnp.abs(z)))) / SOFTMAX_TEMPER
        state = None
        before = jnp.zeros((1, KEY_DIM), F32)
        for n in range(nb):
            r0 = n * SPAN
            within = exact(tri, rate[r0 : r0 + SPAN])
            total = within[SPAN - 1 :]
            v = proj[b, r0 : r0 + SPAN, starts[0] : starts[0] + VALUE_DIM]
            q = proj[b, r0 : r0 + SPAN, starts[2] : starts[2] + KEY_DIM].astype(F32)
            k = proj[b, r0 : r0 + SPAN, starts[3] : starts[3] + KEY_DIM].astype(F32)
            q_dec = q * KEY_DIM**-0.5 * jnp.exp(within)
            k_dec = (k * jnp.exp(-within)).astype(BF)
            k_end = (k * jnp.exp(total - within)).astype(BF)
            scores = jnp.where(lower, nt(q_dec.astype(BF), k_dec), 0.0)
            o = nn(scores.astype(BF), v)
            if state is not None:
                o += nt(q_dec.astype(BF), state.astype(BF))
            local_out[b, r0 : r0 + SPAN] = o
            q_far[b, r0 : r0 + SPAN] = (q_dec * jnp.exp(before)).astype(BF)
            update = tn(v, k_end)
            state = update if state is None else jnp.exp(total) * state + update
            before = before + total
        half = (b % 2) * KEY_DIM
        state_out[b // 2, :VALUE_DIM, half : half + KEY_DIM] = state.astype(BF)
        state_out[b // 2, VALUE_DIM:, half : half + KEY_DIM] = jnp.broadcast_to(
            jnp.exp(before), (16, KEY_DIM)
        ).astype(BF)

    def state_copy(d, sender):
        return remote(
            state_out, state_in.at[sender], state_send.at[d - 1], state_recv.at[sender],
            {"sp": me + d},
        )

    for d in range(1, sp):
        @pl.when(me + d < sp)
        def _():
            state_copy(d, me).start()

    @pl.when(me >= 1)
    def _():
        edge.wait_recv()

    qi = lax.broadcasted_iota(jnp.int32, (WINDOW, 2 * WINDOW), 0)
    ki = lax.broadcasted_iota(jnp.int32, (WINDOW, 2 * WINDOW), 1)
    distance = qi + WINDOW - ki
    inside = (distance >= 0) & (distance < WINDOW)
    for b in range(fs):
        for w in range(rows // WINDOW):
            r0 = w * WINDOW
            here = proj[b, r0 : r0 + WINDOW, starts[4] : starts[4] + 2 * HEAD_DIM]
            if w == 0:
                past = edge_in[b]
                valid = inside & ((ki >= WINDOW) | (me >= 1))
            else:
                past = proj[b, r0 - WINDOW : r0, starts[4] : starts[4] + 2 * HEAD_DIM]
                valid = inside
            band = jnp.concatenate([past, here], 0)
            bk = band[:, :HEAD_DIM]
            bv = band[:, HEAD_DIM:]
            for h in range(heads):
                q0 = starts[1] + h * HEAD_DIM
                q = proj[b, r0 : r0 + WINDOW, q0 : q0 + HEAD_DIM]
                s = jnp.where(valid, nt(q, bk) * HEAD_DIM**-0.5, -1e30)
                sink = sinks[:, h : h + 1]
                top = jnp.maximum(jnp.max(s, -1, keepdims=True), sink)
                e = jnp.exp(s - top)
                den = jnp.sum(e, -1, keepdims=True) + jnp.exp(sink - top)
                a = nn((e / den).astype(BF), bv).astype(BF)
                h0 = VALUE_DIM + h * HEAD_DIM
                hidden[b, r0 : r0 + WINDOW, h0 : h0 + HEAD_DIM] = a

    for i in range(sp - 1):
        @pl.when(i < me)
        def _():
            state_copy(1, i).wait_recv()

        @pl.when(i >= me)
        def _():
            state_in[i] = jnp.zeros(state_in.shape[1:], BF)

    for b in range(fs):
        half = (b % 2) * KEY_DIM
        incoming = jnp.zeros((VALUE_DIM, KEY_DIM), F32)
        for i in range(sp - 1):
            got = state_in[i, b // 2, :VALUE_DIM, half : half + KEY_DIM].astype(F32)
            kept = state_in[i, b // 2, VALUE_DIM : VALUE_DIM + 1, half : half + KEY_DIM].astype(F32)
            incoming = jnp.where(i < me, kept * incoming + got, incoming)
        o = local_out[b] + nt(q_far[b], incoming.astype(BF))
        hidden[b, :, :VALUE_DIM] = rms_rows(o, hgain_ref[...]).astype(BF)

    forward = 2 * me < sp
    nc = o_buf.shape[2]

    def chunk(t):
        return lax.rem(jnp.where(forward, me + t, me - t) + sp, sp)

    def half_copy(s):
        return remote(half_out.at[s], half_in.at[s], half_send.at[s], half_recv.at[s], {"tp": 1 - c})

    def piece_copy(s, d, target):
        return remote(
            piece_out.at[s, d - 1], piece_in.at[s, d - 1],
            piece_send.at[s, d - 1], piece_recv.at[s, d - 1], {"fs": target},
        )

    def produce(t):
        s = chunk(t)

        @pl.when(jnp.logical_not(inner) & (t > 0))
        def _():
            o_copy(s, 0, False).wait_recv()

        w = o_buf[s]
        for b in range(fs):
            part = nn(hidden[b], w)
            lo, hi = part[:own], part[own:]
            half_out[s, b] = jnp.where(c == 0, hi, lo).astype(BF)
            half_own[s, b] = jnp.where(c == 0, lo, hi)
        half_copy(s).start()

    def combine(t):
        s = chunk(t)
        half_copy(s).wait_recv()
        for d in range(1, fs):
            to = lax.rem(f + d, fs)
            piece_out[s, d - 1] = (half_own[s, to] + half_in[s, to].astype(F32)).astype(BF)
            piece_copy(s, d, to).start()
        piece_own[s] = half_own[s, f] + half_in[s, f].astype(F32)

    def finish(t):
        s = chunk(t)
        total = piece_own[s]
        for d in range(1, fs):
            piece_copy(s, d, f).wait_recv()
            total += piece_in[s, d - 1].astype(F32)
        if len(out_ref.shape) == 2:
            out_ref[:, pl.ds(pl.multiple_of(s * nc, nc), nc)] = total.astype(BF)
        else:
            out_ref[s] = total.astype(BF)

    produce(0)

    def steady(t, _):
        produce(t)
        combine(t - 1)
        return 0

    lax.fori_loop(1, sp, steady, 0)
    combine(sp - 1)

    def close(t, _):
        finish(t)
        s = chunk(t)
        half_copy(s).wait_send()
        for d in range(1, fs):
            piece_copy(s, d, f).wait_send()
        return 0

    lax.fori_loop(0, sp, close, 0)

    for k in range(sp - 1):
        @pl.when((me - k >= 0) & (me + 1 < sp))
        def _():
            l_copy(me - k, 0, False).wait_send()
            w_copy(me - k, 0, False).wait_send()
            o_copy(me - k, 0, False).wait_send()

        @pl.when((me + k < sp) & (me >= 1))
        def _():
            l_copy(me + k, 1, False).wait_send()
            w_copy(me + k, 1, False).wait_send()
            o_copy(me + k, 1, False).wait_send()

    for i in range(sp):
        @pl.when(i != me)
        def _():
            for copy in pair_copies(i, side):
                copy.wait_send()

    for d in range(1, plane):
        tok_copy(d, mine, mine).wait_send()

    @pl.when(me + 1 < sp)
    def _():
        edge.wait_send()

    for d in range(1, sp):
        @pl.when(me + d < sp)
        def _():
            state_copy(d, me).wait_send()


def roll_half(a):
    return jnp.concatenate([a[:, a.shape[1] // 2 :], a[:, : a.shape[1] // 2]], 1)


def fold_kernel(
    sizes,
    tok_in,
    gv_ref,
    wq_ref,
    gq_ref,
    gk_ref,
    wk_ref,
    wv_ref,
    low_ref,
    go_ref,
    wo_ref,
    ngain_in,
    up_in,
    bias_in,
    hgain_in,
    sink_in,
    out_hbm,
    tok_ref,
    ngain_ref,
    up_ref,
    bias_ref,
    hgain_ref,
    sink_ref,
    out_ref,
    x_buf,
    ww,
    wg,
    wl,
    o_buf,
    tiles,
    qw,
    kvb,
    gvb,
    qkb,
    acc,
    lowx,
    fill,
    sc,
    ew,
    decays,
    totals,
    states,
    state_out,
    state_in,
    local_out,
    q_far,
    hidden,
    half_out,
    half_in,
    half_own,
    piece_out,
    piece_in,
    piece_own,
    local_sem,
    out_sem,
    l_send,
    l_recv,
    x_send,
    x_recv,
    w_send,
    w_recv,
    p_send,
    p_recv,
    o_send,
    o_recv,
    edge_sem,
    state_sem,
    hid_send,
    hid_recv,
    half_send,
    half_recv,
    piece_send,
    piece_recv,
):
    sp, fs, tp = sizes
    me = lax.axis_index("sp")
    f = lax.axis_index("fs")
    c = lax.axis_index("tp")
    own = tok_in.shape[0]
    rows = own * tp
    kc = gv_ref.shape[0]
    part = kc // 2
    lpart = low_ref.shape[0] // 2
    MESH = pl.DeviceIdType.MESH
    pair = 2 * KEY_DIM
    wide = VALUE_DIM + pair

    slot = lax.rem(me, 2)
    far_slot = 1 - slot
    inner = (me >= 1) & (me + 1 < sp)
    outer = jnp.logical_not(inner)
    middle = 1 + slot
    outside = (sp - 1) * (me - 1)
    buddy = me + 1 - 2 * slot
    third = 2 - me // 2
    fourth = third + 1 - 2 * lax.rem(third, 2)
    chunks = [me, buddy, third, fourth]
    side = lax.rem(f, 2)
    xn = f + 1 - 2 * side
    yn = lax.rem(f + 2, fs)
    n1 = xn * (1 - c) + yn * c
    n2 = xn * c + yn * (1 - c)

    def remote(src, dst, ssem, rsem, target):
        return pltpu.make_async_remote_copy(
            src_ref=src, dst_ref=dst, send_sem=ssem, recv_sem=rsem,
            device_id=target, device_id_type=MESH,
        )

    barrier = pltpu.get_barrier_semaphore()

    def greet(target):
        pl.semaphore_signal(barrier, inc=1, device_id=target, device_id_type=MESH)

    greet({"tp": 1 - c})
    for d in range(1, fs):
        greet({"fs": lax.rem(f + d, fs)})

    @pl.when(me + 1 < sp)
    def _():
        greet({"sp": me + 1})

    @pl.when(me >= 1)
    def _():
        greet({"sp": me - 1})

    def lanes(ref, at, width):
        return ref.at[:, pl.ds(pl.multiple_of(at * width, width), width)]

    def depth(ref, width):
        return ref.at[pl.ds(pl.multiple_of(f * width, width), width)]

    def slice_rows(ref, s):
        return ref.at[pl.ds(pl.multiple_of(s * kc, kc), kc)]

    gd = go_ref.shape[0] // fs
    wd = wo_ref.shape[0] // fs
    heads = sink_in.shape[1] // fs
    wq_cols = heads * HEAD_DIM
    kv = (f * heads) // (SWA_HEADS // KV_HEADS)
    copies_in = [
        (lanes(gq_ref, f // 2, pair), tiles.at[0]),
        (lanes(gk_ref, f // 2, pair), tiles.at[1]),
        (wk_ref, tiles.at[2]),
        (wv_ref, tiles.at[3]),
        (lanes(wq_ref, f, wq_cols), slice_rows(ww, me).at[:, :wq_cols]),
        (lanes(gv_ref, f, VALUE_DIM), slice_rows(wg, me).at[:, :VALUE_DIM]),
        (low_ref, wl.at[me]),
    ]
    nc = o_buf.shape[3]
    for h in range(2):
        cut = pl.ds(h * nc, nc)
        copies_in += [
            (depth(go_ref, gd).at[:, cut], o_buf.at[me, h, pl.ds(0, gd)]),
            (depth(wo_ref, wd).at[:, cut], o_buf.at[me, h, pl.ds(gd, wd)]),
        ]
    copies_in += [
        (ngain_in, ngain_ref),
        (tok_in, tok_ref),
        (up_in, up_ref),
        (bias_in, bias_ref),
        (hgain_in, hgain_ref),
        (sink_in, sink_ref),
    ]
    locals_ = [
        pltpu.make_async_copy(a, b, local_sem.at[i]) for i, (a, b) in enumerate(copies_in)
    ]
    for copy in locals_[11:] + locals_[:11]:
        copy.start()

    mine = f * tp + c
    b1, b2, b3 = n1 * tp + c, n2 * tp + c, (fs - 1 - f) * tp + c

    for copy in locals_[11:]:
        copy.wait()
    normed = rms_rows(tok_ref[...].astype(F32), ngain_ref[...]).astype(BF)
    x_buf[slot, pl.ds(pl.multiple_of(mine * own, own), own)] = normed

    def half_block(s, i, h):
        at = pl.multiple_of(i * own + h * (own // 2), own // 2)
        return x_buf.at[s, pl.ds(at, own // 2)]

    def x_copy(s, i, h, k, target):
        ref = half_block(s, i, h)
        return remote(ref, ref, x_send.at[s, k, h], x_recv.at[s, i, h], target)

    SIB = {"tp": 1 - c}

    def x_first(s, h):
        return [
            x_copy(s, mine, h, 0, {"fs": n1}),
            x_copy(s, mine, h, 1, {"fs": n2}),
            x_copy(s, mine, h, 2, SIB),
        ]

    def x_from1(s, h):
        return [x_copy(s, b1, h, 3, {"fs": n2}), x_copy(s, b1, h, 4, SIB)]

    def x_from2(s, h):
        return [x_copy(s, b2, h, 5, SIB)]

    def x_from3(s, h):
        return [x_copy(s, b3, h, 6, SIB)]

    def x_all(s, h):
        return x_first(s, h) + x_from1(s, h) + x_from2(s, h) + x_from3(s, h)

    def x_out(h):
        return x_copy(slot, mine, h, 0, {"sp": middle})

    def kv_rows(s, h):
        at = pl.multiple_of(s * kc + h * part, part)
        return ww.at[pl.ds(at, part), wq_cols:]

    def low_rows(s, h):
        return wl.at[s, pl.ds(pl.multiple_of(h * lpart, lpart), lpart)]

    def w_copy(kind, s):
        ref = (
            lambda: slice_rows(ww, s).at[:, :wq_cols],
            lambda: kv_rows(s, side),
            lambda: low_rows(s, c),
            lambda: slice_rows(wg, s),
        )[kind]()
        return remote(ref, ref, w_send.at[kind, s], w_recv.at[kind, s], {"sp": middle})

    def kv_share(s, h):
        return remote(
            kv_rows(s, h), kv_rows(s, h), p_send.at[0, s], p_recv.at[0, s], {"fs": xn}
        )

    def low_share(s, h):
        return remote(low_rows(s, h), low_rows(s, h), p_send.at[1, s], p_recv.at[1, s], SIB)

    def o_copy(way, s, h, d):
        target = {"sp": middle if way == 0 else outside}
        ref = o_buf.at[s, h, pl.ds(d * gd, gd)]
        return remote(ref, ref, o_send.at[way, s, h, d], o_recv.at[s, h, d], target)

    def o_relay(way, s, h):
        for d in range(2):
            o_copy(0, s, h, d).wait_recv()
            o_copy(way, s, h, d).start()

    quarters = [(h, d) for h in range(2) for d in range(2)]

    def l_copy(i, k, target):
        return remote(lowx.at[i], lowx.at[i], l_send.at[k], l_recv.at[i], target)

    def l_first():
        peers = [{"fs": n1}, {"fs": n2}, {"fs": fs - 1 - f}, SIB]
        return [l_copy(mine, k, peer) for k, peer in enumerate(peers)]

    def l_onward():
        return [l_copy(i, 4 + k, SIB) for k, i in enumerate((b1, b2, b3))]

    def start(copies):
        for copy in copies:
            copy.start()

    pl.semaphore_wait(barrier, fs + jnp.where(inner, 2, 1))

    LOW, KV, QUERY, STATE = 2, 1, 0, 3
    locals_[6].wait()
    w_copy(LOW, me).start()

    @pl.when(outer)
    def _():
        for h in range(2):
            x_out(h).start()

    @pl.when(inner)
    def _():
        for h in range(2):
            start(x_first(slot, h))

    for copy in locals_[:6]:
        copy.wait()
    own_rows = pl.ds(pl.multiple_of(me * kc, kc), kc)

    def half_of(i, width, which):
        return jnp.where(which == 0, tiles[i, :, :width], tiles[i, :, width:])

    ww[own_rows, wq_cols:] = jnp.concatenate(
        [half_of(2, HEAD_DIM, kv), half_of(3, HEAD_DIM, kv)], 1
    )
    w_copy(KV, me).start()
    w_copy(QUERY, me).start()
    wg[own_rows, VALUE_DIM:] = jnp.concatenate(
        [half_of(0, KEY_DIM, side), half_of(1, KEY_DIM, side)], 1
    )
    for copy in locals_[7:11]:
        copy.wait()

    @pl.when(outer)
    def _():
        w_copy(STATE, me).start()
        for h, d in quarters:
            o_copy(0, me, h, d).start()

    lane = lax.broadcasted_iota(jnp.int32, (rows, pair), 1)
    row = lax.broadcasted_iota(jnp.int32, (rows, pair), 0)
    left = lane < KEY_DIM
    early = row < SPAN
    same = (row < SPAN) == (lane < SPAN)
    diagonal = same & (row >= lane)
    below = (row >= SPAN) & (lane < SPAN)

    def edge_rows(i, h):
        n = fs * rows // 2
        return kvb.at[i, pl.ds(pl.multiple_of(h * n, n), n)]

    edge = remote(
        edge_rows(2, side), edge_rows(0, side), edge_sem.at[0], edge_sem.at[1], {"sp": me + 1}
    )

    def edge_share(h):
        return remote(
            edge_rows(0, h), edge_rows(0, h), edge_sem.at[2], edge_sem.at[3], {"fs": xn}
        )
    state = remote(state_out, state_in, state_sem.at[0], state_sem.at[1], {"sp": me + 1})

    def hid_part(s, i):
        return hidden.at[s, :, i * VALUE_DIM : (i + 1) * VALUE_DIM]

    def hid_copy(i, s):
        return remote(
            hid_part(s, i), hid_part(s, i), hid_send.at[i], hid_recv.at[i], {"sp": outside}
        )

    def seq(b):
        if isinstance(b, int):
            return pl.ds(b * rows, rows)
        return pl.ds(pl.multiple_of(b * rows, rows), rows)

    @pl.when(inner)
    def _():
        for h, d in quarters:
            o_copy(1, me, h, d).start()

        def arrive(kind, s, onward):
            w_copy(kind, s).wait_recv()
            if onward:
                w_copy(kind, s).start()
            if kind == LOW:
                low_share(s, c).start()
            if kind == KV:
                kv_share(s, side).start()

        def neighbours(s, h):
            x_copy(s, b1, h, 0, SIB).wait_recv()
            start(x_from1(s, h))
            x_copy(s, b2, h, 0, SIB).wait_recv()
            start(x_from2(s, h))

        def corner(s):
            for h in range(2):
                x_copy(s, b3, h, 0, SIB).wait_recv()
                start(x_from3(s, h))

        def siblings(s):
            for g in range(fs):
                for h in range(2):
                    x_copy(s, g * tp + 1 - c, h, 0, SIB).wait_recv()

        def columns(s):
            return pl.ds(pl.multiple_of(s * kc, kc), kc)

        bs = [bias_ref[:, i * KEY_DIM : (i + 1) * KEY_DIM] for i in range(fs)]
        ups = [up_ref[:, i * KEY_DIM : (i + 1) * KEY_DIM] for i in range(fs)]
        bias, up = bs[0], ups[0]
        for i in range(1, fs):
            bias = jnp.where(f == i, bs[i], bias)
            up = jnp.where(f == i, ups[i], up)
        up_l = jnp.concatenate([up, jnp.zeros_like(up)], 1)
        up_r = jnp.concatenate([jnp.zeros_like(up), up], 1)
        bias2 = jnp.concatenate([bias, bias], 1)

        def own_low():
            at = pl.ds(pl.multiple_of(mine * own, own), own)
            x = jnp.concatenate([x_buf[slot, at], x_buf[far_slot, at]], 0)
            low = nt(wl[0], x[:, :kc])
            for j in range(1, sp):
                low += nt(wl[j], x[:, j * kc : (j + 1) * kc])
            lowx[mine] = low.astype(BF)

        def gate(p):
            pre = []
            for i in range(tp):
                z = tn(lowx[2 * p * tp + i], up_l) + tn(lowx[(2 * p + 1) * tp + i], up_r)
                pre.append(z + bias2)
            return [
                jnp.concatenate([z[k * own : (k + 1) * own] for z in pre], 0) for k in range(2)
            ]

        def decay():
            tri = diagonal.astype(F32)
            for p in range(fs // 2):
                for s, z in zip((slot, far_slot), gate(p)):
                    decay_of(s, p, z, tri)

        def decay_of(s, p, z, tri):
            rate = (jnp.minimum(z, 0.0) - jnp.log1p(jnp.exp(-jnp.abs(z)))) / SOFTMAX_TEMPER
            within = exact(tri, rate)
            t0, t1 = within[SPAN - 1 : SPAN], within[rows - 1 :]
            grow = jnp.exp(within) * KEY_DIM**-0.5
            end = jnp.exp(jnp.where(early, t0, t1) - within)
            decays[s, p, 0] = grow
            decays[s, p, 1] = jnp.exp(-within)
            decays[s, p, 2] = end
            decays[s, p, 3] = grow * jnp.where(early, 1.0, jnp.exp(t0))
            decays[s, p, 4] = end * jnp.where(early, jnp.exp(t1), 1.0)
            totals[s, p] = jnp.broadcast_to(jnp.exp(t0 + t1), totals.shape[2:])

        def window_maps(s, slices):
            total = nn(x_buf[s, :, columns(slices[0])], slice_rows(ww, slices[0])[...])
            for j in slices[1:]:
                total += nn(x_buf[s, :, columns(j)], slice_rows(ww, j)[...])
            return total

        def far_rows(h):
            x_copy(far_slot, mine, h, 0, SIB).wait_recv()
            start(x_first(far_slot, h))

        arrive(LOW, buddy, True)
        w_copy(STATE, me).start()
        o_copy(0, me, 0, 0).start()
        arrive(LOW, third, False)
        arrive(KV, third, False)
        neighbours(slot, 0)
        far_rows(0)
        arrive(LOW, fourth, False)
        neighbours(slot, 1)
        far_rows(1)
        for s in chunks[1:]:
            low_share(s, 1 - c).wait_recv()
        own_low()
        start(l_first())
        arrive(KV, buddy, True)
        neighbours(far_slot, 0)
        arrive(QUERY, buddy, True)
        o_copy(0, me, 0, 1).start()
        corner(slot)
        siblings(slot)
        arrive(QUERY, third, False)
        kv_share(third, 1 - side).wait_recv()
        acc[slot] = window_maps(slot, (me, third))
        neighbours(far_slot, 1)
        arrive(STATE, buddy, True)
        arrive(KV, fourth, False)
        for i in (b1, b2, b3):
            l_copy(i, 0, SIB).wait_recv()
        start(l_onward())
        o_relay(1, third, 0)
        for g in range(fs):
            l_copy(g * tp + 1 - c, 0, SIB).wait_recv()
        decay()
        corner(far_slot)
        kv_share(buddy, 1 - side).wait_recv()
        siblings(far_slot)
        acc[far_slot] = window_maps(far_slot, chunks[:3])
        arrive(QUERY, fourth, False)
        kv_share(fourth, 1 - side).wait_recv()

        def place(s, slices):
            p = acc[s] + window_maps(s, slices)
            q = p[:, :wq_cols].astype(BF).astype(F32) * HEAD_DIM**-0.5
            for h in range(heads):
                qh = jnp.where(left_all, q if h == 0 else roll_half(q), 0.0)
                qw[s, h] = qh.astype(BF)
            kvb[s + 1] = p[:, wq_cols:].astype(BF)

        left_all = lax.broadcasted_iota(jnp.int32, (fs * rows, pair), 1) < KEY_DIM
        place(slot, (buddy, fourth))

        @pl.when(me == 1)
        def _():
            edge.start()
            kvb[0] = jnp.zeros(kvb.shape[1:], BF)
            state_in[...] = jnp.zeros_like(state_in)

        o_copy(0, me, 1, 0).start()

        @pl.when(me > 1)
        def _():
            o_copy(0, me, 1, 1).start()

        place(far_slot, (fourth,))

        tall = heads * WINDOW
        qi = lax.broadcasted_iota(jnp.int32, (tall, 2 * WINDOW), 0)
        ki = lax.broadcasted_iota(jnp.int32, (tall, 2 * WINDOW), 1)
        distance = lax.rem(qi, WINDOW) + WINDOW - ki
        inside = (distance >= 0) & (distance < WINDOW)
        sinks = sink_ref[:, :heads]
        for i in range(1, fs):
            sinks = jnp.where(f == i, sink_ref[:, i * heads : (i + 1) * heads], sinks)
        sink = sinks[:, :1]
        for h in range(1, heads):
            sink = jnp.where(qi < h * WINDOW, sink, sinks[:, h : h + 1])
        fill[...] = jnp.where(ki == 0, sink, -1e30)
        key_row = lax.broadcasted_iota(jnp.int32, (2 * WINDOW, pair), 0)
        key_lane = lax.broadcasted_iota(jnp.int32, (2 * WINDOW, pair), 1)

        def window(s):
            valid = inside & ((ki >= WINDOW) | (me > 1) | (s > 0))
            bands = [jnp.concatenate([kvb[s, seq(b)], kvb[s + 1, seq(b)]], 0) for b in range(fs)]
            for b in range(fs):
                q = jnp.concatenate([qw[s, h, seq(b)] for h in range(heads)], 0)
                sc[b] = jnp.where(valid, nt(q, bands[b]), fill[...])
            for b in range(fs):
                near = sc[b]
                top = jnp.max(near, -1, keepdims=True)
                ew[b] = jnp.exp(near - top).astype(BF)
            for b in range(fs):
                band = jnp.concatenate([kvb[s, seq(b)], kvb[s + 1, seq(b)]], 0).astype(F32)
                values = jnp.where(
                    key_lane < HEAD_DIM, 1.0, jnp.where(key_row == 0, 0.0, band)
                ).astype(BF)
                both = nn(ew[b], values)
                turned = roll_half(both)
                first = turned[:WINDOW] / both[:WINDOW]
                second = both[WINDOW:] / turned[WINDOW:]
                hidden[s, seq(b), VALUE_DIM:] = jnp.where(left, first, second).astype(BF)

        window(far_slot)
        hid_copy(1, far_slot).start()
        def state_maps(s, slices):
            total = nn(x_buf[s, :, columns(slices[0])], slice_rows(wg, slices[0])[...])
            for j in slices[1:]:
                total += nn(x_buf[s, :, columns(j)], slice_rows(wg, j)[...])
            return total

        w_copy(STATE, third).wait_recv()
        for s in range(2):
            acc[s] = state_maps(s, chunks[:3])
        w_copy(STATE, fourth).wait_recv()

        for s in range(2):
            p = (acc[s] + state_maps(s, chunks[3:])).astype(BF)
            gvb[s] = p[:, :VALUE_DIM]
            qkb[s] = p[:, VALUE_DIM:].astype(F32)

        def keys(s, p):
            return jnp.where(left, roll_half(qkb[s, seq(2 * p)]), qkb[s, seq(2 * p + 1)])

        def queries(s, p):
            return jnp.where(left, qkb[s, seq(2 * p)], roll_half(qkb[s, seq(2 * p + 1)]))

        for s in range(2):
            for p in range(fs // 2):
                k_far = (keys(s, p) * decays[s, p, 4]).astype(BF)
                states[s, p] = jnp.where(
                    left, tn(gvb[s, seq(2 * p)], k_far), tn(gvb[s, seq(2 * p + 1)], k_far)
                )
        for p in range(fs // 2):
            state_out[p] = (totals[1, p, :1] * states[0, p] + states[1, p]).astype(BF)

        @pl.when(me == 1)
        def _():
            state.start()
            o_copy(0, me, 1, 1).start()

        for h in range(2):
            o_relay(0, buddy, h)

        for s in range(2):
            for p in range(fs // 2):
                k = keys(s, p)
                q = queries(s, p)
                qd = q * decays[s, p, 0]
                qf = q * decays[s, p, 3]
                kd = (k * decays[s, p, 1]).astype(BF)
                ke = (k * decays[s, p, 2]).astype(BF)
                for j in range(2):
                    here = left if j == 0 else jnp.logical_not(left)
                    qj = jnp.where(here, qd, 0.0).astype(BF)
                    scores = jnp.where(
                        diagonal, nt(qj, kd), jnp.where(below, nt(qj, ke), 0.0)
                    ).astype(BF)
                    local_out[s, seq(2 * p + j)] = nn(scores, gvb[s, seq(2 * p + j)])
                    q_far[s, seq(2 * p + j)] = jnp.where(here, qf, 0.0).astype(BF)

        @pl.when(me > 1)
        def _():
            edge.wait_recv()
            edge_share(side).start()
            state.wait_recv()

        def finish_state(s):
            for p in range(fs // 2):
                arrived = state_in[p].astype(F32)
                entering = jnp.where(s == 0, arrived, totals[0, p, :1] * arrived + states[0, p])
                entering = entering.astype(BF)
                for j in range(2):
                    b = 2 * p + j
                    o = local_out[s, seq(b)] + nt(q_far[s, seq(b)], entering)
                    hidden[s, seq(b), :VALUE_DIM] = rms_rows(o, hgain_ref[...]).astype(BF)

        finish_state(far_slot)
        hid_copy(0, far_slot).start()
        finish_state(slot)

        @pl.when(me > 1)
        def _():
            edge_share(1 - side).wait_recv()

        window(slot)
        o_relay(1, third, 1)

    @pl.when(outer)
    def _():
        hid_copy(1, slot).wait_recv()
        hid_copy(0, slot).wait_recv()

    parts = [(s, h) for s in chunks for h in range(2)]

    def half_copy(s, h):
        return remote(
            half_out.at[s, h], half_in.at[s, h], half_send.at[s, h], half_recv.at[s, h], SIB
        )

    def piece_copy(s, h, d, target):
        return remote(
            piece_out.at[s, h, d - 1], piece_in.at[s, h, d - 1],
            piece_send.at[s, h, d - 1], piece_recv.at[s, h, d - 1], {"fs": target},
        )

    def produce(t):
        s, h = parts[t]
        if 2 <= t < 6:
            @pl.when(outer)
            def _():
                for d in range(2):
                    o_copy(0, s, h, d).wait_recv()
        if t >= 6:
            for d in range(2):
                o_copy(0, s, h, d).wait_recv()

                @pl.when(inner)
                def _():
                    o_copy(1, s, h, d).start()

        w = o_buf[s, h]
        for b in range(fs):
            partial = nn(hidden[slot, seq(b)], w)
            lo, hi = partial[:own], partial[own:]
            half_out[s, h, b] = jnp.where(c == 0, hi, lo).astype(BF)
            half_own[s, h, b] = jnp.where(c == 0, lo, hi)
        half_copy(s, h).start()

    def combine(t):
        s, h = parts[t]
        half_copy(s, h).wait_recv()
        for d in range(1, fs):
            to = lax.rem(f + d, fs)
            piece_out[s, h, d - 1] = (half_own[s, h, to] + half_in[s, h, to].astype(F32)).astype(BF)
            piece_copy(s, h, d, to).start()
        piece_own[s, h] = half_own[s, h, f] + half_in[s, h, f].astype(F32)

    def finish(t):
        s, h = parts[t]
        total = piece_own[s, h]
        for d in range(1, fs):
            piece_copy(s, h, d, f).wait_recv()
            total += piece_in[s, h, d - 1].astype(F32)
        at = pl.ds(pl.multiple_of((2 * s + h) * nc, nc), nc)
        out_ref[:, at] = total.astype(BF)
        pltpu.make_async_copy(out_ref.at[:, at], out_hbm.at[:, at], out_sem.at[t]).start()

    produce(0)
    for t in range(1, 2 * sp):
        produce(t)
        combine(t - 1)
    combine(2 * sp - 1)
    for t in range(2 * sp):
        finish(t)
    for t, (s, h) in enumerate(parts):
        at = pl.ds(pl.multiple_of((2 * s + h) * nc, nc), nc)
        pltpu.make_async_copy(out_ref.at[:, at], out_hbm.at[:, at], out_sem.at[t]).wait()
        half_copy(s, h).wait_send()
        for d in range(1, fs):
            piece_copy(s, h, d, f).wait_send()

    for kind in range(4):
        w_copy(kind, me).wait_send()
    for h, d in quarters:
        o_copy(0, me, h, d).wait_send()

    @pl.when(outer)
    def _():
        for h in range(2):
            x_out(h).wait_send()

    @pl.when(inner)
    def _():
        for s in range(2):
            for copy in x_all(s, 0) + x_all(s, 1):
                copy.wait_send()
        for kind in range(4):
            w_copy(kind, buddy).wait_send()
        for copy in l_first() + l_onward():
            copy.wait_send()
        for s in chunks[1:]:
            kv_share(s, side).wait_send()
            low_share(s, c).wait_send()
        for h, d in quarters:
            o_copy(0, buddy, h, d).wait_send()
            for s in (me, third, fourth):
                o_copy(1, s, h, d).wait_send()
        for i in range(2):
            hid_copy(i, far_slot).wait_send()

        @pl.when(me == 1)
        def _():
            edge.wait_send()
            state.wait_send()

        @pl.when(me > 1)
        def _():
            edge_share(side).wait_send()


def fold_call(sizes, operands):
    sp, fs, tp = sizes
    own, d = operands[0].shape
    rows = own * tp
    kc = operands[1].shape[0]
    rank = operands[7].shape[0]
    depth = (operands[8].shape[0] + operands[9].shape[0]) // fs
    nc = operands[8].shape[1]
    pair = 2 * KEY_DIM
    all_rows = fs * rows
    pairs = fs // 2
    vm = pltpu.VMEM
    dma = pltpu.SemaphoreType.DMA
    small = [(o.shape, o.dtype) for o in operands[10:]]
    scratch = [
        vm((own, d), BF),
        *(vm(shape, dtype) for shape, dtype in small),
        vm((own, sp * nc), BF),
        vm((2, all_rows, d), BF),
        vm((d, 2 * pair), BF),
        vm((d, VALUE_DIM + pair), BF),
        vm((sp, rank, kc), BF),
        vm((sp, 2, depth, nc // 2), BF),
        vm((4, kc, pair), BF),
        vm((2, 2, all_rows, pair), BF),
        vm((3, all_rows, pair), BF),
        vm((2, all_rows, VALUE_DIM), BF),
        vm((2, all_rows, pair), F32),
        vm((2, all_rows, 2 * pair), F32),
        vm((fs * tp, rank, 2 * own), BF),
        vm((2 * WINDOW, 2 * WINDOW), F32),
        vm((fs, 2 * WINDOW, 2 * WINDOW), F32),
        vm((fs, 2 * WINDOW, 2 * WINDOW), BF),
        vm((2, pairs, 5, rows, pair), F32),
        vm((2, pairs, 8, pair), F32),
        vm((2, pairs, VALUE_DIM, pair), F32),
        vm((pairs, VALUE_DIM, pair), BF),
        vm((pairs, VALUE_DIM, pair), BF),
        vm((2, all_rows, VALUE_DIM), F32),
        vm((2, all_rows, pair), BF),
        vm((2, all_rows, depth), BF),
        vm((sp, 2, fs, own, nc // 2), BF),
        vm((sp, 2, fs, own, nc // 2), BF),
        vm((sp, 2, fs, own, nc // 2), F32),
        vm((sp, 2, fs - 1, own, nc // 2), BF),
        vm((sp, 2, fs - 1, own, nc // 2), BF),
        vm((sp, 2, own, nc // 2), F32),
        dma((17,)),
        dma((2 * sp,)),
        dma((7,)),
        dma((fs * tp,)),
        dma((2, 7, 2)),
        dma((2, fs * tp, 2)),
        dma((4, sp)),
        dma((4, sp)),
        dma((2, sp)),
        dma((2, sp)),
        dma((2, sp, 2, 2)),
        dma((sp, 2, 2)),
        dma((4,)),
        dma((2,)),
        dma((2,)),
        dma((2,)),
        dma((sp, 2)),
        dma((sp, 2)),
        dma((sp, 2, fs - 1)),
        dma((sp, 2, fs - 1)),
    ]
    anywhere = pl.BlockSpec(memory_space=pl.ANY)
    return pl.pallas_call(
        functools.partial(fold_kernel, sizes),
        out_shape=jax.ShapeDtypeStruct((own, sp * nc), BF),
        in_specs=[anywhere] * 15,
        out_specs=anywhere,
        scratch_shapes=scratch,
        compiler_params=pltpu.CompilerParams(
            has_side_effects=True, vmem_limit_bytes=60 * 1024 * 1024, collective_id=0
        ),
    )(*operands)


def folds(sp, fs, tp, shape, rows, kc, width, rank, nc, depth):
    whole_rows = rows == WINDOW == 2 * SPAN
    lanes_fit = nc % 256 == 0 and kc % 128 == 0 and depth == 2 * VALUE_DIM and 2 * HEAD_DIM == 2 * KEY_DIM
    return sp == 4 and fs == 4 and tp == 2 and whole_rows and lanes_fit and rank % 32 == 0


def per_device(
    tokens,
    norm_gain,
    gla_query_weight,
    gla_key_weight,
    gla_value_weight,
    decay_down,
    decay_up,
    decay_bias,
    head_gain,
    window_query_weight,
    window_key_weight,
    window_value_weight,
    sink_logit,
    gla_output_weight,
    window_output_weight,
):
    fs, tp, sp = (lax.axis_size(n) for n in ("fs", "tp", "sp"))
    low = decay_down.T
    own = tokens.shape[1]
    rows = own * tp
    kc = decay_down.shape[0]
    width = VALUE_DIM + 4 * HEAD_DIM + 2 * KEY_DIM
    rank = low.shape[0]
    depth = (gla_output_weight.shape[0] + window_output_weight.shape[0]) // fs
    nc = gla_output_weight.shape[1]
    flat = nc % 128 == 0
    operands = (
        tokens[0],
        gla_value_weight,
        window_query_weight,
        gla_query_weight,
        gla_key_weight,
        window_key_weight,
        window_value_weight,
        low,
        gla_output_weight,
        window_output_weight,
        norm_gain[None],
        decay_up,
        decay_bias[None],
        head_gain[None],
        sink_logit[None],
    )
    if folds(sp, fs, tp, tokens.shape, rows, kc, width, rank, nc, depth):
        return fold_call((sp, fs, tp), operands).reshape(1, own, sp * nc)
    vm = pltpu.VMEM
    dma = pltpu.SemaphoreType.DMA
    scratch = [
        vm((fs * rows, tokens.shape[2]), BF),
        vm((sp * kc, width), BF),
        vm((sp, rank, kc), BF),
        vm((sp, depth, nc), BF),
        vm((fs, rows, width + 128), BF),
        vm((fs, WINDOW, 2 * HEAD_DIM), BF),
        vm((fs, WINDOW, 2 * HEAD_DIM), BF),
        vm((fs // 2, VALUE_DIM + 16, 2 * KEY_DIM), BF),
        vm((sp, fs // 2, VALUE_DIM + 16, 2 * KEY_DIM), BF),
        vm((fs, rows, VALUE_DIM), F32),
        vm((fs, rows, KEY_DIM), BF),
        vm((fs, rows, depth), BF),
        vm((sp, fs, own, nc), BF),
        vm((sp, fs, own, nc), BF),
        vm((sp, fs, own, nc), F32),
        vm((sp, fs - 1, own, nc), BF),
        vm((sp, fs - 1, own, nc), BF),
        vm((sp, own, nc), F32),
        dma((6,)),
        dma((fs * tp - 1,)),
        dma((fs * tp - 1,)),
        dma((2, sp)),
        dma((sp,)),
        dma((2, sp)),
        dma((sp,)),
        dma((2, sp)),
        dma((sp,)),
        dma((sp,)),
        dma((sp,)),
        dma((sp,)),
        dma((sp,)),
        dma((2, sp)),
        dma((sp,)),
        dma((2,)),
        dma((sp,)),
        dma((sp,)),
        dma((sp,)),
        dma((sp,)),
        dma((sp, fs - 1)),
        dma((sp, fs - 1)),
    ]
    spec = pl.BlockSpec(memory_space=pltpu.VMEM)
    anywhere = pl.BlockSpec(memory_space=pl.ANY)
    mixed = pl.pallas_call(
        functools.partial(mixer_kernel, (sp, fs, tp)),
        out_shape=jax.ShapeDtypeStruct((own, sp * nc) if flat else (sp, own, nc), BF),
        in_specs=[
            anywhere if i in (1, 2, 8, 9) else spec for i in range(15)
        ],
        out_specs=spec,
        scratch_shapes=scratch,
        compiler_params=pltpu.CompilerParams(
            has_side_effects=True, vmem_limit_bytes=60 * 1024 * 1024
        ),
    )(*operands)
    return (mixed if flat else mixed.transpose(1, 0, 2)).reshape(1, own, sp * nc)


def solution(mesh):
    in_specs = (
        P("fs", ("sp", "tp"), None),
        P(),
        P("sp", "tp"),
        P("sp", "tp"),
        P("sp", "tp"),
        P("sp", None),
        P(None, "tp"),
        P("tp"),
        P(),
        P("sp", "tp"),
        P("sp", "tp"),
        P("sp", "tp"),
        P("tp"),
        P("tp", "sp"),
        P("tp", "sp"),
    )
    out_specs = P("fs", ("sp", "tp"), None)
    return jax.shard_map(
        per_device, mesh=mesh, in_specs=in_specs, out_specs=out_specs, check_vma=False
    )
```

```python
import functools

import jax
import jax.numpy as jnp
from jax import lax
from jax.experimental import pallas as pl
from jax.experimental.pallas import tpu as pltpu
from jax.sharding import PartitionSpec as P

KEY_DIM = 64
VALUE_DIM = 128
SWA_HEADS = 16
KV_HEADS = 4
HEAD_DIM = 64
WINDOW = 128
SPAN = 64

EPS = 1e-06
SOFTMAX_TEMPER = 16.0
BF = jnp.bfloat16
F32 = jnp.float32


def rms_rows(values, gain):
    mean_square = jnp.mean(values * values, axis=-1, keepdims=True)
    return values * lax.rsqrt(mean_square + EPS) * gain


def nt(a, b):
    return lax.dot_general(a, b, (((1,), (1,)), ((), ())), preferred_element_type=F32)


def nn(a, b):
    return lax.dot_general(a, b, (((1,), (0,)), ((), ())), preferred_element_type=F32)


def tn(a, b):
    return lax.dot_general(a, b, (((0,), (0,)), ((), ())), preferred_element_type=F32)


def exact(a, b):
    return lax.dot_general(
        a, b, (((1,), (0,)), ((), ())), precision=lax.Precision.HIGHEST, preferred_element_type=F32
    )


def mixer_kernel(
    sizes,
    tok_ref,
    gv_ref,
    wq_ref,
    gq_ref,
    gk_ref,
    wk_ref,
    wv_ref,
    low_ref,
    go_ref,
    wo_ref,
    ngain_ref,
    up_ref,
    bias_ref,
    hgain_ref,
    sink_ref,
    out_ref,
    x_buf,
    w_buf,
    l_buf,
    o_buf,
    proj,
    edge_out,
    edge_in,
    state_out,
    state_in,
    local_out,
    q_far,
    hidden,
    half_out,
    half_in,
    half_own,
    piece_out,
    piece_in,
    piece_own,
    local_sem,
    tok_send,
    tok_recv,
    w_send,
    w_recv,
    l_send,
    l_recv,
    v_send,
    v_recv,
    vp_send,
    vp_recv,
    lp_send,
    lp_recv,
    o_send,
    o_recv,
    edge_sem,
    state_send,
    state_recv,
    half_send,
    half_recv,
    piece_send,
    piece_recv,
):
    sp, fs, tp = sizes
    me = lax.axis_index("sp")
    f = lax.axis_index("fs")
    c = lax.axis_index("tp")
    plane = fs * tp
    mine = f * tp + c
    own = tok_ref.shape[0]
    rows = own * tp
    kc = gv_ref.shape[0]
    MESH = pl.DeviceIdType.MESH

    def remote(src, dst, ssem, rsem, target):
        return pltpu.make_async_remote_copy(
            src_ref=src, dst_ref=dst, send_sem=ssem, recv_sem=rsem,
            device_id=target, device_id_type=MESH,
        )

    def w_rows(s):
        return w_buf.at[pl.ds(pl.multiple_of(s * kc, kc), kc)]

    def w_copy(s, way, first):
        target = {"sp": me + (1 if way == 0 else -1)}
        return remote(
            w_main(s), w_main(s), w_send.at[way, s], w_recv.at[s], target
        )

    side = f % 2
    part = kc // 2
    lpart = low_ref.shape[0] // 2

    def w_main(s):
        return w_rows(s).at[:, : starts[4]]

    def v_rows(s, h):
        at = pl.multiple_of(s * kc + h * part, part)
        return w_buf.at[pl.ds(at, part), starts[4] : starts[4] + 2 * HEAD_DIM]

    def l_rows(s, h):
        return l_buf.at[s, pl.ds(pl.multiple_of(h * lpart, lpart), lpart)]

    def v_copy(s, way):
        target = {"sp": me + (1 if way == 0 else -1)}
        return remote(v_rows(s, side), v_rows(s, side), v_send.at[way, s], v_recv.at[s], target)

    def lh_copy(s, way):
        target = {"sp": me + (1 if way == 0 else -1)}
        return remote(l_rows(s, side), l_rows(s, side), l_send.at[way, s], l_recv.at[s], target)

    def pair_copies(s, h):
        target = {"fs": f + 1 - 2 * side}
        return (
            remote(v_rows(s, h), v_rows(s, h), vp_send.at[s], vp_recv.at[s], target),
            remote(l_rows(s, h), l_rows(s, h), lp_send.at[s], lp_recv.at[s], target),
        )

    class l_copy:
        def __init__(self, s, way, first):
            self.s = s
            self.both = (v_copy(s, way), lh_copy(s, way))

        def start(self):
            for copy in self.both:
                copy.start()

        def wait_recv(self):
            for copy, onward in zip(self.both, pair_copies(self.s, side)):
                copy.wait_recv()
                onward.start()

        def wait_send(self):
            for copy in self.both:
                copy.wait_send()

    def o_copy(s, way, first):
        target = {"sp": me + (1 if way == 0 else -1)}
        return remote(
            o_buf.at[s], o_buf.at[s], o_send.at[way, s], o_recv.at[s], target
        )

    def tok_rows(i):
        return x_buf.at[pl.ds(pl.multiple_of(i * own, own), own)]

    def tok_copy(d, peer, sender):
        return remote(
            tok_ref, tok_rows(sender), tok_send.at[d - 1], tok_recv.at[d - 1],
            {"fs": peer // tp, "tp": peer % tp},
        )

    def pick(ref, width, which):
        value = ref[:, :width]
        for i in range(1, ref.shape[1] // width):
            value = jnp.where(which == i, ref[:, i * width : (i + 1) * width], value)
        return value

    def lanes(ref, width):
        return ref.at[:, pl.ds(pl.multiple_of(f * width, width), width)]

    def depth(ref, width):
        return ref.at[pl.ds(pl.multiple_of(f * width, width), width)]

    cols = [VALUE_DIM, 2 * HEAD_DIM, KEY_DIM, KEY_DIM, HEAD_DIM, HEAD_DIM]
    starts = [sum(cols[:i]) for i in range(len(cols))]
    gd = go_ref.shape[0] // fs
    wd = wo_ref.shape[0] // fs
    heads = sink_ref.shape[1] // fs
    copies_in = [
        (lanes(gv_ref, cols[0]), w_rows(me).at[:, : cols[0]]),
        (lanes(wq_ref, cols[1]), w_rows(me).at[:, starts[1] : starts[2]]),
        (depth(go_ref, gd), o_buf.at[me, pl.ds(0, gd)]),
        (depth(wo_ref, wd), o_buf.at[me, pl.ds(gd, wd)]),
        (low_ref, l_buf.at[me]),
        (tok_ref, tok_rows(mine)),
    ]
    locals_ = [
        pltpu.make_async_copy(a, b, local_sem.at[i]) for i, (a, b) in enumerate(copies_in)
    ]
    for copy in locals_:
        copy.start()
    for d in range(1, plane):
        tok_copy(d, lax.rem(mine + d, plane), mine).start()
    own_rows = pl.ds(pl.multiple_of(me * kc, kc), kc)
    kv = (f * heads) // (SWA_HEADS // KV_HEADS)
    w_buf[own_rows, starts[2] : starts[4]] = jnp.concatenate(
        [pick(gq_ref, KEY_DIM, f), pick(gk_ref, KEY_DIM, f)], 1
    )
    w_buf[own_rows, starts[4] :] = jnp.concatenate(
        [pick(wk_ref, HEAD_DIM, kv), pick(wv_ref, HEAD_DIM, kv)], 1
    )
    for copy in locals_[:5]:
        copy.wait()

    def sends(k):
        @pl.when((me - k >= 0) & (me + 1 < sp))
        def _():
            l_copy(me - k, 0, k == 0).start()
            w_copy(me - k, 0, k == 0).start()

        @pl.when((me + k < sp) & (me >= 1))
        def _():
            l_copy(me + k, 1, k == 0).start()
            w_copy(me + k, 1, k == 0).start()

        @pl.when((me == k) & (me + 1 < sp))
        def _():
            o_copy(me, 0, True).start()

        @pl.when((sp - 1 - me == k) & (me >= 1))
        def _():
            o_copy(me, 1, True).start()

    for k in range(sp - 1):
        sends(k)

        @pl.when(me - 1 - k >= 0)
        def _():
            l_copy(me - 1 - k, 0, False).wait_recv()
            w_copy(me - 1 - k, 0, False).wait_recv()

        @pl.when(me + 1 + k < sp)
        def _():
            l_copy(me + 1 + k, 1, False).wait_recv()
            w_copy(me + 1 + k, 1, False).wait_recv()

    inner = (me >= 1) & (me + 1 < sp)
    for k in range(1, sp - 1):
        @pl.when(inner & (me - k >= 0))
        def _():
            o_copy(me - k, 0, False).wait_recv()
            o_copy(me - k, 0, False).start()

        @pl.when(inner & (me + k < sp))
        def _():
            o_copy(me + k, 1, False).wait_recv()
            o_copy(me + k, 1, False).start()

    for copy in locals_[5:]:
        copy.wait()
    for i in range(sp):
        @pl.when(i != me)
        def _():
            for copy in pair_copies(i, 1 - side):
                copy.wait_recv()

    for d in range(1, plane):
        tok_copy(d, mine, lax.rem(mine + plane - d, plane)).wait_recv()


    def project(b, _):
        x = x_buf[pl.ds(pl.multiple_of(b * rows, rows), rows)].astype(F32)
        normed = rms_rows(x, ngain_ref[...]).astype(BF)
        p = nn(normed, w_buf[...]).astype(BF)
        proj[b, :, : p.shape[1]] = p
        edge_out[b] = p[rows - WINDOW :, starts[4] : starts[4] + 2 * HEAD_DIM]
        low = nt(normed[:, :kc], l_buf[0])
        for s in range(1, sp):
            low += nt(normed[:, s * kc : (s + 1) * kc], l_buf[s])
        proj[b, :, p.shape[1] : p.shape[1] + low.shape[1]] = low.astype(BF)
        return 0

    lax.fori_loop(0, fs, project, 0)
    edge = remote(edge_out, edge_in, edge_sem.at[0], edge_sem.at[1], {"sp": me + 1})

    @pl.when(me + 1 < sp)
    def _():
        edge.start()

    @pl.when(me == 0)
    def _():
        edge_in[...] = jnp.zeros_like(edge_in)

    nb = rows // SPAN
    low_at = sum(cols)
    lower = (
        lax.broadcasted_iota(jnp.int32, (SPAN, SPAN), 0)
        >= lax.broadcasted_iota(jnp.int32, (SPAN, SPAN), 1)
    )
    tri = lower.astype(F32)
    up = pick(up_ref, KEY_DIM, f)
    bias = pick(bias_ref, KEY_DIM, f)
    sinks = pick(sink_ref, heads, f)
    for b in range(fs):
        low = proj[b, :, low_at : low_at + up_ref.shape[0]]
        z = nn(low, up) + bias
        rate = (jnp.minimum(z, 0.0) - jnp.log1p(jnp.exp(-jnp.abs(z)))) / SOFTMAX_TEMPER
        state = None
        before = jnp.zeros((1, KEY_DIM), F32)
        for n in range(nb):
            r0 = n * SPAN
            within = exact(tri, rate[r0 : r0 + SPAN])
            total = within[SPAN - 1 :]
            v = proj[b, r0 : r0 + SPAN, starts[0] : starts[0] + VALUE_DIM]
            q = proj[b, r0 : r0 + SPAN, starts[2] : starts[2] + KEY_DIM].astype(F32)
            k = proj[b, r0 : r0 + SPAN, starts[3] : starts[3] + KEY_DIM].astype(F32)
            q_dec = q * KEY_DIM**-0.5 * jnp.exp(within)
            k_dec = (k * jnp.exp(-within)).astype(BF)
            k_end = (k * jnp.exp(total - within)).astype(BF)
            scores = jnp.where(lower, nt(q_dec.astype(BF), k_dec), 0.0)
            o = nn(scores.astype(BF), v)
            if state is not None:
                o += nt(q_dec.astype(BF), state.astype(BF))
            local_out[b, r0 : r0 + SPAN] = o
            q_far[b, r0 : r0 + SPAN] = (q_dec * jnp.exp(before)).astype(BF)
            update = tn(v, k_end)
            state = update if state is None else jnp.exp(total) * state + update
            before = before + total
        half = (b % 2) * KEY_DIM
        state_out[b // 2, :VALUE_DIM, half : half + KEY_DIM] = state.astype(BF)
        state_out[b // 2, VALUE_DIM:, half : half + KEY_DIM] = jnp.broadcast_to(
            jnp.exp(before), (16, KEY_DIM)
        ).astype(BF)

    def state_copy(d, sender):
        return remote(
            state_out, state_in.at[sender], state_send.at[d - 1], state_recv.at[sender],
            {"sp": me + d},
        )

    for d in range(1, sp):
        @pl.when(me + d < sp)
        def _():
            state_copy(d, me).start()

    @pl.when(me >= 1)
    def _():
        edge.wait_recv()

    qi = lax.broadcasted_iota(jnp.int32, (WINDOW, 2 * WINDOW), 0)
    ki = lax.broadcasted_iota(jnp.int32, (WINDOW, 2 * WINDOW), 1)
    distance = qi + WINDOW - ki
    inside = (distance >= 0) & (distance < WINDOW)
    for b in range(fs):
        for w in range(rows // WINDOW):
            r0 = w * WINDOW
            here = proj[b, r0 : r0 + WINDOW, starts[4] : starts[4] + 2 * HEAD_DIM]
            if w == 0:
                past = edge_in[b]
                valid = inside & ((ki >= WINDOW) | (me >= 1))
            else:
                past = proj[b, r0 - WINDOW : r0, starts[4] : starts[4] + 2 * HEAD_DIM]
                valid = inside
            band = jnp.concatenate([past, here], 0)
            bk = band[:, :HEAD_DIM]
            bv = band[:, HEAD_DIM:]
            for h in range(heads):
                q0 = starts[1] + h * HEAD_DIM
                q = proj[b, r0 : r0 + WINDOW, q0 : q0 + HEAD_DIM]
                s = jnp.where(valid, nt(q, bk) * HEAD_DIM**-0.5, -1e30)
                sink = sinks[:, h : h + 1]
                top = jnp.maximum(jnp.max(s, -1, keepdims=True), sink)
                e = jnp.exp(s - top)
                den = jnp.sum(e, -1, keepdims=True) + jnp.exp(sink - top)
                a = nn((e / den).astype(BF), bv).astype(BF)
                h0 = VALUE_DIM + h * HEAD_DIM
                hidden[b, r0 : r0 + WINDOW, h0 : h0 + HEAD_DIM] = a

    for i in range(sp - 1):
        @pl.when(i < me)
        def _():
            state_copy(1, i).wait_recv()

        @pl.when(i >= me)
        def _():
            state_in[i] = jnp.zeros(state_in.shape[1:], BF)

    for b in range(fs):
        half = (b % 2) * KEY_DIM
        incoming = jnp.zeros((VALUE_DIM, KEY_DIM), F32)
        for i in range(sp - 1):
            got = state_in[i, b // 2, :VALUE_DIM, half : half + KEY_DIM].astype(F32)
            kept = state_in[i, b // 2, VALUE_DIM : VALUE_DIM + 1, half : half + KEY_DIM].astype(F32)
            incoming = jnp.where(i < me, kept * incoming + got, incoming)
        o = local_out[b] + nt(q_far[b], incoming.astype(BF))
        hidden[b, :, :VALUE_DIM] = rms_rows(o, hgain_ref[...]).astype(BF)

    forward = 2 * me < sp
    nc = o_buf.shape[2]

    def chunk(t):
        return lax.rem(jnp.where(forward, me + t, me - t) + sp, sp)

    def half_copy(s):
        return remote(half_out.at[s], half_in.at[s], half_send.at[s], half_recv.at[s], {"tp": 1 - c})

    def piece_copy(s, d, target):
        return remote(
            piece_out.at[s, d - 1], piece_in.at[s, d - 1],
            piece_send.at[s, d - 1], piece_recv.at[s, d - 1], {"fs": target},
        )

    def produce(t):
        s = chunk(t)

        @pl.when(jnp.logical_not(inner) & (t > 0))
        def _():
            o_copy(s, 0, False).wait_recv()

        w = o_buf[s]
        for b in range(fs):
            part = nn(hidden[b], w)
            lo, hi = part[:own], part[own:]
            half_out[s, b] = jnp.where(c == 0, hi, lo).astype(BF)
            half_own[s, b] = jnp.where(c == 0, lo, hi)
        half_copy(s).start()

    def combine(t):
        s = chunk(t)
        half_copy(s).wait_recv()
        for d in range(1, fs):
            to = lax.rem(f + d, fs)
            piece_out[s, d - 1] = (half_own[s, to] + half_in[s, to].astype(F32)).astype(BF)
            piece_copy(s, d, to).start()
        piece_own[s] = half_own[s, f] + half_in[s, f].astype(F32)

    def finish(t):
        s = chunk(t)
        total = piece_own[s]
        for d in range(1, fs):
            piece_copy(s, d, f).wait_recv()
            total += piece_in[s, d - 1].astype(F32)
        if len(out_ref.shape) == 2:
            out_ref[:, pl.ds(pl.multiple_of(s * nc, nc), nc)] = total.astype(BF)
        else:
            out_ref[s] = total.astype(BF)

    produce(0)

    def steady(t, _):
        produce(t)
        combine(t - 1)
        return 0

    lax.fori_loop(1, sp, steady, 0)
    combine(sp - 1)

    def close(t, _):
        finish(t)
        s = chunk(t)
        half_copy(s).wait_send()
        for d in range(1, fs):
            piece_copy(s, d, f).wait_send()
        return 0

    lax.fori_loop(0, sp, close, 0)

    for k in range(sp - 1):
        @pl.when((me - k >= 0) & (me + 1 < sp))
        def _():
            l_copy(me - k, 0, False).wait_send()
            w_copy(me - k, 0, False).wait_send()
            o_copy(me - k, 0, False).wait_send()

        @pl.when((me + k < sp) & (me >= 1))
        def _():
            l_copy(me + k, 1, False).wait_send()
            w_copy(me + k, 1, False).wait_send()
            o_copy(me + k, 1, False).wait_send()

    for i in range(sp):
        @pl.when(i != me)
        def _():
            for copy in pair_copies(i, side):
                copy.wait_send()

    for d in range(1, plane):
        tok_copy(d, mine, mine).wait_send()

    @pl.when(me + 1 < sp)
    def _():
        edge.wait_send()

    for d in range(1, sp):
        @pl.when(me + d < sp)
        def _():
            state_copy(d, me).wait_send()


def roll_half(a):
    return jnp.concatenate([a[:, a.shape[1] // 2 :], a[:, : a.shape[1] // 2]], 1)


def fold_kernel(
    sizes,
    tok_in,
    gv_ref,
    wq_ref,
    gq_ref,
    gk_ref,
    wk_ref,
    wv_ref,
    low_ref,
    go_ref,
    wo_ref,
    ngain_in,
    up_in,
    bias_in,
    hgain_in,
    sink_in,
    out_ref,
    tok_ref,
    ngain_ref,
    up_ref,
    bias_ref,
    hgain_ref,
    sink_ref,
    x_buf,
    ww,
    wg,
    wl,
    o_buf,
    tiles,
    qw,
    kvb,
    gvb,
    qkb,
    acc,
    acc2,
    og,
    hall,
    lowx,
    fill,
    sc,
    ew,
    decays,
    totals,
    states,
    state_out,
    state_in,
    local_out,
    q_far,
    hidden,
    half_out,
    half_in,
    half_own,
    piece_out,
    piece_in,
    piece_own,
    local_sem,
    l_send,
    l_recv,
    x_send,
    x_recv,
    x_share,
    w_send,
    w_recv,
    p_send,
    p_recv,
    o_send,
    o_recv,
    edge_sem,
    state_sem,
    hid_send,
    hid_recv,
    half_send,
    half_recv,
    piece_send,
    piece_recv,
    g_send,
    g_recv,
    g_rest,
    a_send,
    a_recv,
):
    sp, fs, tp = sizes
    me = lax.axis_index("sp")
    f = lax.axis_index("fs")
    c = lax.axis_index("tp")
    own = tok_in.shape[0]
    rows = own * tp
    kc = gv_ref.shape[0]
    part = kc // 2
    lpart = low_ref.shape[0] // 2
    MESH = pl.DeviceIdType.MESH
    pair = 2 * KEY_DIM
    wide = VALUE_DIM + pair

    slot = lax.rem(me, 2)
    far_slot = 1 - slot
    inner = (me >= 1) & (me + 1 < sp)
    outer = jnp.logical_not(inner)
    middle = 1 + slot
    outside = (sp - 1) * (me - 1)
    buddy = me + 1 - 2 * slot
    third = 2 - me // 2
    fourth = third + 1 - 2 * lax.rem(third, 2)
    chunks = [me, buddy, third, fourth]
    side = lax.rem(f, 2)
    xn = f + 1 - 2 * side
    yn = lax.rem(f + 2, fs)
    n1 = xn * (1 - c) + yn * c
    n2 = xn * c + yn * (1 - c)

    def remote(src, dst, ssem, rsem, target):
        return pltpu.make_async_remote_copy(
            src_ref=src, dst_ref=dst, send_sem=ssem, recv_sem=rsem,
            device_id=target, device_id_type=MESH,
        )

    barrier = pltpu.get_barrier_semaphore()

    def greet(target):
        pl.semaphore_signal(barrier, inc=1, device_id=target, device_id_type=MESH)

    greet({"tp": 1 - c})
    for d in range(1, fs):
        greet({"fs": lax.rem(f + d, fs)})

    @pl.when(me + 1 < sp)
    def _():
        greet({"sp": me + 1})

    @pl.when(me >= 1)
    def _():
        greet({"sp": me - 1})

    def lanes(ref, at, width):
        return ref.at[:, pl.ds(pl.multiple_of(at * width, width), width)]

    def depth(ref, width):
        return ref.at[pl.ds(pl.multiple_of(f * width, width), width)]

    def slice_rows(ref, s):
        return ref.at[pl.ds(pl.multiple_of(s * kc, kc), kc)]

    gd = go_ref.shape[0] // fs
    wd = wo_ref.shape[0] // fs
    heads = sink_in.shape[1] // fs
    wq_cols = heads * HEAD_DIM
    kv = (f * heads) // (SWA_HEADS // KV_HEADS)
    copies_in = [
        (lanes(gq_ref, f // 2, pair), tiles.at[0]),
        (lanes(gk_ref, f // 2, pair), tiles.at[1]),
        (wk_ref, tiles.at[2]),
        (wv_ref, tiles.at[3]),
        (lanes(wq_ref, f, wq_cols), slice_rows(ww, me).at[:, :wq_cols]),
        (lanes(gv_ref, f, VALUE_DIM), slice_rows(wg, me).at[:, :VALUE_DIM]),
        (low_ref, wl.at[me]),
    ]
    nc = o_buf.shape[3]
    for h in range(2):
        cut = pl.ds(h * nc, nc)
        copies_in += [
            (depth(go_ref, gd).at[:, cut], o_buf.at[me, h, pl.ds(0, gd)]),
            (depth(wo_ref, wd).at[:, cut], o_buf.at[me, h, pl.ds(gd, wd)]),
        ]
    copies_in += [
        (ngain_in, ngain_ref),
        (tok_in, tok_ref),
        (up_in, up_ref),
        (bias_in, bias_ref),
        (hgain_in, hgain_ref),
        (sink_in, sink_ref),
    ]
    shared = [0, 0, 0, 0, 1, 2, 3, 4, 4, 4, 4] + list(range(5, 11))
    locals_ = [
        pltpu.make_async_copy(a, b, local_sem.at[i]) for i, (a, b) in zip(shared, copies_in)
    ]

    def local_wait(ref, i):
        pltpu.make_async_copy(ref, ref, local_sem.at[i]).wait()

    for copy in locals_[11:] + locals_[:11]:
        copy.start()

    mine = f * tp + c
    b1, b2, b3 = n1 * tp + c, n2 * tp + c, (fs - 1 - f) * tp + c

    for copy in locals_[11:]:
        copy.wait()
    normed = rms_rows(tok_ref[...].astype(F32), ngain_ref[...]).astype(BF)
    x_buf[slot, pl.ds(pl.multiple_of(mine * own, own), own)] = normed

    def half_block(s, i, h):
        at = pl.multiple_of(i * own + h * (own // 2), own // 2)
        return x_buf.at[s, pl.ds(at, own // 2)]

    def x_copy(s, i, h, target, src):
        ref = half_block(s, i, h)
        return remote(ref, ref, x_send.at[s], x_recv.at[s, src, h], target)

    def x_sib(s, i, h):
        ref = half_block(s, i, h)
        return remote(ref, ref, x_send.at[s], x_share.at[s], SIB)

    def x_bulk(s, n):
        ref = x_buf.at[s, pl.ds(0, n * (own // 2))]
        return remote(ref, ref, x_send.at[s], x_share.at[s], SIB)

    SIB = {"tp": 1 - c}

    def x_first(s, h):
        return [
            x_copy(s, mine, h, {"fs": n1}, 1),
            x_copy(s, mine, h, {"fs": n2}, 2),
            x_sib(s, mine, h),
        ]

    def x_from1(s, h):
        return [x_copy(s, b1, h, {"fs": n2}, 3), x_sib(s, b1, h)]

    def x_out(h):
        return x_copy(slot, mine, h, {"sp": middle}, 0)

    def kv_rows(s, h):
        at = pl.multiple_of(s * kc + h * part, part)
        return ww.at[pl.ds(at, part), wq_cols:]

    def low_rows(s, h):
        return wl.at[s, pl.ds(pl.multiple_of(h * lpart, lpart), lpart)]

    def w_copy(kind, s):
        ref = (
            lambda: slice_rows(ww, s).at[:, :wq_cols],
            lambda: kv_rows(s, side),
            lambda: low_rows(s, c),
            lambda: slice_rows(wg, s),
        )[kind]()
        return remote(ref, ref, w_send.at[kind], w_recv.at[kind, s], {"sp": middle})

    def w_bulk(kind, n):
        ref = (
            lambda: ww.at[pl.ds(0, n * kc), :wq_cols],
            lambda: ww.at[pl.ds(0, n * part), wq_cols:],
            lambda: wl.at[0, pl.ds(0, n * lpart)],
            lambda: wg.at[pl.ds(0, n * kc)],
        )[kind]()
        return remote(ref, ref, w_send.at[kind], w_recv.at[kind, 0], {"sp": middle})

    def kv_share(s, h):
        return remote(kv_rows(s, h), kv_rows(s, h), p_send.at[0], p_recv.at[s], {"fs": xn})

    def low_share(s, h):
        return remote(low_rows(s, h), low_rows(s, h), p_send.at[1], p_recv.at[sp], SIB)

    def share_bulk(i):
        ref = ww.at[pl.ds(0, 3 * part), wq_cols:] if i == 0 else wl.at[pl.ds(0, 3), pl.ds(0, lpart)]
        return remote(ref, ref, p_send.at[i], p_recv.at[sp], SIB)

    def o_copy(way, s, h, d):
        target = {"sp": middle if way == 0 else outside}
        ref = o_buf.at[s, h, pl.ds(d * gd, gd)]
        return remote(ref, ref, o_send.at[way], o_recv.at[s, h, d], target)

    def o_bulk(way, n):
        ref = o_buf.at[pl.ds(0, n)]
        return remote(ref, ref, o_send.at[way], o_recv.at[0, 0, 0], {"sp": middle})

    def o_relay(way, s, h):
        for d in range(2):
            o_copy(0, s, h, d).wait_recv()
            o_copy(way, s, h, d).start()

    quarters = [(h, d) for h in range(2) for d in range(2)]

    def l_copy(i, k, target):
        return remote(lowx.at[i], lowx.at[i], l_send.at[0], l_recv.at[min(k // 3, 1)], target)

    def l_first():
        peers = [{"fs": n1}, {"fs": n2}, {"fs": fs - 1 - f}, SIB]
        return [l_copy(mine, k, peer) for k, peer in enumerate(peers)]

    def l_bulk(n, which):
        return remote(lowx.at[pl.ds(0, n)], lowx.at[pl.ds(0, n)], l_send.at[0], l_recv.at[which], SIB)

    def l_onward():
        return [l_copy(i, 4 + k, SIB) for k, i in enumerate((b1, b2, b3))]

    def start(copies):
        for copy in copies:
            copy.start()

    pl.semaphore_wait(barrier, fs + jnp.where(inner, 2, 1))

    LOW, KV, QUERY, STATE = 2, 1, 0, 3
    locals_[6].wait()
    w_copy(LOW, me).start()

    @pl.when(outer)
    def _():
        for h in range(2):
            x_out(h).start()

    @pl.when(inner)
    def _():
        for h in range(2):
            start(x_first(slot, h))

    local_wait(tiles, 0)
    for copy in locals_[4:6]:
        copy.wait()
    own_rows = pl.ds(pl.multiple_of(me * kc, kc), kc)

    def half_of(i, width, which):
        return jnp.where(which == 0, tiles[i, :, :width], tiles[i, :, width:])

    ww[own_rows, wq_cols:] = jnp.concatenate(
        [half_of(2, HEAD_DIM, kv), half_of(3, HEAD_DIM, kv)], 1
    )
    w_copy(KV, me).start()
    w_copy(QUERY, me).start()
    wg[own_rows, VALUE_DIM:] = jnp.concatenate(
        [half_of(0, KEY_DIM, side), half_of(1, KEY_DIM, side)], 1
    )
    local_wait(o_buf.at[me], 4)

    @pl.when(outer)
    def _():
        w_copy(STATE, me).start()
        for h, d in quarters:
            o_copy(0, me, h, d).start()

    lane = lax.broadcasted_iota(jnp.int32, (rows, pair), 1)
    row = lax.broadcasted_iota(jnp.int32, (rows, pair), 0)
    left = lane < KEY_DIM
    early = row < SPAN
    same = (row < SPAN) == (lane < SPAN)
    diagonal = same & (row >= lane)
    below = (row >= SPAN) & (lane < SPAN)

    def edge_rows(i, h):
        n = fs * rows // 2
        return kvb.at[i, pl.ds(pl.multiple_of(h * n, n), n)]

    edge = remote(
        edge_rows(2, side), edge_rows(0, side), edge_sem.at[0], edge_sem.at[1], {"sp": me + 1}
    )

    def edge_share(h):
        return remote(
            edge_rows(0, h), edge_rows(0, h), edge_sem.at[2], edge_sem.at[3], {"fs": xn}
        )
    state = remote(state_out, state_in, state_sem.at[0], state_sem.at[1], {"sp": me + 1})

    def hid_part(s, i):
        return hidden.at[s, :, i * VALUE_DIM : (i + 1) * VALUE_DIM]

    def hid_copy(i, s):
        return remote(
            hid_part(s, i), hid_part(s, i), hid_send.at[i], hid_recv.at[i], {"sp": outside}
        )

    def seq(b):
        if isinstance(b, int):
            return pl.ds(b * rows, rows)
        return pl.ds(pl.multiple_of(b * rows, rows), rows)

    @pl.when(inner)
    def _():
        for h, d in quarters:
            o_copy(1, me, h, d).start()

        def arrive(kind, s, onward):
            w_copy(kind, s).wait_recv()
            if onward:
                w_copy(kind, s).start()
            if kind == LOW:
                low_share(s, c).start()
            if kind == KV:
                kv_share(s, side).start()

        def neighbours(s, h):
            x_copy(s, b1, h, SIB, 1).wait_recv()
            start(x_from1(s, h))
            x_copy(s, b2, h, SIB, 2).wait_recv()
            x_sib(s, b2, h).start()

        def corner(s):
            for h in range(2):
                x_copy(s, b3, h, SIB, 3).wait_recv()
                x_sib(s, b3, h).start()

        def siblings(s):
            x_bulk(s, 2 * fs).wait_recv()

        def columns(s):
            return pl.ds(pl.multiple_of(s * kc, kc), kc)

        bs = [bias_ref[:, i * KEY_DIM : (i + 1) * KEY_DIM] for i in range(fs)]
        ups = [up_ref[:, i * KEY_DIM : (i + 1) * KEY_DIM] for i in range(fs)]
        bias, up = bs[0], ups[0]
        for i in range(1, fs):
            bias = jnp.where(f == i, bs[i], bias)
            up = jnp.where(f == i, ups[i], up)
        up_l = jnp.concatenate([up, jnp.zeros_like(up)], 1)
        up_r = jnp.concatenate([jnp.zeros_like(up), up], 1)
        bias2 = jnp.concatenate([bias, bias], 1)

        def own_low():
            at = pl.ds(pl.multiple_of(mine * own, own), own)
            x = jnp.concatenate([x_buf[slot, at], x_buf[far_slot, at]], 0)
            low = nt(wl[0], x[:, :kc])
            for j in range(1, sp):
                low += nt(wl[j], x[:, j * kc : (j + 1) * kc])
            lowx[mine] = low.astype(BF)

        def gate(p):
            pre = []
            for i in range(tp):
                z = tn(lowx[2 * p * tp + i], up_l) + tn(lowx[(2 * p + 1) * tp + i], up_r)
                pre.append(z + bias2)
            return [
                jnp.concatenate([z[k * own : (k + 1) * own] for z in pre], 0) for k in range(2)
            ]

        def decay():
            tri = diagonal.astype(F32)
            for p in range(fs // 2):
                for s, z in zip((slot, far_slot), gate(p)):
                    decay_of(s, p, z, tri)

        def decay_of(s, p, z, tri):
            rate = (jnp.minimum(z, 0.0) - jnp.log1p(jnp.exp(-jnp.abs(z)))) / SOFTMAX_TEMPER
            within = exact(tri, rate)
            t0, t1 = within[SPAN - 1 : SPAN], within[rows - 1 :]
            grow = jnp.exp(within) * KEY_DIM**-0.5
            end = jnp.exp(jnp.where(early, t0, t1) - within)
            decays[s, p, 0] = grow
            decays[s, p, 1] = jnp.exp(-within)
            decays[s, p, 2] = end
            decays[s, p, 3] = grow * jnp.where(early, 1.0, jnp.exp(t0))
            decays[s, p, 4] = end * jnp.where(early, jnp.exp(t1), 1.0)
            totals[s, p] = jnp.broadcast_to(jnp.exp(t0 + t1), totals.shape[2:])

        def window_maps(s, slices):
            total = nn(x_buf[s, :, columns(slices[0])], slice_rows(ww, slices[0])[...])
            for j in slices[1:]:
                total += nn(x_buf[s, :, columns(j)], slice_rows(ww, j)[...])
            return total

        def state_maps(s, slices):
            total = nn(x_buf[s, :, columns(slices[0])], slice_rows(wg, slices[0])[...])
            for j in slices[1:]:
                total += nn(x_buf[s, :, columns(j)], slice_rows(wg, j)[...])
            return total

        def place(s, p):
            q = p[:, :wq_cols].astype(BF).astype(F32) * HEAD_DIM**-0.5
            for h in range(heads):
                qh = jnp.where(left_all, q if h == 0 else roll_half(q), 0.0)
                qw[s, h] = qh.astype(BF)
            kvb[s + 1] = p[:, wq_cols:].astype(BF)

        left_all = lax.broadcasted_iota(jnp.int32, (fs * rows, pair), 1) < KEY_DIM
        tall = heads * WINDOW
        qi = lax.broadcasted_iota(jnp.int32, (tall, 2 * WINDOW), 0)
        ki = lax.broadcasted_iota(jnp.int32, (tall, 2 * WINDOW), 1)
        distance = lax.rem(qi, WINDOW) + WINDOW - ki
        inside = (distance >= 0) & (distance < WINDOW)
        sinks = sink_ref[:, :heads]
        for i in range(1, fs):
            sinks = jnp.where(f == i, sink_ref[:, i * heads : (i + 1) * heads], sinks)
        sink = sinks[:, :1]
        for h in range(1, heads):
            sink = jnp.where(qi < h * WINDOW, sink, sinks[:, h : h + 1])
        fill[...] = jnp.where(ki == 0, sink, -1e30)
        key_row = lax.broadcasted_iota(jnp.int32, (2 * WINDOW, pair), 0)
        key_lane = lax.broadcasted_iota(jnp.int32, (2 * WINDOW, pair), 1)

        @pl.when(me == 1)
        def _():
            kvb[0] = jnp.zeros(kvb.shape[1:], BF)
            state_in[...] = jnp.zeros_like(state_in)

        def far_rows(h):
            x_copy(far_slot, mine, h, SIB, 0).wait_recv()
            start(x_first(far_slot, h))

        arrive(LOW, buddy, True)
        w_copy(STATE, me).start()
        o_copy(0, me, 0, 0).start()
        arrive(LOW, third, False)
        arrive(KV, third, False)
        neighbours(slot, 0)
        far_rows(0)
        arrive(LOW, fourth, False)
        neighbours(slot, 1)
        far_rows(1)
        share_bulk(1).wait_recv()
        own_low()
        start(l_first())
        arrive(KV, buddy, True)
        neighbours(far_slot, 0)
        arrive(QUERY, buddy, True)
        o_copy(0, me, 0, 1).start()
        corner(slot)
        siblings(slot)
        arrive(QUERY, third, False)
        kv_share(third, 1 - side).wait_recv()
        acc[slot] = window_maps(slot, (me, third))
        neighbours(far_slot, 1)
        arrive(STATE, buddy, True)
        arrive(KV, fourth, False)
        l_bulk(3, 0).wait_recv()
        start(l_onward())
        l_bulk(4, 1).wait_recv()
        decay()
        w_copy(STATE, third).wait_recv()
        acc2[slot] = state_maps(slot, chunks[:3])
        o_relay(1, third, 0)
        corner(far_slot)
        arrive(QUERY, fourth, False)
        kv_share(buddy, 1 - side).wait_recv()
        kv_share(fourth, 1 - side).wait_recv()

        place(slot, acc[slot] + window_maps(slot, (buddy, fourth)))

        @pl.when(me == 1)
        def _():
            edge.start()

        o_copy(0, me, 1, 0).start()

        @pl.when(me > 1)
        def _():
            o_copy(0, me, 1, 1).start()

        siblings(far_slot)
        place(far_slot, window_maps(far_slot, chunks))

        def window(s):
            valid = inside & ((ki >= WINDOW) | (me > 1) | (s > 0))
            bands = [jnp.concatenate([kvb[s, seq(b)], kvb[s + 1, seq(b)]], 0) for b in range(fs)]
            for b in range(fs):
                q = jnp.concatenate([qw[s, h, seq(b)] for h in range(heads)], 0)
                sc[b] = jnp.where(valid, nt(q, bands[b]), fill[...])
            for b in range(fs):
                near = sc[b]
                top = jnp.max(near, -1, keepdims=True)
                ew[b] = jnp.exp(near - top).astype(BF)
            for b in range(fs):
                band = jnp.concatenate([kvb[s, seq(b)], kvb[s + 1, seq(b)]], 0).astype(F32)
                values = jnp.where(
                    key_lane < HEAD_DIM, 1.0, jnp.where(key_row == 0, 0.0, band)
                ).astype(BF)
                both = nn(ew[b], values)
                turned = roll_half(both)
                first = turned[:WINDOW] / both[:WINDOW]
                second = both[WINDOW:] / turned[WINDOW:]
                hidden[s, seq(b), VALUE_DIM:] = jnp.where(left, first, second).astype(BF)

        window(far_slot)
        hid_copy(1, far_slot).start()
        acc2[far_slot] = state_maps(far_slot, chunks[:3])

        @pl.when(me > 1)
        def _():
            edge.wait_recv()
            edge_share(side).start()

        w_copy(STATE, fourth).wait_recv()

        for s in range(2):
            p = (acc2[s] + state_maps(s, chunks[3:])).astype(BF)
            gvb[s] = p[:, :VALUE_DIM]
            qkb[s] = p[:, VALUE_DIM:].astype(F32)

        def keys(s, p):
            return jnp.where(left, roll_half(qkb[s, seq(2 * p)]), qkb[s, seq(2 * p + 1)])

        def queries(s, p):
            return jnp.where(left, qkb[s, seq(2 * p)], roll_half(qkb[s, seq(2 * p + 1)]))

        for s in range(2):
            for p in range(fs // 2):
                k_far = (keys(s, p) * decays[s, p, 4]).astype(BF)
                states[s, p] = jnp.where(
                    left, tn(gvb[s, seq(2 * p)], k_far), tn(gvb[s, seq(2 * p + 1)], k_far)
                )
        for p in range(fs // 2):
            state_out[p] = (totals[1, p, :1] * states[0, p] + states[1, p]).astype(BF)

        @pl.when(me == 1)
        def _():
            state.start()

        for s in range(2):
            for p in range(fs // 2):
                k = keys(s, p)
                q = queries(s, p)
                qd = q * decays[s, p, 0]
                qf = q * decays[s, p, 3]
                kd = (k * decays[s, p, 1]).astype(BF)
                ke = (k * decays[s, p, 2]).astype(BF)
                for j in range(2):
                    here = left if j == 0 else jnp.logical_not(left)
                    qj = jnp.where(here, qd, 0.0).astype(BF)
                    scores = jnp.where(
                        diagonal, nt(qj, kd), jnp.where(below, nt(qj, ke), 0.0)
                    ).astype(BF)
                    local_out[s, seq(2 * p + j)] = nn(scores, gvb[s, seq(2 * p + j)])
                    q_far[s, seq(2 * p + j)] = jnp.where(here, qf, 0.0).astype(BF)

        @pl.when(me == 1)
        def _():
            o_copy(0, me, 1, 1).start()

        for h in range(2):
            o_relay(0, buddy, h)

        @pl.when(me > 1)
        def _():
            edge_share(1 - side).wait_recv()
            window(slot)
            state.wait_recv()

        def finish_state(s):
            for p in range(fs // 2):
                arrived = state_in[p].astype(F32)
                entering = jnp.where(s == 0, arrived, totals[0, p, :1] * arrived + states[0, p])
                entering = entering.astype(BF)
                for j in range(2):
                    b = 2 * p + j
                    o = local_out[s, seq(b)] + nt(q_far[s, seq(b)], entering)
                    hidden[s, seq(b), :VALUE_DIM] = rms_rows(o, hgain_ref[...]).astype(BF)

        finish_state(far_slot)
        hid_copy(0, far_slot).start()
        finish_state(slot)

        @pl.when(me == 1)
        def _():
            window(slot)

    def g_copy(k, j, g, h, target):
        ref = og.at[j, g, h]
        into = g_recv.at[j, h] if k == 0 else g_rest.at[0]
        return remote(ref, ref, g_send.at[0], into, target)

    def g_bulk(n, ssem):
        ref = og.at[:, pl.ds(0, n)]
        return remote(ref, ref, ssem.at[0], g_rest.at[0], SIB)

    corner_f = fs - 1 - f

    def g_first(j, h):
        return [g_copy(0, j, f, h, {"fs": n1}), g_copy(1, j, f, h, {"fs": n2})]

    def g_relay(j, h):
        return g_copy(2, j, n1, h, {"fs": n2})

    def a_part(g, i):
        return hidden.at[slot, seq(g), i * VALUE_DIM : (i + 1) * VALUE_DIM]

    def a_copy(k, i):
        g = (n1, n2, corner_f)[k]
        here = hall.at[f, :, i * VALUE_DIM : (i + 1) * VALUE_DIM]
        return remote(a_part(g, i), here, a_send.at[0], a_recv.at[0], {"fs": g})

    def a_bulk():
        ref = hall.at[pl.ds(0, fs - 1)]
        return remote(ref, ref, a_send.at[0], a_recv.at[0], {"fs": n1})

    @pl.when(outer)
    def _():
        for h in range(2):
            og[0, f, h] = o_buf[me, h]
            start(g_first(0, h))
        for h in range(2):
            for d in range(2):
                o_copy(0, buddy, h, d).wait_recv()
            og[1, f, h] = o_buf[buddy, h]
        for j in range(2):
            for h in range(2):
                g_copy(0, j, n1, h, SIB).wait_recv()
                g_relay(j, h).start()
                if j == 0:
                    start(g_first(1, h))
        g_bulk(2, g_send).wait_recv()
        for i in (1, 0):
            hid_copy(i, slot).wait_recv()
            for k in range(3):
                a_copy(k, i).start()
        hall[f] = hidden[slot, seq(f)]

    parts = [(s, h) for s in chunks for h in range(2)]

    def half_copy(s, h):
        return remote(
            half_out.at[s, h], half_in.at[s, h], half_send.at[0], half_recv.at[s, h], SIB
        )

    def piece_copy(s, h, d, target):
        return remote(
            piece_out.at[s, h, d - 1], piece_in.at[s, h, d - 1],
            piece_send.at[0], piece_recv.at[s, h], {"fs": target},
        )

    def produce(t):
        s, h = parts[t]
        if 4 <= t < 6:
            @pl.when(outer)
            def _():
                for d in range(2):
                    o_copy(0, s, h, d).wait_recv()
        if t >= 6:
            for d in range(2):
                o_copy(0, s, h, d).wait_recv()

                @pl.when(inner)
                def _():
                    o_copy(1, s, h, d).start()

        w = o_buf[s, h]
        for b in range(fs):
            partial = nn(hidden[slot, seq(b)], w)
            lo, hi = partial[:own], partial[own:]
            half_out[s, h, b] = jnp.where(c == 0, hi, lo).astype(BF)
            half_own[s, h, b] = jnp.where(c == 0, lo, hi)
        half_copy(s, h).start()

    def combine(t):
        s, h = parts[t]
        half_copy(s, h).wait_recv()
        for d in range(1, fs):
            to = lax.rem(f + d, fs)
            piece_out[s, h, d - 1] = (half_own[s, h, to] + half_in[s, h, to].astype(F32)).astype(BF)
            piece_copy(s, h, d, to).start()
        piece_own[s, h] = half_own[s, h, f] + half_in[s, h, f].astype(F32)

    def store(t, total):
        s, h = parts[t]
        at = pl.ds(pl.multiple_of((2 * s + h) * nc, nc), nc)
        out_ref[:, at] = total.astype(BF)

    def finish(t):
        s, h = parts[t]
        total = piece_own[s, h]
        remote(
            piece_out.at[s, h], piece_in.at[s, h], piece_send.at[0], piece_recv.at[s, h], SIB
        ).wait_recv()
        for d in range(1, fs):
            total += piece_in[s, h, d - 1].astype(F32)
        store(t, total)

    def whole_copy(s, h):
        return remote(
            half_out.at[s, h, 0], half_in.at[s, h, 0], half_send.at[1], half_recv.at[s, h], SIB
        )

    def produce_whole(t):
        s, h = parts[t]
        total = nn(hall[0], og[t // 2, 0, h])
        for g in range(1, fs):
            total += nn(hall[g], og[t // 2, g, h])
        lo, hi = total[:own], total[own:]
        half_out[s, h, 0] = jnp.where(c == 0, hi, lo).astype(BF)
        half_own[s, h, 0] = jnp.where(c == 0, lo, hi)
        whole_copy(s, h).start()

    def finish_whole(t):
        s, h = parts[t]
        whole_copy(s, h).wait_recv()
        store(t, half_own[s, h, 0] + half_in[s, h, 0].astype(F32))

    def tail_sent(n):
        ref = half_out.at[pl.ds(0, n)]
        remote(ref, ref, half_send.at[0], half_recv.at[0, 0], SIB).wait_send()
        ref = piece_out.at[pl.ds(0, n)]
        remote(ref, ref, piece_send.at[0], piece_recv.at[0, 0], SIB).wait_send()

    @pl.when(inner)
    def _():
        produce(0)
        for t in range(1, 2 * sp):
            produce(t)
            combine(t - 1)
            if t == 2:
                o_relay(1, third, 1)
        combine(2 * sp - 1)
        for t in range(2 * sp):
            finish(t)
        tail_sent(sp)

    @pl.when(outer)
    def _():
        produce(4)
        combine(4)
        a_bulk().wait_recv()
        for t in range(4):
            produce_whole(t)
        for t in range(4):
            finish_whole(t)
        for t in range(5, 2 * sp):
            produce(t)
            combine(t)
        for t in range(4, 2 * sp):
            finish(t)
        tail_sent(sp // 2)
        ref = half_out.at[0, 0]
        remote(ref, ref, half_send.at[1], half_recv.at[0, 0], SIB).wait_send()
        g_bulk(3, g_send).wait_send()
        a_bulk().wait_send()

    @pl.when(outer)
    def _():
        x_bulk(slot, 2).wait_send()
        for kind in range(4):
            w_bulk(kind, 1).wait_send()
        o_bulk(0, 1).wait_send()

    @pl.when(inner)
    def _():
        for s in range(2):
            x_bulk(s, 14).wait_send()
        l_bulk(7, 0).wait_send()
        for kind in range(4):
            w_bulk(kind, 2).wait_send()
        share_bulk(0).wait_send()
        share_bulk(1).wait_send()
        o_bulk(0, 2).wait_send()
        o_bulk(1, 3).wait_send()
        for i in range(2):
            hid_copy(i, far_slot).wait_send()

        @pl.when(me == 1)
        def _():
            edge.wait_send()
            state.wait_send()

        @pl.when(me > 1)
        def _():
            edge_share(side).wait_send()


def fold_call(sizes, operands):
    sp, fs, tp = sizes
    own, d = operands[0].shape
    rows = own * tp
    kc = operands[1].shape[0]
    rank = operands[7].shape[0]
    depth = (operands[8].shape[0] + operands[9].shape[0]) // fs
    nc = operands[8].shape[1]
    pair = 2 * KEY_DIM
    all_rows = fs * rows
    pairs = fs // 2
    vm = pltpu.VMEM
    dma = pltpu.SemaphoreType.DMA
    small = [(o.shape, o.dtype) for o in operands[10:]]
    scratch = [
        vm((own, d), BF),
        *(vm(shape, dtype) for shape, dtype in small),
        vm((2, all_rows, d), BF),
        vm((d, 2 * pair), BF),
        vm((d, VALUE_DIM + pair), BF),
        vm((sp, rank, kc), BF),
        vm((sp, 2, depth, nc // 2), BF),
        vm((4, kc, pair), BF),
        vm((2, 2, all_rows, pair), BF),
        vm((3, all_rows, pair), BF),
        vm((2, all_rows, VALUE_DIM), BF),
        vm((2, all_rows, pair), F32),
        vm((2, all_rows, 2 * pair), F32),
        vm((2, all_rows, VALUE_DIM + pair), F32),
        vm((2, fs, 2, depth, nc // 2), BF),
        vm((fs, rows, depth), BF),
        vm((fs * tp, rank, 2 * own), BF),
        vm((2 * WINDOW, 2 * WINDOW), F32),
        vm((fs, 2 * WINDOW, 2 * WINDOW), F32),
        vm((fs, 2 * WINDOW, 2 * WINDOW), BF),
        vm((2, pairs, 5, rows, pair), F32),
        vm((2, pairs, 8, pair), F32),
        vm((2, pairs, VALUE_DIM, pair), F32),
        vm((pairs, VALUE_DIM, pair), BF),
        vm((pairs, VALUE_DIM, pair), BF),
        vm((2, all_rows, VALUE_DIM), F32),
        vm((2, all_rows, pair), BF),
        vm((2, all_rows, depth), BF),
        vm((sp, 2, fs, own, nc // 2), BF),
        vm((sp, 2, fs, own, nc // 2), BF),
        vm((sp, 2, fs, own, nc // 2), F32),
        vm((sp, 2, fs - 1, own, nc // 2), BF),
        vm((sp, 2, fs - 1, own, nc // 2), BF),
        vm((sp, 2, own, nc // 2), F32),
        dma((11,)),
        dma((1,)),
        dma((2,)),
        dma((2,)),
        dma((2, 4, 2)),
        dma((2,)),
        dma((4,)),
        dma((4, sp)),
        dma((2,)),
        dma((sp + 1,)),
        dma((2,)),
        dma((sp, 2, 2)),
        dma((4,)),
        dma((2,)),
        dma((2,)),
        dma((2,)),
        dma((2,)),
        dma((sp, 2)),
        dma((1,)),
        dma((sp, 2)),
        dma((1,)),
        dma((2, 2)),
        dma((1,)),
        dma((1,)),
        dma((1,)),
    ]
    anywhere = pl.BlockSpec(memory_space=pl.ANY)
    return pl.pallas_call(
        functools.partial(fold_kernel, sizes),
        out_shape=pltpu.VMEM((own, sp * nc), BF),
        in_specs=[anywhere] * 15,
        out_specs=pl.BlockSpec(memory_space=pltpu.VMEM),
        scratch_shapes=scratch,
        compiler_params=pltpu.CompilerParams(
            has_side_effects=True, vmem_limit_bytes=60 * 1024 * 1024, collective_id=0
        ),
    )(*operands)


def folds(sp, fs, tp, shape, rows, kc, width, rank, nc, depth):
    whole_rows = rows == WINDOW == 2 * SPAN
    lanes_fit = nc % 256 == 0 and kc % 128 == 0 and depth == 2 * VALUE_DIM and 2 * HEAD_DIM == 2 * KEY_DIM
    return sp == 4 and fs == 4 and tp == 2 and whole_rows and lanes_fit and rank % 32 == 0


def per_device(
    tokens,
    norm_gain,
    gla_query_weight,
    gla_key_weight,
    gla_value_weight,
    decay_down,
    decay_up,
    decay_bias,
    head_gain,
    window_query_weight,
    window_key_weight,
    window_value_weight,
    sink_logit,
    gla_output_weight,
    window_output_weight,
):
    fs, tp, sp = (lax.axis_size(n) for n in ("fs", "tp", "sp"))
    low = decay_down.T
    own = tokens.shape[1]
    rows = own * tp
    kc = decay_down.shape[0]
    width = VALUE_DIM + 4 * HEAD_DIM + 2 * KEY_DIM
    rank = low.shape[0]
    depth = (gla_output_weight.shape[0] + window_output_weight.shape[0]) // fs
    nc = gla_output_weight.shape[1]
    flat = nc % 128 == 0
    operands = (
        tokens[0],
        gla_value_weight,
        window_query_weight,
        gla_query_weight,
        gla_key_weight,
        window_key_weight,
        window_value_weight,
        low,
        gla_output_weight,
        window_output_weight,
        norm_gain[None],
        decay_up,
        decay_bias[None],
        head_gain[None],
        sink_logit[None],
    )
    if folds(sp, fs, tp, tokens.shape, rows, kc, width, rank, nc, depth):
        return fold_call((sp, fs, tp), operands).reshape(1, own, sp * nc)
    vm = pltpu.VMEM
    dma = pltpu.SemaphoreType.DMA
    scratch = [
        vm((fs * rows, tokens.shape[2]), BF),
        vm((sp * kc, width), BF),
        vm((sp, rank, kc), BF),
        vm((sp, depth, nc), BF),
        vm((fs, rows, width + 128), BF),
        vm((fs, WINDOW, 2 * HEAD_DIM), BF),
        vm((fs, WINDOW, 2 * HEAD_DIM), BF),
        vm((fs // 2, VALUE_DIM + 16, 2 * KEY_DIM), BF),
        vm((sp, fs // 2, VALUE_DIM + 16, 2 * KEY_DIM), BF),
        vm((fs, rows, VALUE_DIM), F32),
        vm((fs, rows, KEY_DIM), BF),
        vm((fs, rows, depth), BF),
        vm((sp, fs, own, nc), BF),
        vm((sp, fs, own, nc), BF),
        vm((sp, fs, own, nc), F32),
        vm((sp, fs - 1, own, nc), BF),
        vm((sp, fs - 1, own, nc), BF),
        vm((sp, own, nc), F32),
        dma((6,)),
        dma((fs * tp - 1,)),
        dma((fs * tp - 1,)),
        dma((2, sp)),
        dma((sp,)),
        dma((2, sp)),
        dma((sp,)),
        dma((2, sp)),
        dma((sp,)),
        dma((sp,)),
        dma((sp,)),
        dma((sp,)),
        dma((sp,)),
        dma((2, sp)),
        dma((sp,)),
        dma((2,)),
        dma((sp,)),
        dma((sp,)),
        dma((sp,)),
        dma((sp,)),
        dma((sp, fs - 1)),
        dma((sp, fs - 1)),
    ]
    spec = pl.BlockSpec(memory_space=pltpu.VMEM)
    anywhere = pl.BlockSpec(memory_space=pl.ANY)
    mixed = pl.pallas_call(
        functools.partial(mixer_kernel, (sp, fs, tp)),
        out_shape=jax.ShapeDtypeStruct((own, sp * nc) if flat else (sp, own, nc), BF),
        in_specs=[
            anywhere if i in (1, 2, 8, 9) else spec for i in range(15)
        ],
        out_specs=spec,
        scratch_shapes=scratch,
        compiler_params=pltpu.CompilerParams(
            has_side_effects=True, vmem_limit_bytes=60 * 1024 * 1024
        ),
    )(*operands)
    return (mixed if flat else mixed.transpose(1, 0, 2)).reshape(1, own, sp * nc)


def solution(mesh):
    in_specs = (
        P("fs", ("sp", "tp"), None),
        P(),
        P("sp", "tp"),
        P("sp", "tp"),
        P("sp", "tp"),
        P("sp", None),
        P(None, "tp"),
        P("tp"),
        P(),
        P("sp", "tp"),
        P("sp", "tp"),
        P("sp", "tp"),
        P("tp"),
        P("tp", "sp"),
        P("tp", "sp"),
    )
    out_specs = P("fs", ("sp", "tp"), None)
    return jax.shard_map(
        per_device, mesh=mesh, in_specs=in_specs, out_specs=out_specs, check_vma=False
    )
```

```python
import functools

import jax
import jax.numpy as jnp
from jax import lax
from jax.experimental import pallas as pl
from jax.experimental.pallas import tpu as pltpu
from jax.sharding import PartitionSpec as P

KEY_DIM = 64
VALUE_DIM = 128
SWA_HEADS = 16
KV_HEADS = 4
HEAD_DIM = 64
WINDOW = 128
SPAN = 64

EPS = 1e-06
SOFTMAX_TEMPER = 16.0
BF = jnp.bfloat16
F32 = jnp.float32


def rms_rows(values, gain):
    mean_square = jnp.mean(values * values, axis=-1, keepdims=True)
    return values * lax.rsqrt(mean_square + EPS) * gain


def nt(a, b):
    return lax.dot_general(a, b, (((1,), (1,)), ((), ())), preferred_element_type=F32)


def nn(a, b):
    return lax.dot_general(a, b, (((1,), (0,)), ((), ())), preferred_element_type=F32)


def tn(a, b):
    return lax.dot_general(a, b, (((0,), (0,)), ((), ())), preferred_element_type=F32)


def exact(a, b):
    return lax.dot_general(
        a, b, (((1,), (0,)), ((), ())), precision=lax.Precision.HIGHEST, preferred_element_type=F32
    )


def mixer_kernel(
    sizes,
    tok_ref,
    gv_ref,
    wq_ref,
    gq_ref,
    gk_ref,
    wk_ref,
    wv_ref,
    low_ref,
    go_ref,
    wo_ref,
    ngain_ref,
    up_ref,
    bias_ref,
    hgain_ref,
    sink_ref,
    out_ref,
    x_buf,
    w_buf,
    l_buf,
    o_buf,
    proj,
    edge_out,
    edge_in,
    state_out,
    state_in,
    local_out,
    q_far,
    hidden,
    half_out,
    half_in,
    half_own,
    piece_out,
    piece_in,
    piece_own,
    local_sem,
    tok_send,
    tok_recv,
    w_send,
    w_recv,
    l_send,
    l_recv,
    v_send,
    v_recv,
    vp_send,
    vp_recv,
    lp_send,
    lp_recv,
    o_send,
    o_recv,
    edge_sem,
    state_send,
    state_recv,
    half_send,
    half_recv,
    piece_send,
    piece_recv,
):
    sp, fs, tp = sizes
    me = lax.axis_index("sp")
    f = lax.axis_index("fs")
    c = lax.axis_index("tp")
    plane = fs * tp
    mine = f * tp + c
    own = tok_ref.shape[0]
    rows = own * tp
    kc = gv_ref.shape[0]
    MESH = pl.DeviceIdType.MESH

    def remote(src, dst, ssem, rsem, target):
        return pltpu.make_async_remote_copy(
            src_ref=src, dst_ref=dst, send_sem=ssem, recv_sem=rsem,
            device_id=target, device_id_type=MESH,
        )

    def w_rows(s):
        return w_buf.at[pl.ds(pl.multiple_of(s * kc, kc), kc)]

    def w_copy(s, way, first):
        target = {"sp": me + (1 if way == 0 else -1)}
        return remote(
            w_main(s), w_main(s), w_send.at[way, s], w_recv.at[s], target
        )

    side = f % 2
    part = kc // 2
    lpart = low_ref.shape[0] // 2

    def w_main(s):
        return w_rows(s).at[:, : starts[4]]

    def v_rows(s, h):
        at = pl.multiple_of(s * kc + h * part, part)
        return w_buf.at[pl.ds(at, part), starts[4] : starts[4] + 2 * HEAD_DIM]

    def l_rows(s, h):
        return l_buf.at[s, pl.ds(pl.multiple_of(h * lpart, lpart), lpart)]

    def v_copy(s, way):
        target = {"sp": me + (1 if way == 0 else -1)}
        return remote(v_rows(s, side), v_rows(s, side), v_send.at[way, s], v_recv.at[s], target)

    def lh_copy(s, way):
        target = {"sp": me + (1 if way == 0 else -1)}
        return remote(l_rows(s, side), l_rows(s, side), l_send.at[way, s], l_recv.at[s], target)

    def pair_copies(s, h):
        target = {"fs": f + 1 - 2 * side}
        return (
            remote(v_rows(s, h), v_rows(s, h), vp_send.at[s], vp_recv.at[s], target),
            remote(l_rows(s, h), l_rows(s, h), lp_send.at[s], lp_recv.at[s], target),
        )

    class l_copy:
        def __init__(self, s, way, first):
            self.s = s
            self.both = (v_copy(s, way), lh_copy(s, way))

        def start(self):
            for copy in self.both:
                copy.start()

        def wait_recv(self):
            for copy, onward in zip(self.both, pair_copies(self.s, side)):
                copy.wait_recv()
                onward.start()

        def wait_send(self):
            for copy in self.both:
                copy.wait_send()

    def o_copy(s, way, first):
        target = {"sp": me + (1 if way == 0 else -1)}
        return remote(
            o_buf.at[s], o_buf.at[s], o_send.at[way, s], o_recv.at[s], target
        )

    def tok_rows(i):
        return x_buf.at[pl.ds(pl.multiple_of(i * own, own), own)]

    def tok_copy(d, peer, sender):
        return remote(
            tok_ref, tok_rows(sender), tok_send.at[d - 1], tok_recv.at[d - 1],
            {"fs": peer // tp, "tp": peer % tp},
        )

    def pick(ref, width, which):
        value = ref[:, :width]
        for i in range(1, ref.shape[1] // width):
            value = jnp.where(which == i, ref[:, i * width : (i + 1) * width], value)
        return value

    def lanes(ref, width):
        return ref.at[:, pl.ds(pl.multiple_of(f * width, width), width)]

    def depth(ref, width):
        return ref.at[pl.ds(pl.multiple_of(f * width, width), width)]

    cols = [VALUE_DIM, 2 * HEAD_DIM, KEY_DIM, KEY_DIM, HEAD_DIM, HEAD_DIM]
    starts = [sum(cols[:i]) for i in range(len(cols))]
    gd = go_ref.shape[0] // fs
    wd = wo_ref.shape[0] // fs
    heads = sink_ref.shape[1] // fs
    copies_in = [
        (lanes(gv_ref, cols[0]), w_rows(me).at[:, : cols[0]]),
        (lanes(wq_ref, cols[1]), w_rows(me).at[:, starts[1] : starts[2]]),
        (depth(go_ref, gd), o_buf.at[me, pl.ds(0, gd)]),
        (depth(wo_ref, wd), o_buf.at[me, pl.ds(gd, wd)]),
        (low_ref, l_buf.at[me]),
        (tok_ref, tok_rows(mine)),
    ]
    locals_ = [
        pltpu.make_async_copy(a, b, local_sem.at[i]) for i, (a, b) in enumerate(copies_in)
    ]
    for copy in locals_:
        copy.start()
    for d in range(1, plane):
        tok_copy(d, lax.rem(mine + d, plane), mine).start()
    own_rows = pl.ds(pl.multiple_of(me * kc, kc), kc)
    kv = (f * heads) // (SWA_HEADS // KV_HEADS)
    w_buf[own_rows, starts[2] : starts[4]] = jnp.concatenate(
        [pick(gq_ref, KEY_DIM, f), pick(gk_ref, KEY_DIM, f)], 1
    )
    w_buf[own_rows, starts[4] :] = jnp.concatenate(
        [pick(wk_ref, HEAD_DIM, kv), pick(wv_ref, HEAD_DIM, kv)], 1
    )
    for copy in locals_[:5]:
        copy.wait()

    def sends(k):
        @pl.when((me - k >= 0) & (me + 1 < sp))
        def _():
            l_copy(me - k, 0, k == 0).start()
            w_copy(me - k, 0, k == 0).start()

        @pl.when((me + k < sp) & (me >= 1))
        def _():
            l_copy(me + k, 1, k == 0).start()
            w_copy(me + k, 1, k == 0).start()

        @pl.when((me == k) & (me + 1 < sp))
        def _():
            o_copy(me, 0, True).start()

        @pl.when((sp - 1 - me == k) & (me >= 1))
        def _():
            o_copy(me, 1, True).start()

    for k in range(sp - 1):
        sends(k)

        @pl.when(me - 1 - k >= 0)
        def _():
            l_copy(me - 1 - k, 0, False).wait_recv()
            w_copy(me - 1 - k, 0, False).wait_recv()

        @pl.when(me + 1 + k < sp)
        def _():
            l_copy(me + 1 + k, 1, False).wait_recv()
            w_copy(me + 1 + k, 1, False).wait_recv()

    inner = (me >= 1) & (me + 1 < sp)
    for k in range(1, sp - 1):
        @pl.when(inner & (me - k >= 0))
        def _():
            o_copy(me - k, 0, False).wait_recv()
            o_copy(me - k, 0, False).start()

        @pl.when(inner & (me + k < sp))
        def _():
            o_copy(me + k, 1, False).wait_recv()
            o_copy(me + k, 1, False).start()

    for copy in locals_[5:]:
        copy.wait()
    for i in range(sp):
        @pl.when(i != me)
        def _():
            for copy in pair_copies(i, 1 - side):
                copy.wait_recv()

    for d in range(1, plane):
        tok_copy(d, mine, lax.rem(mine + plane - d, plane)).wait_recv()


    def project(b, _):
        x = x_buf[pl.ds(pl.multiple_of(b * rows, rows), rows)].astype(F32)
        normed = rms_rows(x, ngain_ref[...]).astype(BF)
        p = nn(normed, w_buf[...]).astype(BF)
        proj[b, :, : p.shape[1]] = p
        edge_out[b] = p[rows - WINDOW :, starts[4] : starts[4] + 2 * HEAD_DIM]
        low = nt(normed[:, :kc], l_buf[0])
        for s in range(1, sp):
            low += nt(normed[:, s * kc : (s + 1) * kc], l_buf[s])
        proj[b, :, p.shape[1] : p.shape[1] + low.shape[1]] = low.astype(BF)
        return 0

    lax.fori_loop(0, fs, project, 0)
    edge = remote(edge_out, edge_in, edge_sem.at[0], edge_sem.at[1], {"sp": me + 1})

    @pl.when(me + 1 < sp)
    def _():
        edge.start()

    @pl.when(me == 0)
    def _():
        edge_in[...] = jnp.zeros_like(edge_in)

    nb = rows // SPAN
    low_at = sum(cols)
    lower = (
        lax.broadcasted_iota(jnp.int32, (SPAN, SPAN), 0)
        >= lax.broadcasted_iota(jnp.int32, (SPAN, SPAN), 1)
    )
    tri = lower.astype(F32)
    up = pick(up_ref, KEY_DIM, f)
    bias = pick(bias_ref, KEY_DIM, f)
    sinks = pick(sink_ref, heads, f)
    for b in range(fs):
        low = proj[b, :, low_at : low_at + up_ref.shape[0]]
        z = nn(low, up) + bias
        rate = (jnp.minimum(z, 0.0) - jnp.log1p(jnp.exp(-jnp.abs(z)))) / SOFTMAX_TEMPER
        state = None
        before = jnp.zeros((1, KEY_DIM), F32)
        for n in range(nb):
            r0 = n * SPAN
            within = exact(tri, rate[r0 : r0 + SPAN])
            total = within[SPAN - 1 :]
            v = proj[b, r0 : r0 + SPAN, starts[0] : starts[0] + VALUE_DIM]
            q = proj[b, r0 : r0 + SPAN, starts[2] : starts[2] + KEY_DIM].astype(F32)
            k = proj[b, r0 : r0 + SPAN, starts[3] : starts[3] + KEY_DIM].astype(F32)
            q_dec = q * KEY_DIM**-0.5 * jnp.exp(within)
            k_dec = (k * jnp.exp(-within)).astype(BF)
            k_end = (k * jnp.exp(total - within)).astype(BF)
            scores = jnp.where(lower, nt(q_dec.astype(BF), k_dec), 0.0)
            o = nn(scores.astype(BF), v)
            if state is not None:
                o += nt(q_dec.astype(BF), state.astype(BF))
            local_out[b, r0 : r0 + SPAN] = o
            q_far[b, r0 : r0 + SPAN] = (q_dec * jnp.exp(before)).astype(BF)
            update = tn(v, k_end)
            state = update if state is None else jnp.exp(total) * state + update
            before = before + total
        half = (b % 2) * KEY_DIM
        state_out[b // 2, :VALUE_DIM, half : half + KEY_DIM] = state.astype(BF)
        state_out[b // 2, VALUE_DIM:, half : half + KEY_DIM] = jnp.broadcast_to(
            jnp.exp(before), (16, KEY_DIM)
        ).astype(BF)

    def state_copy(d, sender):
        return remote(
            state_out, state_in.at[sender], state_send.at[d - 1], state_recv.at[sender],
            {"sp": me + d},
        )

    for d in range(1, sp):
        @pl.when(me + d < sp)
        def _():
            state_copy(d, me).start()

    @pl.when(me >= 1)
    def _():
        edge.wait_recv()

    qi = lax.broadcasted_iota(jnp.int32, (WINDOW, 2 * WINDOW), 0)
    ki = lax.broadcasted_iota(jnp.int32, (WINDOW, 2 * WINDOW), 1)
    distance = qi + WINDOW - ki
    inside = (distance >= 0) & (distance < WINDOW)
    for b in range(fs):
        for w in range(rows // WINDOW):
            r0 = w * WINDOW
            here = proj[b, r0 : r0 + WINDOW, starts[4] : starts[4] + 2 * HEAD_DIM]
            if w == 0:
                past = edge_in[b]
                valid = inside & ((ki >= WINDOW) | (me >= 1))
            else:
                past = proj[b, r0 - WINDOW : r0, starts[4] : starts[4] + 2 * HEAD_DIM]
                valid = inside
            band = jnp.concatenate([past, here], 0)
            bk = band[:, :HEAD_DIM]
            bv = band[:, HEAD_DIM:]
            for h in range(heads):
                q0 = starts[1] + h * HEAD_DIM
                q = proj[b, r0 : r0 + WINDOW, q0 : q0 + HEAD_DIM]
                s = jnp.where(valid, nt(q, bk) * HEAD_DIM**-0.5, -1e30)
                sink = sinks[:, h : h + 1]
                top = jnp.maximum(jnp.max(s, -1, keepdims=True), sink)
                e = jnp.exp(s - top)
                den = jnp.sum(e, -1, keepdims=True) + jnp.exp(sink - top)
                a = nn((e / den).astype(BF), bv).astype(BF)
                h0 = VALUE_DIM + h * HEAD_DIM
                hidden[b, r0 : r0 + WINDOW, h0 : h0 + HEAD_DIM] = a

    for i in range(sp - 1):
        @pl.when(i < me)
        def _():
            state_copy(1, i).wait_recv()

        @pl.when(i >= me)
        def _():
            state_in[i] = jnp.zeros(state_in.shape[1:], BF)

    for b in range(fs):
        half = (b % 2) * KEY_DIM
        incoming = jnp.zeros((VALUE_DIM, KEY_DIM), F32)
        for i in range(sp - 1):
            got = state_in[i, b // 2, :VALUE_DIM, half : half + KEY_DIM].astype(F32)
            kept = state_in[i, b // 2, VALUE_DIM : VALUE_DIM + 1, half : half + KEY_DIM].astype(F32)
            incoming = jnp.where(i < me, kept * incoming + got, incoming)
        o = local_out[b] + nt(q_far[b], incoming.astype(BF))
        hidden[b, :, :VALUE_DIM] = rms_rows(o, hgain_ref[...]).astype(BF)

    forward = 2 * me < sp
    nc = o_buf.shape[2]

    def chunk(t):
        return lax.rem(jnp.where(forward, me + t, me - t) + sp, sp)

    def half_copy(s):
        return remote(half_out.at[s], half_in.at[s], half_send.at[s], half_recv.at[s], {"tp": 1 - c})

    def piece_copy(s, d, target):
        return remote(
            piece_out.at[s, d - 1], piece_in.at[s, d - 1],
            piece_send.at[s, d - 1], piece_recv.at[s, d - 1], {"fs": target},
        )

    def produce(t):
        s = chunk(t)

        @pl.when(jnp.logical_not(inner) & (t > 0))
        def _():
            o_copy(s, 0, False).wait_recv()

        w = o_buf[s]
        for b in range(fs):
            part = nn(hidden[b], w)
            lo, hi = part[:own], part[own:]
            half_out[s, b] = jnp.where(c == 0, hi, lo).astype(BF)
            half_own[s, b] = jnp.where(c == 0, lo, hi)
        half_copy(s).start()

    def combine(t):
        s = chunk(t)
        half_copy(s).wait_recv()
        for d in range(1, fs):
            to = lax.rem(f + d, fs)
            piece_out[s, d - 1] = (half_own[s, to] + half_in[s, to].astype(F32)).astype(BF)
            piece_copy(s, d, to).start()
        piece_own[s] = half_own[s, f] + half_in[s, f].astype(F32)

    def finish(t):
        s = chunk(t)
        total = piece_own[s]
        for d in range(1, fs):
            piece_copy(s, d, f).wait_recv()
            total += piece_in[s, d - 1].astype(F32)
        if len(out_ref.shape) == 2:
            out_ref[:, pl.ds(pl.multiple_of(s * nc, nc), nc)] = total.astype(BF)
        else:
            out_ref[s] = total.astype(BF)

    produce(0)

    def steady(t, _):
        produce(t)
        combine(t - 1)
        return 0

    lax.fori_loop(1, sp, steady, 0)
    combine(sp - 1)

    def close(t, _):
        finish(t)
        s = chunk(t)
        half_copy(s).wait_send()
        for d in range(1, fs):
            piece_copy(s, d, f).wait_send()
        return 0

    lax.fori_loop(0, sp, close, 0)

    for k in range(sp - 1):
        @pl.when((me - k >= 0) & (me + 1 < sp))
        def _():
            l_copy(me - k, 0, False).wait_send()
            w_copy(me - k, 0, False).wait_send()
            o_copy(me - k, 0, False).wait_send()

        @pl.when((me + k < sp) & (me >= 1))
        def _():
            l_copy(me + k, 1, False).wait_send()
            w_copy(me + k, 1, False).wait_send()
            o_copy(me + k, 1, False).wait_send()

    for i in range(sp):
        @pl.when(i != me)
        def _():
            for copy in pair_copies(i, side):
                copy.wait_send()

    for d in range(1, plane):
        tok_copy(d, mine, mine).wait_send()

    @pl.when(me + 1 < sp)
    def _():
        edge.wait_send()

    for d in range(1, sp):
        @pl.when(me + d < sp)
        def _():
            state_copy(d, me).wait_send()


def roll_half(a):
    return jnp.concatenate([a[:, a.shape[1] // 2 :], a[:, : a.shape[1] // 2]], 1)


def fold_kernel(
    sizes,
    tok_in,
    gv_ref,
    wq_ref,
    gq_ref,
    gk_ref,
    wk_ref,
    wv_ref,
    low_ref,
    go_ref,
    wo_ref,
    ngain_in,
    up_in,
    bias_in,
    hgain_in,
    sink_in,
    out_ref,
    tok_ref,
    ngain_ref,
    up_ref,
    bias_ref,
    hgain_ref,
    sink_ref,
    x_buf,
    ww,
    wg,
    wl,
    o_buf,
    tiles,
    qw,
    kvb,
    gvb,
    qkb,
    acc,
    acc2,
    og,
    hall,
    lowx,
    fill,
    sc,
    ew,
    decays,
    totals,
    states,
    state_out,
    state_in,
    local_out,
    q_far,
    hidden,
    half_out,
    half_in,
    half_own,
    piece_out,
    piece_in,
    piece_own,
    local_sem,
    l_send,
    l_recv,
    x_send,
    x_recv,
    x_share,
    w_send,
    w_recv,
    p_send,
    p_recv,
    o_send,
    o_recv,
    edge_sem,
    state_sem,
    hid_send,
    hid_recv,
    half_send,
    half_recv,
    piece_send,
    piece_recv,
    g_send,
    g_recv,
    g_rest,
    a_send,
    a_recv,
):
    sp, fs, tp = sizes
    me = lax.axis_index("sp")
    f = lax.axis_index("fs")
    c = lax.axis_index("tp")
    own = tok_in.shape[0]
    rows = own * tp
    kc = gv_ref.shape[0]
    part = kc // 2
    lpart = low_ref.shape[0] // 2
    MESH = pl.DeviceIdType.MESH
    pair = 2 * KEY_DIM
    wide = VALUE_DIM + pair

    slot = lax.rem(me, 2)
    far_slot = 1 - slot
    inner = (me >= 1) & (me + 1 < sp)
    outer = jnp.logical_not(inner)
    middle = 1 + slot
    outside = (sp - 1) * (me - 1)
    buddy = me + 1 - 2 * slot
    third = 2 - me // 2
    fourth = third + 1 - 2 * lax.rem(third, 2)
    chunks = [me, buddy, third, fourth]
    side = lax.rem(f, 2)
    xn = f + 1 - 2 * side
    yn = lax.rem(f + 2, fs)
    n1 = xn * (1 - c) + yn * c
    n2 = xn * c + yn * (1 - c)

    def remote(src, dst, ssem, rsem, target):
        return pltpu.make_async_remote_copy(
            src_ref=src, dst_ref=dst, send_sem=ssem, recv_sem=rsem,
            device_id=target, device_id_type=MESH,
        )

    barrier = pltpu.get_barrier_semaphore()

    def greet(target):
        pl.semaphore_signal(barrier, inc=1, device_id=target, device_id_type=MESH)

    greet({"tp": 1 - c})
    for d in range(1, fs):
        greet({"fs": lax.rem(f + d, fs)})

    @pl.when(me + 1 < sp)
    def _():
        greet({"sp": me + 1})

    @pl.when(me >= 1)
    def _():
        greet({"sp": me - 1})

    def lanes(ref, at, width):
        return ref.at[:, pl.ds(pl.multiple_of(at * width, width), width)]

    def depth(ref, width):
        return ref.at[pl.ds(pl.multiple_of(f * width, width), width)]

    def slice_rows(ref, s):
        return ref.at[pl.ds(pl.multiple_of(s * kc, kc), kc)]

    gd = go_ref.shape[0] // fs
    wd = wo_ref.shape[0] // fs
    heads = sink_in.shape[1] // fs
    wq_cols = heads * HEAD_DIM
    kv = (f * heads) // (SWA_HEADS // KV_HEADS)
    copies_in = [
        (lanes(gq_ref, f // 2, pair), tiles.at[0]),
        (lanes(gk_ref, f // 2, pair), tiles.at[1]),
        (wk_ref, tiles.at[2]),
        (wv_ref, tiles.at[3]),
        (lanes(wq_ref, f, wq_cols), slice_rows(ww, me).at[:, :wq_cols]),
        (lanes(gv_ref, f, VALUE_DIM), slice_rows(wg, me).at[:, :VALUE_DIM]),
        (low_ref, wl.at[me]),
    ]
    nc = o_buf.shape[3]
    for h in range(2):
        cut = pl.ds(h * nc, nc)
        copies_in += [
            (depth(go_ref, gd).at[:, cut], o_buf.at[me, h, pl.ds(0, gd)]),
            (depth(wo_ref, wd).at[:, cut], o_buf.at[me, h, pl.ds(gd, wd)]),
        ]
    copies_in += [
        (ngain_in, ngain_ref),
        (tok_in, tok_ref),
        (up_in, up_ref),
        (bias_in, bias_ref),
        (hgain_in, hgain_ref),
        (sink_in, sink_ref),
    ]
    shared = [0, 0, 0, 0, 1, 2, 3, 4, 4, 4, 4] + list(range(5, 11))
    locals_ = [
        pltpu.make_async_copy(a, b, local_sem.at[i]) for i, (a, b) in zip(shared, copies_in)
    ]

    def local_wait(ref, i):
        pltpu.make_async_copy(ref, ref, local_sem.at[i]).wait()

    for copy in locals_[11:] + locals_[:11]:
        copy.start()

    mine = f * tp + c
    b1, b2, b3 = xn * tp + c, yn * tp + c, (fs - 1 - f) * tp + c

    for copy in locals_[11:]:
        copy.wait()
    normed = rms_rows(tok_ref[...].astype(F32), ngain_ref[...]).astype(BF)
    x_buf[slot, pl.ds(pl.multiple_of(mine * own, own), own)] = normed

    def half_block(s, i, h):
        at = pl.multiple_of(i * own + h * (own // 2), own // 2)
        return x_buf.at[s, pl.ds(at, own // 2)]

    def x_copy(s, i, h, target, src):
        ref = half_block(s, i, h)
        return remote(ref, ref, x_send.at[s], x_recv.at[s, src, h], target)

    def x_sib(s, i, h):
        ref = half_block(s, i, h)
        return remote(ref, ref, x_send.at[s], x_share.at[s], SIB)

    def x_bulk(s, n):
        ref = x_buf.at[s, pl.ds(0, n * (own // 2))]
        return remote(ref, ref, x_send.at[s], x_share.at[s], SIB)

    SIB = {"tp": 1 - c}

    def ways(far, h):
        return (xn, yn) if far and h == 1 else (n1, n2)

    def x_first(s, h, far):
        w1, w2 = ways(far, h)
        return [
            x_copy(s, mine, h, {"fs": w1}, 1),
            x_copy(s, mine, h, {"fs": w2}, 2),
            x_sib(s, mine, h),
        ]

    def x_out(h):
        return x_copy(slot, mine, h, {"sp": middle}, 0)

    def kv_rows(s, h):
        at = pl.multiple_of(s * kc + h * part, part)
        return ww.at[pl.ds(at, part), wq_cols:]

    def low_rows(s, h):
        return wl.at[s, pl.ds(pl.multiple_of(h * lpart, lpart), lpart)]

    def w_copy(kind, s):
        ref = (
            lambda: slice_rows(ww, s).at[:, :wq_cols],
            lambda: kv_rows(s, side),
            lambda: low_rows(s, c),
            lambda: slice_rows(wg, s),
        )[kind]()
        return remote(ref, ref, w_send.at[kind], w_recv.at[kind, s], {"sp": middle})

    def w_bulk(kind, n):
        ref = (
            lambda: ww.at[pl.ds(0, n * kc), :wq_cols],
            lambda: ww.at[pl.ds(0, n * part), wq_cols:],
            lambda: wl.at[0, pl.ds(0, n * lpart)],
            lambda: wg.at[pl.ds(0, n * kc)],
        )[kind]()
        return remote(ref, ref, w_send.at[kind], w_recv.at[kind, 0], {"sp": middle})

    def kv_share(s, h):
        return remote(kv_rows(s, h), kv_rows(s, h), p_send.at[0], p_recv.at[s], {"fs": xn})

    def low_share(s, h):
        return remote(low_rows(s, h), low_rows(s, h), p_send.at[1], p_recv.at[sp], SIB)

    def share_bulk(i):
        ref = ww.at[pl.ds(0, 3 * part), wq_cols:] if i == 0 else wl.at[pl.ds(0, 3), pl.ds(0, lpart)]
        return remote(ref, ref, p_send.at[i], p_recv.at[sp], SIB)

    def o_copy(way, s, h, d):
        target = {"sp": middle if way == 0 else outside}
        ref = o_buf.at[s, h, pl.ds(d * gd, gd)]
        return remote(ref, ref, o_send.at[way], o_recv.at[s, h, d], target)

    def o_bulk(way, n):
        ref = o_buf.at[pl.ds(0, n)]
        return remote(ref, ref, o_send.at[way], o_recv.at[0, 0, 0], {"sp": middle})

    def o_part(way, s, h, d):
        o_copy(0, s, h, d).wait_recv()
        o_copy(way, s, h, d).start()

    def o_relay(way, s, h):
        for d in range(2):
            o_part(way, s, h, d)

    quarters = [(h, d) for h in range(2) for d in range(2)]

    def l_copy(i, k, target):
        return remote(lowx.at[i], lowx.at[i], l_send.at[0], l_recv.at[min(k // 3, 1)], target)

    def l_first():
        peers = [{"fs": n1}, {"fs": n2}, {"fs": fs - 1 - f}, SIB]
        return [l_copy(mine, k, peer) for k, peer in enumerate(peers)]

    def l_bulk(n, which):
        return remote(lowx.at[pl.ds(0, n)], lowx.at[pl.ds(0, n)], l_send.at[0], l_recv.at[which], SIB)

    def l_onward():
        return [l_copy(i, 4 + k, SIB) for k, i in enumerate((b1, b2, b3))]

    def start(copies):
        for copy in copies:
            copy.start()

    pl.semaphore_wait(barrier, fs + jnp.where(inner, 2, 1))

    LOW, KV, QUERY, STATE = 2, 1, 0, 3
    locals_[6].wait()
    w_copy(LOW, me).start()

    @pl.when(outer)
    def _():
        for h in range(2):
            x_out(h).start()

    @pl.when(inner)
    def _():
        for h in range(2):
            start(x_first(slot, h, False))

    local_wait(tiles, 0)
    for copy in locals_[4:6]:
        copy.wait()
    own_rows = pl.ds(pl.multiple_of(me * kc, kc), kc)

    def half_of(i, width, which):
        return jnp.where(which == 0, tiles[i, :, :width], tiles[i, :, width:])

    ww[own_rows, wq_cols:] = jnp.concatenate(
        [half_of(2, HEAD_DIM, kv), half_of(3, HEAD_DIM, kv)], 1
    )
    w_copy(KV, me).start()
    w_copy(QUERY, me).start()
    wg[own_rows, VALUE_DIM:] = jnp.concatenate(
        [half_of(0, KEY_DIM, side), half_of(1, KEY_DIM, side)], 1
    )
    local_wait(o_buf.at[me], 4)

    @pl.when(outer)
    def _():
        w_copy(STATE, me).start()
        for h, d in quarters:
            o_copy(0, me, h, d).start()

    lane = lax.broadcasted_iota(jnp.int32, (rows, pair), 1)
    row = lax.broadcasted_iota(jnp.int32, (rows, pair), 0)
    left = lane < KEY_DIM
    early = row < SPAN
    same = (row < SPAN) == (lane < SPAN)
    diagonal = same & (row >= lane)
    below = (row >= SPAN) & (lane < SPAN)

    def edge_rows(i, h):
        n = fs * rows // 2
        return kvb.at[i, pl.ds(pl.multiple_of(h * n, n), n)]

    edge = remote(
        edge_rows(2, side), edge_rows(0, side), edge_sem.at[0], edge_sem.at[1], {"sp": me + 1}
    )

    def edge_share(h):
        return remote(
            edge_rows(0, h), edge_rows(0, h), edge_sem.at[2], edge_sem.at[3], {"fs": xn}
        )
    state = remote(state_out, state_in, state_sem.at[0], state_sem.at[1], {"sp": me + 1})

    def hid_part(s, i):
        return hidden.at[s, :, i * VALUE_DIM : (i + 1) * VALUE_DIM]

    def hid_copy(i, s):
        return remote(
            hid_part(s, i), hid_part(s, i), hid_send.at[i], hid_recv.at[i], {"sp": outside}
        )

    def seq(b):
        if isinstance(b, int):
            return pl.ds(b * rows, rows)
        return pl.ds(pl.multiple_of(b * rows, rows), rows)

    @pl.when(inner)
    def _():
        for h, d in quarters:
            o_copy(1, me, h, d).start()

        def arrive(kind, s, onward):
            w_copy(kind, s).wait_recv()
            if onward:
                w_copy(kind, s).start()
            if kind == LOW:
                low_share(s, c).start()
            if kind == KV:
                kv_share(s, side).start()

        def neighbours(s, h, far):
            w1, w2 = ways(far, h)
            i1, i2 = w1 * tp + c, w2 * tp + c
            x_copy(s, i1, h, SIB, 1).wait_recv()
            x_copy(s, i1, h, {"fs": w2}, 3).start()
            x_sib(s, i1, h).start()
            x_copy(s, i2, h, SIB, 2).wait_recv()
            x_sib(s, i2, h).start()

        def corner(s):
            for h in range(2):
                x_copy(s, b3, h, SIB, 3).wait_recv()
                x_sib(s, b3, h).start()

        def siblings(s):
            x_bulk(s, 2 * fs).wait_recv()

        def columns(s):
            return pl.ds(pl.multiple_of(s * kc, kc), kc)

        bs = [bias_ref[:, i * KEY_DIM : (i + 1) * KEY_DIM] for i in range(fs)]
        ups = [up_ref[:, i * KEY_DIM : (i + 1) * KEY_DIM] for i in range(fs)]
        bias, up = bs[0], ups[0]
        for i in range(1, fs):
            bias = jnp.where(f == i, bs[i], bias)
            up = jnp.where(f == i, ups[i], up)
        up_l = jnp.concatenate([up, jnp.zeros_like(up)], 1)
        up_r = jnp.concatenate([jnp.zeros_like(up), up], 1)
        bias2 = jnp.concatenate([bias, bias], 1)

        def own_low():
            at = pl.ds(pl.multiple_of(mine * own, own), own)
            x = jnp.concatenate([x_buf[slot, at], x_buf[far_slot, at]], 0)
            low = nt(wl[0], x[:, :kc])
            for j in range(1, sp):
                low += nt(wl[j], x[:, j * kc : (j + 1) * kc])
            lowx[mine] = low.astype(BF)

        def gate(p):
            pre = []
            for i in range(tp):
                z = tn(lowx[2 * p * tp + i], up_l) + tn(lowx[(2 * p + 1) * tp + i], up_r)
                pre.append(z + bias2)
            return [
                jnp.concatenate([z[k * own : (k + 1) * own] for z in pre], 0) for k in range(2)
            ]

        def decay():
            tri = diagonal.astype(F32)
            for p in range(fs // 2):
                for s, z in zip((slot, far_slot), gate(p)):
                    decay_of(s, p, z, tri)

        def decay_of(s, p, z, tri):
            rate = (jnp.minimum(z, 0.0) - jnp.log1p(jnp.exp(-jnp.abs(z)))) / SOFTMAX_TEMPER
            within = exact(tri, rate)
            t0, t1 = within[SPAN - 1 : SPAN], within[rows - 1 :]
            grow = jnp.exp(within) * KEY_DIM**-0.5
            end = jnp.exp(jnp.where(early, t0, t1) - within)
            decays[s, p, 0] = grow
            decays[s, p, 1] = jnp.exp(-within)
            decays[s, p, 2] = end
            decays[s, p, 3] = grow * jnp.where(early, 1.0, jnp.exp(t0))
            decays[s, p, 4] = end * jnp.where(early, jnp.exp(t1), 1.0)
            totals[s, p] = jnp.broadcast_to(jnp.exp(t0 + t1), totals.shape[2:])

        def window_maps(s, slices):
            total = nn(x_buf[s, :, columns(slices[0])], slice_rows(ww, slices[0])[...])
            for j in slices[1:]:
                total += nn(x_buf[s, :, columns(j)], slice_rows(ww, j)[...])
            return total

        def state_maps(s, slices):
            total = nn(x_buf[s, :, columns(slices[0])], slice_rows(wg, slices[0])[...])
            for j in slices[1:]:
                total += nn(x_buf[s, :, columns(j)], slice_rows(wg, j)[...])
            return total

        def place(s, p):
            q = p[:, :wq_cols].astype(BF).astype(F32) * HEAD_DIM**-0.5
            for h in range(heads):
                qh = jnp.where(left_all, q if h == 0 else roll_half(q), 0.0)
                qw[s, h] = qh.astype(BF)
            kvb[s + 1] = p[:, wq_cols:].astype(BF)

        left_all = lax.broadcasted_iota(jnp.int32, (fs * rows, pair), 1) < KEY_DIM
        tall = heads * WINDOW
        qi = lax.broadcasted_iota(jnp.int32, (tall, 2 * WINDOW), 0)
        ki = lax.broadcasted_iota(jnp.int32, (tall, 2 * WINDOW), 1)
        distance = lax.rem(qi, WINDOW) + WINDOW - ki
        inside = (distance >= 0) & (distance < WINDOW)
        sinks = sink_ref[:, :heads]
        for i in range(1, fs):
            sinks = jnp.where(f == i, sink_ref[:, i * heads : (i + 1) * heads], sinks)
        sink = sinks[:, :1]
        for h in range(1, heads):
            sink = jnp.where(qi < h * WINDOW, sink, sinks[:, h : h + 1])
        fill[...] = jnp.where(ki == 0, sink, -1e30)
        key_row = lax.broadcasted_iota(jnp.int32, (2 * WINDOW, pair), 0)
        key_lane = lax.broadcasted_iota(jnp.int32, (2 * WINDOW, pair), 1)

        @pl.when(me == 1)
        def _():
            kvb[0] = jnp.zeros(kvb.shape[1:], BF)
            state_in[...] = jnp.zeros_like(state_in)

        def far_rows(h):
            x_copy(far_slot, mine, h, SIB, 0).wait_recv()
            start(x_first(far_slot, h, True))

        arrive(LOW, buddy, True)
        w_copy(STATE, me).start()
        o_copy(0, me, 0, 0).start()
        arrive(LOW, third, False)
        arrive(KV, third, False)
        neighbours(slot, 0, False)
        far_rows(0)
        arrive(LOW, fourth, False)
        neighbours(slot, 1, False)
        far_rows(1)
        share_bulk(1).wait_recv()
        own_low()
        start(l_first())
        arrive(KV, buddy, True)
        neighbours(far_slot, 0, True)
        arrive(QUERY, buddy, True)
        o_copy(0, me, 0, 1).start()
        corner(slot)
        siblings(slot)
        arrive(QUERY, third, False)
        kv_share(third, 1 - side).wait_recv()
        acc[slot] = window_maps(slot, (me, third))
        neighbours(far_slot, 1, True)
        arrive(STATE, buddy, True)
        arrive(KV, fourth, False)
        l_bulk(3, 0).wait_recv()
        start(l_onward())
        l_bulk(4, 1).wait_recv()
        decay()
        w_copy(STATE, third).wait_recv()
        acc2[slot] = state_maps(slot, chunks[:3])
        o_relay(1, third, 0)
        corner(far_slot)
        arrive(QUERY, fourth, False)
        kv_share(buddy, 1 - side).wait_recv()
        kv_share(fourth, 1 - side).wait_recv()

        place(slot, acc[slot] + window_maps(slot, (buddy, fourth)))

        @pl.when(me == 1)
        def _():
            edge.start()

        for d in range(2):
            o_copy(0, me, 1, d).start()

        siblings(far_slot)
        place(far_slot, window_maps(far_slot, chunks))

        def window(s):
            valid = inside & ((ki >= WINDOW) | (me > 1) | (s > 0))
            bands = [jnp.concatenate([kvb[s, seq(b)], kvb[s + 1, seq(b)]], 0) for b in range(fs)]
            for b in range(fs):
                q = jnp.concatenate([qw[s, h, seq(b)] for h in range(heads)], 0)
                sc[b] = jnp.where(valid, nt(q, bands[b]), fill[...])
            for b in range(fs):
                near = sc[b]
                top = jnp.max(near, -1, keepdims=True)
                ew[b] = jnp.exp(near - top).astype(BF)
            for b in range(fs):
                band = jnp.concatenate([kvb[s, seq(b)], kvb[s + 1, seq(b)]], 0).astype(F32)
                values = jnp.where(
                    key_lane < HEAD_DIM, 1.0, jnp.where(key_row == 0, 0.0, band)
                ).astype(BF)
                both = nn(ew[b], values)
                turned = roll_half(both)
                first = turned[:WINDOW] / both[:WINDOW]
                second = both[WINDOW:] / turned[WINDOW:]
                hidden[s, seq(b), VALUE_DIM:] = jnp.where(left, first, second).astype(BF)

        window(far_slot)
        hid_copy(1, far_slot).start()

        @pl.when(me > 1)
        def _():
            for h in range(2):
                o_relay(0, buddy, h)

        acc2[far_slot] = state_maps(far_slot, chunks[:3])

        @pl.when(me > 1)
        def _():
            edge.wait_recv()
            edge_share(side).start()

        w_copy(STATE, fourth).wait_recv()

        for s in range(2):
            p = (acc2[s] + state_maps(s, chunks[3:])).astype(BF)
            gvb[s] = p[:, :VALUE_DIM]
            qkb[s] = p[:, VALUE_DIM:].astype(F32)

        def keys(s, p):
            return jnp.where(left, roll_half(qkb[s, seq(2 * p)]), qkb[s, seq(2 * p + 1)])

        def queries(s, p):
            return jnp.where(left, qkb[s, seq(2 * p)], roll_half(qkb[s, seq(2 * p + 1)]))

        for s in range(2):
            for p in range(fs // 2):
                k_far = (keys(s, p) * decays[s, p, 4]).astype(BF)
                states[s, p] = jnp.where(
                    left, tn(gvb[s, seq(2 * p)], k_far), tn(gvb[s, seq(2 * p + 1)], k_far)
                )
        for p in range(fs // 2):
            state_out[p] = (totals[1, p, :1] * states[0, p] + states[1, p]).astype(BF)

        @pl.when(me == 1)
        def _():
            state.start()
            o_relay(0, buddy, 0)

        for s in range(2):
            for p in range(fs // 2):
                k = keys(s, p)
                q = queries(s, p)
                qd = q * decays[s, p, 0]
                qf = q * decays[s, p, 3]
                kd = (k * decays[s, p, 1]).astype(BF)
                ke = (k * decays[s, p, 2]).astype(BF)
                for j in range(2):
                    here = left if j == 0 else jnp.logical_not(left)
                    qj = jnp.where(here, qd, 0.0).astype(BF)
                    scores = jnp.where(
                        diagonal, nt(qj, kd), jnp.where(below, nt(qj, ke), 0.0)
                    ).astype(BF)
                    local_out[s, seq(2 * p + j)] = nn(scores, gvb[s, seq(2 * p + j)])
                    q_far[s, seq(2 * p + j)] = jnp.where(here, qf, 0.0).astype(BF)
            if s == 0:
                @pl.when(me == 1)
                def _():
                    o_relay(1, third, 1)

        @pl.when(me == 1)
        def _():
            o_relay(0, buddy, 1)

        @pl.when(me > 1)
        def _():
            o_relay(1, third, 1)
            edge_share(1 - side).wait_recv()
            window(slot)
            state.wait_recv()

        def finish_state(s):
            for p in range(fs // 2):
                arrived = state_in[p].astype(F32)
                entering = jnp.where(s == 0, arrived, totals[0, p, :1] * arrived + states[0, p])
                entering = entering.astype(BF)
                for j in range(2):
                    b = 2 * p + j
                    o = local_out[s, seq(b)] + nt(q_far[s, seq(b)], entering)
                    hidden[s, seq(b), :VALUE_DIM] = rms_rows(o, hgain_ref[...]).astype(BF)

        finish_state(far_slot)
        hid_copy(0, far_slot).start()
        finish_state(slot)

        @pl.when(me == 1)
        def _():
            window(slot)

    def g_copy(k, j, g, h, target):
        ref = og.at[j, g, h]
        into = g_recv.at[j, h] if k == 0 else g_rest.at[0]
        return remote(ref, ref, g_send.at[0], into, target)

    def g_bulk(n, ssem):
        ref = og.at[:, pl.ds(0, n)]
        return remote(ref, ref, ssem.at[0], g_rest.at[0], SIB)

    corner_f = fs - 1 - f

    def g_first(j, h):
        return [g_copy(0, j, f, h, {"fs": n1}), g_copy(1, j, f, h, {"fs": n2})]

    def g_relay(j, h):
        return g_copy(2, j, n1, h, {"fs": n2})

    def a_part(g, i):
        return hidden.at[slot, seq(g), i * VALUE_DIM : (i + 1) * VALUE_DIM]

    def a_copy(k, i):
        g = (n1, n2, corner_f)[k]
        here = hall.at[f, :, i * VALUE_DIM : (i + 1) * VALUE_DIM]
        return remote(a_part(g, i), here, a_send.at[0], a_recv.at[0], {"fs": g})

    def a_bulk():
        ref = hall.at[pl.ds(0, fs - 1)]
        return remote(ref, ref, a_send.at[0], a_recv.at[0], {"fs": n1})

    @pl.when(outer)
    def _():
        for h in range(2):
            og[0, f, h] = o_buf[me, h]
            start(g_first(0, h))
        for h in range(2):
            for d in range(2):
                o_copy(0, buddy, h, d).wait_recv()
            og[1, f, h] = o_buf[buddy, h]
        for j in range(2):
            for h in range(2):
                g_copy(0, j, n1, h, SIB).wait_recv()
                g_relay(j, h).start()
                if j == 0:
                    start(g_first(1, h))
        g_bulk(2, g_send).wait_recv()
        for i in (1, 0):
            hid_copy(i, slot).wait_recv()
            for k in range(3):
                a_copy(k, i).start()
        hall[f] = hidden[slot, seq(f)]

    parts = [(s, h) for s in chunks for h in range(2)]

    def half_copy(s, h):
        return remote(
            half_out.at[s, h], half_in.at[s, h], half_send.at[0], half_recv.at[s, h], SIB
        )

    peers = (corner_f, n1, n2)

    def piece_copy(s, h, d):
        target = peers[d - 1]
        return remote(
            piece_out.at[s, h, d - 1], piece_in.at[s, h, d - 1],
            piece_send.at[0], piece_recv.at[s, h], {"fs": target},
        )

    def produce(t):
        s, h = parts[t]
        if 4 <= t < 6:
            @pl.when(outer)
            def _():
                for d in range(2):
                    o_copy(0, s, h, d).wait_recv()
        if t >= 6:
            @pl.when(outer)
            def _():
                for d in range(2):
                    o_copy(0, s, h, d).wait_recv()

        w = o_buf[s, h]
        for b in range(fs):
            partial = nn(hidden[slot, seq(b)], w)
            lo, hi = partial[:own], partial[own:]
            half_out[s, h, b] = jnp.where(c == 0, hi, lo).astype(BF)
            half_own[s, h, b] = jnp.where(c == 0, lo, hi)
        half_copy(s, h).start()

    def combine(t):
        s, h = parts[t]
        half_copy(s, h).wait_recv()
        for d in range(1, fs):
            to = peers[d - 1]
            piece_out[s, h, d - 1] = (half_own[s, h, to] + half_in[s, h, to].astype(F32)).astype(BF)
            piece_copy(s, h, d).start()
        piece_own[s, h] = half_own[s, h, f] + half_in[s, h, f].astype(F32)

    def store(t, total):
        s, h = parts[t]
        at = pl.ds(pl.multiple_of((2 * s + h) * nc, nc), nc)
        out_ref[:, at] = total.astype(BF)

    def finish(t):
        s, h = parts[t]
        total = piece_own[s, h]
        remote(
            piece_out.at[s, h], piece_in.at[s, h], piece_send.at[0], piece_recv.at[s, h], SIB
        ).wait_recv()
        for d in range(1, fs):
            total += piece_in[s, h, d - 1].astype(F32)
        store(t, total)

    def whole_copy(s, h):
        return remote(
            half_out.at[s, h, 0], half_in.at[s, h, 0], half_send.at[1], half_recv.at[s, h], SIB
        )

    def produce_whole(t):
        s, h = parts[t]
        total = nn(hall[0], og[t // 2, 0, h])
        for g in range(1, fs):
            total += nn(hall[g], og[t // 2, g, h])
        lo, hi = total[:own], total[own:]
        half_out[s, h, 0] = jnp.where(c == 0, hi, lo).astype(BF)
        half_own[s, h, 0] = jnp.where(c == 0, lo, hi)
        whole_copy(s, h).start()

    def finish_whole(t):
        s, h = parts[t]
        whole_copy(s, h).wait_recv()
        store(t, half_own[s, h, 0] + half_in[s, h, 0].astype(F32))

    def tail_sent(n):
        ref = half_out.at[pl.ds(0, n)]
        remote(ref, ref, half_send.at[0], half_recv.at[0, 0], SIB).wait_send()
        ref = piece_out.at[pl.ds(0, n)]
        remote(ref, ref, piece_send.at[0], piece_recv.at[0, 0], SIB).wait_send()

    @pl.when(inner)
    def _():
        produce(0)
        for t in range(1, 2 * sp):
            produce(t)
            combine(t - 1)
            for h, d in {2: quarters[:2], 4: quarters[2:3], 5: quarters[3:]}.get(t, ()):
                o_part(1, fourth, h, d)
        combine(2 * sp - 1)
        for t in range(2 * sp):
            finish(t)
        tail_sent(sp)

    @pl.when(outer)
    def _():
        produce(4)
        produce(5)
        combine(4)
        a_bulk().wait_recv()
        for t in range(4):
            produce_whole(t)
        combine(5)
        produce(6)
        produce(7)
        combine(6)
        combine(7)
        for t in range(4):
            finish_whole(t)
        for t in range(4, 2 * sp):
            finish(t)
        tail_sent(sp // 2)
        ref = half_out.at[0, 0]
        remote(ref, ref, half_send.at[1], half_recv.at[0, 0], SIB).wait_send()
        g_bulk(3, g_send).wait_send()
        a_bulk().wait_send()

    @pl.when(outer)
    def _():
        x_bulk(slot, 2).wait_send()
        for kind in range(4):
            w_bulk(kind, 1).wait_send()
        o_bulk(0, 1).wait_send()

    @pl.when(inner)
    def _():
        for s in range(2):
            x_bulk(s, 14).wait_send()
        l_bulk(7, 0).wait_send()
        for kind in range(4):
            w_bulk(kind, 2).wait_send()
        share_bulk(0).wait_send()
        share_bulk(1).wait_send()
        o_bulk(0, 2).wait_send()
        o_bulk(1, 3).wait_send()
        for i in range(2):
            hid_copy(i, far_slot).wait_send()

        @pl.when(me == 1)
        def _():
            edge.wait_send()
            state.wait_send()

        @pl.when(me > 1)
        def _():
            edge_share(side).wait_send()


def fold_call(sizes, operands):
    sp, fs, tp = sizes
    own, d = operands[0].shape
    rows = own * tp
    kc = operands[1].shape[0]
    rank = operands[7].shape[0]
    depth = (operands[8].shape[0] + operands[9].shape[0]) // fs
    nc = operands[8].shape[1]
    pair = 2 * KEY_DIM
    all_rows = fs * rows
    pairs = fs // 2
    vm = pltpu.VMEM
    dma = pltpu.SemaphoreType.DMA
    small = [(o.shape, o.dtype) for o in operands[10:]]
    scratch = [
        vm((own, d), BF),
        *(vm(shape, dtype) for shape, dtype in small),
        vm((2, all_rows, d), BF),
        vm((d, 2 * pair), BF),
        vm((d, VALUE_DIM + pair), BF),
        vm((sp, rank, kc), BF),
        vm((sp, 2, depth, nc // 2), BF),
        vm((4, kc, pair), BF),
        vm((2, 2, all_rows, pair), BF),
        vm((3, all_rows, pair), BF),
        vm((2, all_rows, VALUE_DIM), BF),
        vm((2, all_rows, pair), F32),
        vm((2, all_rows, 2 * pair), F32),
        vm((2, all_rows, VALUE_DIM + pair), F32),
        vm((2, fs, 2, depth, nc // 2), BF),
        vm((fs, rows, depth), BF),
        vm((fs * tp, rank, 2 * own), BF),
        vm((2 * WINDOW, 2 * WINDOW), F32),
        vm((fs, 2 * WINDOW, 2 * WINDOW), F32),
        vm((fs, 2 * WINDOW, 2 * WINDOW), BF),
        vm((2, pairs, 5, rows, pair), F32),
        vm((2, pairs, 8, pair), F32),
        vm((2, pairs, VALUE_DIM, pair), F32),
        vm((pairs, VALUE_DIM, pair), BF),
        vm((pairs, VALUE_DIM, pair), BF),
        vm((2, all_rows, VALUE_DIM), F32),
        vm((2, all_rows, pair), BF),
        vm((2, all_rows, depth), BF),
        vm((sp, 2, fs, own, nc // 2), BF),
        vm((sp, 2, fs, own, nc // 2), BF),
        vm((sp, 2, fs, own, nc // 2), F32),
        vm((sp, 2, fs - 1, own, nc // 2), BF),
        vm((sp, 2, fs - 1, own, nc // 2), BF),
        vm((sp, 2, own, nc // 2), F32),
        dma((11,)),
        dma((1,)),
        dma((2,)),
        dma((2,)),
        dma((2, 4, 2)),
        dma((2,)),
        dma((4,)),
        dma((4, sp)),
        dma((2,)),
        dma((sp + 1,)),
        dma((2,)),
        dma((sp, 2, 2)),
        dma((4,)),
        dma((2,)),
        dma((2,)),
        dma((2,)),
        dma((2,)),
        dma((sp, 2)),
        dma((1,)),
        dma((sp, 2)),
        dma((1,)),
        dma((2, 2)),
        dma((1,)),
        dma((1,)),
        dma((1,)),
    ]
    anywhere = pl.BlockSpec(memory_space=pl.ANY)
    return pl.pallas_call(
        functools.partial(fold_kernel, sizes),
        out_shape=pltpu.VMEM((own, sp * nc), BF),
        in_specs=[anywhere] * 15,
        out_specs=pl.BlockSpec(memory_space=pltpu.VMEM),
        scratch_shapes=scratch,
        compiler_params=pltpu.CompilerParams(
            has_side_effects=True, vmem_limit_bytes=60 * 1024 * 1024, collective_id=0
        ),
    )(*operands)


def folds(sp, fs, tp, shape, rows, kc, width, rank, nc, depth):
    whole_rows = rows == WINDOW == 2 * SPAN
    lanes_fit = nc % 256 == 0 and kc % 128 == 0 and depth == 2 * VALUE_DIM and 2 * HEAD_DIM == 2 * KEY_DIM
    return sp == 4 and fs == 4 and tp == 2 and whole_rows and lanes_fit and rank % 32 == 0


def per_device(
    tokens,
    norm_gain,
    gla_query_weight,
    gla_key_weight,
    gla_value_weight,
    decay_down,
    decay_up,
    decay_bias,
    head_gain,
    window_query_weight,
    window_key_weight,
    window_value_weight,
    sink_logit,
    gla_output_weight,
    window_output_weight,
):
    fs, tp, sp = (lax.axis_size(n) for n in ("fs", "tp", "sp"))
    low = decay_down.T
    own = tokens.shape[1]
    rows = own * tp
    kc = decay_down.shape[0]
    width = VALUE_DIM + 4 * HEAD_DIM + 2 * KEY_DIM
    rank = low.shape[0]
    depth = (gla_output_weight.shape[0] + window_output_weight.shape[0]) // fs
    nc = gla_output_weight.shape[1]
    flat = nc % 128 == 0
    operands = (
        tokens[0],
        gla_value_weight,
        window_query_weight,
        gla_query_weight,
        gla_key_weight,
        window_key_weight,
        window_value_weight,
        low,
        gla_output_weight,
        window_output_weight,
        norm_gain[None],
        decay_up,
        decay_bias[None],
        head_gain[None],
        sink_logit[None],
    )
    if folds(sp, fs, tp, tokens.shape, rows, kc, width, rank, nc, depth):
        return fold_call((sp, fs, tp), operands).reshape(1, own, sp * nc)
    vm = pltpu.VMEM
    dma = pltpu.SemaphoreType.DMA
    scratch = [
        vm((fs * rows, tokens.shape[2]), BF),
        vm((sp * kc, width), BF),
        vm((sp, rank, kc), BF),
        vm((sp, depth, nc), BF),
        vm((fs, rows, width + 128), BF),
        vm((fs, WINDOW, 2 * HEAD_DIM), BF),
        vm((fs, WINDOW, 2 * HEAD_DIM), BF),
        vm((fs // 2, VALUE_DIM + 16, 2 * KEY_DIM), BF),
        vm((sp, fs // 2, VALUE_DIM + 16, 2 * KEY_DIM), BF),
        vm((fs, rows, VALUE_DIM), F32),
        vm((fs, rows, KEY_DIM), BF),
        vm((fs, rows, depth), BF),
        vm((sp, fs, own, nc), BF),
        vm((sp, fs, own, nc), BF),
        vm((sp, fs, own, nc), F32),
        vm((sp, fs - 1, own, nc), BF),
        vm((sp, fs - 1, own, nc), BF),
        vm((sp, own, nc), F32),
        dma((6,)),
        dma((fs * tp - 1,)),
        dma((fs * tp - 1,)),
        dma((2, sp)),
        dma((sp,)),
        dma((2, sp)),
        dma((sp,)),
        dma((2, sp)),
        dma((sp,)),
        dma((sp,)),
        dma((sp,)),
        dma((sp,)),
        dma((sp,)),
        dma((2, sp)),
        dma((sp,)),
        dma((2,)),
        dma((sp,)),
        dma((sp,)),
        dma((sp,)),
        dma((sp,)),
        dma((sp, fs - 1)),
        dma((sp, fs - 1)),
    ]
    spec = pl.BlockSpec(memory_space=pltpu.VMEM)
    anywhere = pl.BlockSpec(memory_space=pl.ANY)
    mixed = pl.pallas_call(
        functools.partial(mixer_kernel, (sp, fs, tp)),
        out_shape=jax.ShapeDtypeStruct((own, sp * nc) if flat else (sp, own, nc), BF),
        in_specs=[
            anywhere if i in (1, 2, 8, 9) else spec for i in range(15)
        ],
        out_specs=spec,
        scratch_shapes=scratch,
        compiler_params=pltpu.CompilerParams(
            has_side_effects=True, vmem_limit_bytes=60 * 1024 * 1024
        ),
    )(*operands)
    return (mixed if flat else mixed.transpose(1, 0, 2)).reshape(1, own, sp * nc)


def solution(mesh):
    in_specs = (
        P("fs", ("sp", "tp"), None),
        P(),
        P("sp", "tp"),
        P("sp", "tp"),
        P("sp", "tp"),
        P("sp", None),
        P(None, "tp"),
        P("tp"),
        P(),
        P("sp", "tp"),
        P("sp", "tp"),
        P("sp", "tp"),
        P("tp"),
        P("tp", "sp"),
        P("tp", "sp"),
    )
    out_specs = P("fs", ("sp", "tp"), None)
    return jax.shard_map(
        per_device, mesh=mesh, in_specs=in_specs, out_specs=out_specs, check_vma=False
    )
```

```python
import functools

import jax
import jax.numpy as jnp
from jax import lax
from jax.experimental import pallas as pl
from jax.experimental.pallas import tpu as pltpu
from jax.sharding import PartitionSpec as P

KEY_DIM = 64
VALUE_DIM = 128
SWA_HEADS = 16
KV_HEADS = 4
HEAD_DIM = 64
WINDOW = 128
SPAN = 64

EPS = 1e-06
SOFTMAX_TEMPER = 16.0
BF = jnp.bfloat16
F32 = jnp.float32


def rms_rows(values, gain):
    mean_square = jnp.mean(values * values, axis=-1, keepdims=True)
    return values * lax.rsqrt(mean_square + EPS) * gain


def nt(a, b):
    return lax.dot_general(a, b, (((1,), (1,)), ((), ())), preferred_element_type=F32)


def nn(a, b):
    return lax.dot_general(a, b, (((1,), (0,)), ((), ())), preferred_element_type=F32)


def tn(a, b):
    return lax.dot_general(a, b, (((0,), (0,)), ((), ())), preferred_element_type=F32)


def exact(a, b):
    return lax.dot_general(
        a, b, (((1,), (0,)), ((), ())), precision=lax.Precision.HIGHEST, preferred_element_type=F32
    )


def mixer_kernel(
    sizes,
    tok_ref,
    gv_ref,
    wq_ref,
    gq_ref,
    gk_ref,
    wk_ref,
    wv_ref,
    low_ref,
    go_ref,
    wo_ref,
    ngain_ref,
    up_ref,
    bias_ref,
    hgain_ref,
    sink_ref,
    out_ref,
    x_buf,
    w_buf,
    l_buf,
    o_buf,
    proj,
    edge_out,
    edge_in,
    state_out,
    state_in,
    local_out,
    q_far,
    hidden,
    half_out,
    half_in,
    half_own,
    piece_out,
    piece_in,
    piece_own,
    local_sem,
    tok_send,
    tok_recv,
    w_send,
    w_recv,
    l_send,
    l_recv,
    v_send,
    v_recv,
    vp_send,
    vp_recv,
    lp_send,
    lp_recv,
    o_send,
    o_recv,
    edge_sem,
    state_send,
    state_recv,
    half_send,
    half_recv,
    piece_send,
    piece_recv,
):
    sp, fs, tp = sizes
    me = lax.axis_index("sp")
    f = lax.axis_index("fs")
    c = lax.axis_index("tp")
    plane = fs * tp
    mine = f * tp + c
    own = tok_ref.shape[0]
    rows = own * tp
    kc = gv_ref.shape[0]
    MESH = pl.DeviceIdType.MESH

    def remote(src, dst, ssem, rsem, target):
        return pltpu.make_async_remote_copy(
            src_ref=src, dst_ref=dst, send_sem=ssem, recv_sem=rsem,
            device_id=target, device_id_type=MESH,
        )

    def w_rows(s):
        return w_buf.at[pl.ds(pl.multiple_of(s * kc, kc), kc)]

    def w_copy(s, way, first):
        target = {"sp": me + (1 if way == 0 else -1)}
        return remote(
            w_main(s), w_main(s), w_send.at[way, s], w_recv.at[s], target
        )

    side = f % 2
    part = kc // 2
    lpart = low_ref.shape[0] // 2

    def w_main(s):
        return w_rows(s).at[:, : starts[4]]

    def v_rows(s, h):
        at = pl.multiple_of(s * kc + h * part, part)
        return w_buf.at[pl.ds(at, part), starts[4] : starts[4] + 2 * HEAD_DIM]

    def l_rows(s, h):
        return l_buf.at[s, pl.ds(pl.multiple_of(h * lpart, lpart), lpart)]

    def v_copy(s, way):
        target = {"sp": me + (1 if way == 0 else -1)}
        return remote(v_rows(s, side), v_rows(s, side), v_send.at[way, s], v_recv.at[s], target)

    def lh_copy(s, way):
        target = {"sp": me + (1 if way == 0 else -1)}
        return remote(l_rows(s, side), l_rows(s, side), l_send.at[way, s], l_recv.at[s], target)

    def pair_copies(s, h):
        target = {"fs": f + 1 - 2 * side}
        return (
            remote(v_rows(s, h), v_rows(s, h), vp_send.at[s], vp_recv.at[s], target),
            remote(l_rows(s, h), l_rows(s, h), lp_send.at[s], lp_recv.at[s], target),
        )

    class l_copy:
        def __init__(self, s, way, first):
            self.s = s
            self.both = (v_copy(s, way), lh_copy(s, way))

        def start(self):
            for copy in self.both:
                copy.start()

        def wait_recv(self):
            for copy, onward in zip(self.both, pair_copies(self.s, side)):
                copy.wait_recv()
                onward.start()

        def wait_send(self):
            for copy in self.both:
                copy.wait_send()

    def o_copy(s, way, first):
        target = {"sp": me + (1 if way == 0 else -1)}
        return remote(
            o_buf.at[s], o_buf.at[s], o_send.at[way, s], o_recv.at[s], target
        )

    def tok_rows(i):
        return x_buf.at[pl.ds(pl.multiple_of(i * own, own), own)]

    def tok_copy(d, peer, sender):
        return remote(
            tok_ref, tok_rows(sender), tok_send.at[d - 1], tok_recv.at[d - 1],
            {"fs": peer // tp, "tp": peer % tp},
        )

    def pick(ref, width, which):
        value = ref[:, :width]
        for i in range(1, ref.shape[1] // width):
            value = jnp.where(which == i, ref[:, i * width : (i + 1) * width], value)
        return value

    def lanes(ref, width):
        return ref.at[:, pl.ds(pl.multiple_of(f * width, width), width)]

    def depth(ref, width):
        return ref.at[pl.ds(pl.multiple_of(f * width, width), width)]

    cols = [VALUE_DIM, 2 * HEAD_DIM, KEY_DIM, KEY_DIM, HEAD_DIM, HEAD_DIM]
    starts = [sum(cols[:i]) for i in range(len(cols))]
    gd = go_ref.shape[0] // fs
    wd = wo_ref.shape[0] // fs
    heads = sink_ref.shape[1] // fs
    copies_in = [
        (lanes(gv_ref, cols[0]), w_rows(me).at[:, : cols[0]]),
        (lanes(wq_ref, cols[1]), w_rows(me).at[:, starts[1] : starts[2]]),
        (depth(go_ref, gd), o_buf.at[me, pl.ds(0, gd)]),
        (depth(wo_ref, wd), o_buf.at[me, pl.ds(gd, wd)]),
        (low_ref, l_buf.at[me]),
        (tok_ref, tok_rows(mine)),
    ]
    locals_ = [
        pltpu.make_async_copy(a, b, local_sem.at[i]) for i, (a, b) in enumerate(copies_in)
    ]
    for copy in locals_:
        copy.start()
    for d in range(1, plane):
        tok_copy(d, lax.rem(mine + d, plane), mine).start()
    own_rows = pl.ds(pl.multiple_of(me * kc, kc), kc)
    kv = (f * heads) // (SWA_HEADS // KV_HEADS)
    w_buf[own_rows, starts[2] : starts[4]] = jnp.concatenate(
        [pick(gq_ref, KEY_DIM, f), pick(gk_ref, KEY_DIM, f)], 1
    )
    w_buf[own_rows, starts[4] :] = jnp.concatenate(
        [pick(wk_ref, HEAD_DIM, kv), pick(wv_ref, HEAD_DIM, kv)], 1
    )
    for copy in locals_[:5]:
        copy.wait()

    def sends(k):
        @pl.when((me - k >= 0) & (me + 1 < sp))
        def _():
            l_copy(me - k, 0, k == 0).start()
            w_copy(me - k, 0, k == 0).start()

        @pl.when((me + k < sp) & (me >= 1))
        def _():
            l_copy(me + k, 1, k == 0).start()
            w_copy(me + k, 1, k == 0).start()

        @pl.when((me == k) & (me + 1 < sp))
        def _():
            o_copy(me, 0, True).start()

        @pl.when((sp - 1 - me == k) & (me >= 1))
        def _():
            o_copy(me, 1, True).start()

    for k in range(sp - 1):
        sends(k)

        @pl.when(me - 1 - k >= 0)
        def _():
            l_copy(me - 1 - k, 0, False).wait_recv()
            w_copy(me - 1 - k, 0, False).wait_recv()

        @pl.when(me + 1 + k < sp)
        def _():
            l_copy(me + 1 + k, 1, False).wait_recv()
            w_copy(me + 1 + k, 1, False).wait_recv()

    inner = (me >= 1) & (me + 1 < sp)
    for k in range(1, sp - 1):
        @pl.when(inner & (me - k >= 0))
        def _():
            o_copy(me - k, 0, False).wait_recv()
            o_copy(me - k, 0, False).start()

        @pl.when(inner & (me + k < sp))
        def _():
            o_copy(me + k, 1, False).wait_recv()
            o_copy(me + k, 1, False).start()

    for copy in locals_[5:]:
        copy.wait()
    for i in range(sp):
        @pl.when(i != me)
        def _():
            for copy in pair_copies(i, 1 - side):
                copy.wait_recv()

    for d in range(1, plane):
        tok_copy(d, mine, lax.rem(mine + plane - d, plane)).wait_recv()


    def project(b, _):
        x = x_buf[pl.ds(pl.multiple_of(b * rows, rows), rows)].astype(F32)
        normed = rms_rows(x, ngain_ref[...]).astype(BF)
        p = nn(normed, w_buf[...]).astype(BF)
        proj[b, :, : p.shape[1]] = p
        edge_out[b] = p[rows - WINDOW :, starts[4] : starts[4] + 2 * HEAD_DIM]
        low = nt(normed[:, :kc], l_buf[0])
        for s in range(1, sp):
            low += nt(normed[:, s * kc : (s + 1) * kc], l_buf[s])
        proj[b, :, p.shape[1] : p.shape[1] + low.shape[1]] = low.astype(BF)
        return 0

    lax.fori_loop(0, fs, project, 0)
    edge = remote(edge_out, edge_in, edge_sem.at[0], edge_sem.at[1], {"sp": me + 1})

    @pl.when(me + 1 < sp)
    def _():
        edge.start()

    @pl.when(me == 0)
    def _():
        edge_in[...] = jnp.zeros_like(edge_in)

    nb = rows // SPAN
    low_at = sum(cols)
    lower = (
        lax.broadcasted_iota(jnp.int32, (SPAN, SPAN), 0)
        >= lax.broadcasted_iota(jnp.int32, (SPAN, SPAN), 1)
    )
    tri = lower.astype(F32)
    up = pick(up_ref, KEY_DIM, f)
    bias = pick(bias_ref, KEY_DIM, f)
    sinks = pick(sink_ref, heads, f)
    for b in range(fs):
        low = proj[b, :, low_at : low_at + up_ref.shape[0]]
        z = nn(low, up) + bias
        rate = (jnp.minimum(z, 0.0) - jnp.log1p(jnp.exp(-jnp.abs(z)))) / SOFTMAX_TEMPER
        state = None
        before = jnp.zeros((1, KEY_DIM), F32)
        for n in range(nb):
            r0 = n * SPAN
            within = exact(tri, rate[r0 : r0 + SPAN])
            total = within[SPAN - 1 :]
            v = proj[b, r0 : r0 + SPAN, starts[0] : starts[0] + VALUE_DIM]
            q = proj[b, r0 : r0 + SPAN, starts[2] : starts[2] + KEY_DIM].astype(F32)
            k = proj[b, r0 : r0 + SPAN, starts[3] : starts[3] + KEY_DIM].astype(F32)
            q_dec = q * KEY_DIM**-0.5 * jnp.exp(within)
            k_dec = (k * jnp.exp(-within)).astype(BF)
            k_end = (k * jnp.exp(total - within)).astype(BF)
            scores = jnp.where(lower, nt(q_dec.astype(BF), k_dec), 0.0)
            o = nn(scores.astype(BF), v)
            if state is not None:
                o += nt(q_dec.astype(BF), state.astype(BF))
            local_out[b, r0 : r0 + SPAN] = o
            q_far[b, r0 : r0 + SPAN] = (q_dec * jnp.exp(before)).astype(BF)
            update = tn(v, k_end)
            state = update if state is None else jnp.exp(total) * state + update
            before = before + total
        half = (b % 2) * KEY_DIM
        state_out[b // 2, :VALUE_DIM, half : half + KEY_DIM] = state.astype(BF)
        state_out[b // 2, VALUE_DIM:, half : half + KEY_DIM] = jnp.broadcast_to(
            jnp.exp(before), (16, KEY_DIM)
        ).astype(BF)

    def state_copy(d, sender):
        return remote(
            state_out, state_in.at[sender], state_send.at[d - 1], state_recv.at[sender],
            {"sp": me + d},
        )

    for d in range(1, sp):
        @pl.when(me + d < sp)
        def _():
            state_copy(d, me).start()

    @pl.when(me >= 1)
    def _():
        edge.wait_recv()

    qi = lax.broadcasted_iota(jnp.int32, (WINDOW, 2 * WINDOW), 0)
    ki = lax.broadcasted_iota(jnp.int32, (WINDOW, 2 * WINDOW), 1)
    distance = qi + WINDOW - ki
    inside = (distance >= 0) & (distance < WINDOW)
    for b in range(fs):
        for w in range(rows // WINDOW):
            r0 = w * WINDOW
            here = proj[b, r0 : r0 + WINDOW, starts[4] : starts[4] + 2 * HEAD_DIM]
            if w == 0:
                past = edge_in[b]
                valid = inside & ((ki >= WINDOW) | (me >= 1))
            else:
                past = proj[b, r0 - WINDOW : r0, starts[4] : starts[4] + 2 * HEAD_DIM]
                valid = inside
            band = jnp.concatenate([past, here], 0)
            bk = band[:, :HEAD_DIM]
            bv = band[:, HEAD_DIM:]
            for h in range(heads):
                q0 = starts[1] + h * HEAD_DIM
                q = proj[b, r0 : r0 + WINDOW, q0 : q0 + HEAD_DIM]
                s = jnp.where(valid, nt(q, bk) * HEAD_DIM**-0.5, -1e30)
                sink = sinks[:, h : h + 1]
                top = jnp.maximum(jnp.max(s, -1, keepdims=True), sink)
                e = jnp.exp(s - top)
                den = jnp.sum(e, -1, keepdims=True) + jnp.exp(sink - top)
                a = nn((e / den).astype(BF), bv).astype(BF)
                h0 = VALUE_DIM + h * HEAD_DIM
                hidden[b, r0 : r0 + WINDOW, h0 : h0 + HEAD_DIM] = a

    for i in range(sp - 1):
        @pl.when(i < me)
        def _():
            state_copy(1, i).wait_recv()

        @pl.when(i >= me)
        def _():
            state_in[i] = jnp.zeros(state_in.shape[1:], BF)

    for b in range(fs):
        half = (b % 2) * KEY_DIM
        incoming = jnp.zeros((VALUE_DIM, KEY_DIM), F32)
        for i in range(sp - 1):
            got = state_in[i, b // 2, :VALUE_DIM, half : half + KEY_DIM].astype(F32)
            kept = state_in[i, b // 2, VALUE_DIM : VALUE_DIM + 1, half : half + KEY_DIM].astype(F32)
            incoming = jnp.where(i < me, kept * incoming + got, incoming)
        o = local_out[b] + nt(q_far[b], incoming.astype(BF))
        hidden[b, :, :VALUE_DIM] = rms_rows(o, hgain_ref[...]).astype(BF)

    forward = 2 * me < sp
    nc = o_buf.shape[2]

    def chunk(t):
        return lax.rem(jnp.where(forward, me + t, me - t) + sp, sp)

    def half_copy(s):
        return remote(half_out.at[s], half_in.at[s], half_send.at[s], half_recv.at[s], {"tp": 1 - c})

    def piece_copy(s, d, target):
        return remote(
            piece_out.at[s, d - 1], piece_in.at[s, d - 1],
            piece_send.at[s, d - 1], piece_recv.at[s, d - 1], {"fs": target},
        )

    def produce(t):
        s = chunk(t)

        @pl.when(jnp.logical_not(inner) & (t > 0))
        def _():
            o_copy(s, 0, False).wait_recv()

        w = o_buf[s]
        for b in range(fs):
            part = nn(hidden[b], w)
            lo, hi = part[:own], part[own:]
            half_out[s, b] = jnp.where(c == 0, hi, lo).astype(BF)
            half_own[s, b] = jnp.where(c == 0, lo, hi)
        half_copy(s).start()

    def combine(t):
        s = chunk(t)
        half_copy(s).wait_recv()
        for d in range(1, fs):
            to = lax.rem(f + d, fs)
            piece_out[s, d - 1] = (half_own[s, to] + half_in[s, to].astype(F32)).astype(BF)
            piece_copy(s, d, to).start()
        piece_own[s] = half_own[s, f] + half_in[s, f].astype(F32)

    def finish(t):
        s = chunk(t)
        total = piece_own[s]
        for d in range(1, fs):
            piece_copy(s, d, f).wait_recv()
            total += piece_in[s, d - 1].astype(F32)
        if len(out_ref.shape) == 2:
            out_ref[:, pl.ds(pl.multiple_of(s * nc, nc), nc)] = total.astype(BF)
        else:
            out_ref[s] = total.astype(BF)

    produce(0)

    def steady(t, _):
        produce(t)
        combine(t - 1)
        return 0

    lax.fori_loop(1, sp, steady, 0)
    combine(sp - 1)

    def close(t, _):
        finish(t)
        s = chunk(t)
        half_copy(s).wait_send()
        for d in range(1, fs):
            piece_copy(s, d, f).wait_send()
        return 0

    lax.fori_loop(0, sp, close, 0)

    for k in range(sp - 1):
        @pl.when((me - k >= 0) & (me + 1 < sp))
        def _():
            l_copy(me - k, 0, False).wait_send()
            w_copy(me - k, 0, False).wait_send()
            o_copy(me - k, 0, False).wait_send()

        @pl.when((me + k < sp) & (me >= 1))
        def _():
            l_copy(me + k, 1, False).wait_send()
            w_copy(me + k, 1, False).wait_send()
            o_copy(me + k, 1, False).wait_send()

    for i in range(sp):
        @pl.when(i != me)
        def _():
            for copy in pair_copies(i, side):
                copy.wait_send()

    for d in range(1, plane):
        tok_copy(d, mine, mine).wait_send()

    @pl.when(me + 1 < sp)
    def _():
        edge.wait_send()

    for d in range(1, sp):
        @pl.when(me + d < sp)
        def _():
            state_copy(d, me).wait_send()


def roll_half(a):
    return jnp.concatenate([a[:, a.shape[1] // 2 :], a[:, : a.shape[1] // 2]], 1)


def fold_kernel(
    sizes,
    tok_in,
    gv_ref,
    wq_ref,
    gq_ref,
    gk_ref,
    wk_ref,
    wv_ref,
    low_ref,
    go_ref,
    wo_ref,
    ngain_in,
    up_in,
    bias_in,
    hgain_in,
    sink_in,
    out_ref,
    tok_ref,
    ngain_ref,
    up_ref,
    bias_ref,
    hgain_ref,
    sink_ref,
    x_buf,
    ww,
    wg,
    wl,
    o_buf,
    tiles,
    qw,
    kvb,
    gvb,
    qkb,
    acc,
    acc2,
    og,
    hall,
    lowx,
    fill,
    sc,
    ew,
    decays,
    totals,
    states,
    state_out,
    state_in,
    local_out,
    q_far,
    hidden,
    half_out,
    half_in,
    half_own,
    piece_out,
    piece_in,
    piece_own,
    local_sem,
    l_send,
    l_recv,
    x_send,
    x_recv,
    x_share,
    w_send,
    w_recv,
    p_send,
    p_recv,
    o_send,
    o_recv,
    edge_sem,
    state_sem,
    hid_send,
    hid_recv,
    half_send,
    half_recv,
    piece_send,
    piece_recv,
    g_send,
    g_recv,
    g_rest,
    a_send,
    a_recv,
):
    sp, fs, tp = sizes
    me = lax.axis_index("sp")
    f = lax.axis_index("fs")
    c = lax.axis_index("tp")
    own = tok_in.shape[0]
    rows = own * tp
    kc = gv_ref.shape[0]
    part = kc // 2
    lpart = low_ref.shape[0] // 2
    MESH = pl.DeviceIdType.MESH
    pair = 2 * KEY_DIM
    wide = VALUE_DIM + pair

    slot = lax.rem(me, 2)
    far_slot = 1 - slot
    inner = (me >= 1) & (me + 1 < sp)
    outer = jnp.logical_not(inner)
    middle = 1 + slot
    outside = (sp - 1) * (me - 1)
    buddy = me + 1 - 2 * slot
    third = 2 - me // 2
    fourth = third + 1 - 2 * lax.rem(third, 2)
    chunks = [me, buddy, third, fourth]
    side = lax.rem(f, 2)
    xn = f + 1 - 2 * side
    yn = lax.rem(f + 2, fs)
    n1 = xn * (1 - c) + yn * c
    n2 = xn * c + yn * (1 - c)

    def remote(src, dst, ssem, rsem, target):
        return pltpu.make_async_remote_copy(
            src_ref=src, dst_ref=dst, send_sem=ssem, recv_sem=rsem,
            device_id=target, device_id_type=MESH,
        )

    barrier = pltpu.get_barrier_semaphore()

    def greet(target):
        pl.semaphore_signal(barrier, inc=1, device_id=target, device_id_type=MESH)

    greet({"tp": 1 - c})
    for d in range(1, fs):
        greet({"fs": lax.rem(f + d, fs)})

    @pl.when(me + 1 < sp)
    def _():
        greet({"sp": me + 1})

    @pl.when(me >= 1)
    def _():
        greet({"sp": me - 1})

    def lanes(ref, at, width):
        return ref.at[:, pl.ds(pl.multiple_of(at * width, width), width)]

    def depth(ref, width):
        return ref.at[pl.ds(pl.multiple_of(f * width, width), width)]

    def slice_rows(ref, s):
        return ref.at[pl.ds(pl.multiple_of(s * kc, kc), kc)]

    gd = go_ref.shape[0] // fs
    wd = wo_ref.shape[0] // fs
    heads = sink_in.shape[1] // fs
    wq_cols = heads * HEAD_DIM
    kv = (f * heads) // (SWA_HEADS // KV_HEADS)
    copies_in = [
        (lanes(gq_ref, f // 2, pair), tiles.at[0]),
        (lanes(gk_ref, f // 2, pair), tiles.at[1]),
        (wk_ref, tiles.at[2]),
        (wv_ref, tiles.at[3]),
        (lanes(wq_ref, f, wq_cols), slice_rows(ww, me).at[:, :wq_cols]),
        (lanes(gv_ref, f, VALUE_DIM), slice_rows(wg, me).at[:, :VALUE_DIM]),
        (low_ref, wl.at[me]),
    ]
    nc = o_buf.shape[3]
    for h in range(2):
        cut = pl.ds(h * nc, nc)
        copies_in += [
            (depth(go_ref, gd).at[:, cut], o_buf.at[me, h, pl.ds(0, gd)]),
            (depth(wo_ref, wd).at[:, cut], o_buf.at[me, h, pl.ds(gd, wd)]),
        ]
    copies_in += [
        (ngain_in, ngain_ref),
        (tok_in, tok_ref),
        (up_in, up_ref),
        (bias_in, bias_ref),
        (hgain_in, hgain_ref),
        (sink_in, sink_ref),
    ]
    shared = [0, 0, 0, 0, 1, 2, 3, 4, 4, 4, 4] + list(range(5, 11))
    locals_ = [
        pltpu.make_async_copy(a, b, local_sem.at[i]) for i, (a, b) in zip(shared, copies_in)
    ]

    def local_wait(ref, i):
        pltpu.make_async_copy(ref, ref, local_sem.at[i]).wait()

    for copy in locals_[11:] + locals_[:11]:
        copy.start()

    mine = f * tp + c
    b1, b2, b3 = xn * tp + c, yn * tp + c, (fs - 1 - f) * tp + c

    for copy in locals_[11:]:
        copy.wait()
    normed = rms_rows(tok_ref[...].astype(F32), ngain_ref[...]).astype(BF)
    x_buf[slot, pl.ds(pl.multiple_of(mine * own, own), own)] = normed

    def half_block(s, i, h):
        at = pl.multiple_of(i * own + h * (own // 2), own // 2)
        return x_buf.at[s, pl.ds(at, own // 2)]

    def x_copy(s, i, h, target, src):
        ref = half_block(s, i, h)
        return remote(ref, ref, x_send.at[s], x_recv.at[s, src, h], target)

    def x_sib(s, i, h):
        ref = half_block(s, i, h)
        return remote(ref, ref, x_send.at[s], x_share.at[s], SIB)

    def x_bulk(s, n):
        ref = x_buf.at[s, pl.ds(0, n * (own // 2))]
        return remote(ref, ref, x_send.at[s], x_share.at[s], SIB)

    SIB = {"tp": 1 - c}

    def ways(far, h):
        return (xn, yn) if far and h == 1 else (n1, n2)

    def x_first(s, h, far):
        w1, w2 = ways(far, h)
        return [
            x_copy(s, mine, h, {"fs": w1}, 1),
            x_copy(s, mine, h, {"fs": w2}, 2),
            x_sib(s, mine, h),
        ]

    def x_out(h):
        return x_copy(slot, mine, h, {"sp": middle}, 0)

    def kv_rows(s, h):
        at = pl.multiple_of(s * kc + h * part, part)
        return ww.at[pl.ds(at, part), wq_cols:]

    def low_rows(s, h):
        return wl.at[s, pl.ds(pl.multiple_of(h * lpart, lpart), lpart)]

    def w_copy(kind, s):
        ref = (
            lambda: slice_rows(ww, s).at[:, :wq_cols],
            lambda: kv_rows(s, side),
            lambda: low_rows(s, c),
            lambda: slice_rows(wg, s),
        )[kind]()
        return remote(ref, ref, w_send.at[kind], w_recv.at[kind, s], {"sp": middle})

    def w_bulk(kind, n):
        ref = (
            lambda: ww.at[pl.ds(0, n * kc), :wq_cols],
            lambda: ww.at[pl.ds(0, n * part), wq_cols:],
            lambda: wl.at[0, pl.ds(0, n * lpart)],
            lambda: wg.at[pl.ds(0, n * kc)],
        )[kind]()
        return remote(ref, ref, w_send.at[kind], w_recv.at[kind, 0], {"sp": middle})

    def kv_share(s, h):
        return remote(kv_rows(s, h), kv_rows(s, h), p_send.at[0], p_recv.at[s], {"fs": xn})

    def low_share(s, h):
        return remote(low_rows(s, h), low_rows(s, h), p_send.at[1], p_recv.at[sp], SIB)

    def share_bulk(i):
        ref = ww.at[pl.ds(0, 3 * part), wq_cols:] if i == 0 else wl.at[pl.ds(0, 3), pl.ds(0, lpart)]
        return remote(ref, ref, p_send.at[i], p_recv.at[sp], SIB)

    def o_copy(way, s, h, d):
        target = {"sp": middle if way == 0 else outside}
        ref = o_buf.at[s, h, pl.ds(d * gd, gd)]
        return remote(ref, ref, o_send.at[way], o_recv.at[s, h, d], target)

    def o_bulk(way, n):
        ref = o_buf.at[pl.ds(0, n)]
        return remote(ref, ref, o_send.at[way], o_recv.at[0, 0, 0], {"sp": middle})

    def o_part(way, s, h, d):
        o_copy(0, s, h, d).wait_recv()
        o_copy(way, s, h, d).start()

    def o_relay(way, s, h):
        for d in range(2):
            o_part(way, s, h, d)

    quarters = [(h, d) for h in range(2) for d in range(2)]

    def l_copy(i, k, target):
        return remote(lowx.at[i], lowx.at[i], l_send.at[0], l_recv.at[min(k // 3, 1)], target)

    def l_first():
        peers = [{"fs": n1}, {"fs": n2}, {"fs": fs - 1 - f}, SIB]
        return [l_copy(mine, k, peer) for k, peer in enumerate(peers)]

    def l_bulk(n, which):
        return remote(lowx.at[pl.ds(0, n)], lowx.at[pl.ds(0, n)], l_send.at[0], l_recv.at[which], SIB)

    def l_onward():
        return [l_copy(i, 4 + k, SIB) for k, i in enumerate((b1, b2, b3))]

    def start(copies):
        for copy in copies:
            copy.start()

    pl.semaphore_wait(barrier, fs + jnp.where(inner, 2, 1))

    LOW, KV, QUERY, STATE = 2, 1, 0, 3
    locals_[6].wait()
    w_copy(LOW, me).start()

    @pl.when(outer)
    def _():
        for h in range(2):
            x_out(h).start()

    @pl.when(inner)
    def _():
        for h in range(2):
            start(x_first(slot, h, False))

    local_wait(tiles, 0)
    for copy in locals_[4:6]:
        copy.wait()
    own_rows = pl.ds(pl.multiple_of(me * kc, kc), kc)

    def half_of(i, width, which):
        return jnp.where(which == 0, tiles[i, :, :width], tiles[i, :, width:])

    ww[own_rows, wq_cols:] = jnp.concatenate(
        [half_of(2, HEAD_DIM, kv), half_of(3, HEAD_DIM, kv)], 1
    )
    w_copy(KV, me).start()
    w_copy(QUERY, me).start()
    wg[own_rows, VALUE_DIM:] = jnp.concatenate(
        [half_of(0, KEY_DIM, side), half_of(1, KEY_DIM, side)], 1
    )
    local_wait(o_buf.at[me], 4)

    @pl.when(outer)
    def _():
        w_copy(STATE, me).start()
        for h, d in quarters:
            o_copy(0, me, h, d).start()

    lane = lax.broadcasted_iota(jnp.int32, (rows, pair), 1)
    row = lax.broadcasted_iota(jnp.int32, (rows, pair), 0)
    left = lane < KEY_DIM
    early = row < SPAN
    same = (row < SPAN) == (lane < SPAN)
    diagonal = same & (row >= lane)
    below = (row >= SPAN) & (lane < SPAN)

    def edge_rows(i, h):
        n = fs * rows // 2
        return kvb.at[i, pl.ds(pl.multiple_of(h * n, n), n)]

    edge = remote(
        edge_rows(2, side), edge_rows(0, side), edge_sem.at[0], edge_sem.at[1], {"sp": me + 1}
    )

    def edge_share(h):
        return remote(
            edge_rows(0, h), edge_rows(0, h), edge_sem.at[2], edge_sem.at[3], {"fs": xn}
        )
    state = remote(state_out, state_in, state_sem.at[0], state_sem.at[1], {"sp": me + 1})

    def hid_part(s, i):
        return hidden.at[s, :, i * VALUE_DIM : (i + 1) * VALUE_DIM]

    def hid_copy(i, s):
        return remote(
            hid_part(s, i), hid_part(s, i), hid_send.at[i], hid_recv.at[i], {"sp": outside}
        )

    def seq(b):
        if isinstance(b, int):
            return pl.ds(b * rows, rows)
        return pl.ds(pl.multiple_of(b * rows, rows), rows)

    @pl.when(inner)
    def _():
        for h, d in quarters:
            o_copy(1, me, h, d).start()

        def arrive(kind, s, onward):
            w_copy(kind, s).wait_recv()
            if onward:
                w_copy(kind, s).start()
            if kind == LOW:
                low_share(s, c).start()
            if kind == KV:
                kv_share(s, side).start()

        def neighbours(s, h, far):
            w1, w2 = ways(far, h)
            i1, i2 = w1 * tp + c, w2 * tp + c
            x_copy(s, i1, h, SIB, 1).wait_recv()
            x_copy(s, i1, h, {"fs": w2}, 3).start()
            x_sib(s, i1, h).start()
            x_copy(s, i2, h, SIB, 2).wait_recv()
            x_sib(s, i2, h).start()

        def corner(s):
            for h in range(2):
                x_copy(s, b3, h, SIB, 3).wait_recv()
                x_sib(s, b3, h).start()

        def siblings(s):
            x_bulk(s, 2 * fs).wait_recv()

        def columns(s):
            return pl.ds(pl.multiple_of(s * kc, kc), kc)

        bs = [bias_ref[:, i * KEY_DIM : (i + 1) * KEY_DIM] for i in range(fs)]
        ups = [up_ref[:, i * KEY_DIM : (i + 1) * KEY_DIM] for i in range(fs)]
        bias, up = bs[0], ups[0]
        for i in range(1, fs):
            bias = jnp.where(f == i, bs[i], bias)
            up = jnp.where(f == i, ups[i], up)
        up_l = jnp.concatenate([up, jnp.zeros_like(up)], 1)
        up_r = jnp.concatenate([jnp.zeros_like(up), up], 1)
        bias2 = jnp.concatenate([bias, bias], 1)

        def own_low():
            at = pl.ds(pl.multiple_of(mine * own, own), own)
            x = jnp.concatenate([x_buf[slot, at], x_buf[far_slot, at]], 0)
            low = nt(wl[0], x[:, :kc])
            for j in range(1, sp):
                low += nt(wl[j], x[:, j * kc : (j + 1) * kc])
            lowx[mine] = low.astype(BF)

        def gate(p):
            pre = []
            for i in range(tp):
                z = tn(lowx[2 * p * tp + i], up_l) + tn(lowx[(2 * p + 1) * tp + i], up_r)
                pre.append(z + bias2)
            return [
                jnp.concatenate([z[k * own : (k + 1) * own] for z in pre], 0) for k in range(2)
            ]

        def decay():
            tri = diagonal.astype(F32)
            for p in range(fs // 2):
                for s, z in zip((slot, far_slot), gate(p)):
                    decay_of(s, p, z, tri)

        def decay_of(s, p, z, tri):
            rate = (jnp.minimum(z, 0.0) - jnp.log1p(jnp.exp(-jnp.abs(z)))) / SOFTMAX_TEMPER
            within = exact(tri, rate)
            t0, t1 = within[SPAN - 1 : SPAN], within[rows - 1 :]
            grow = jnp.exp(within) * KEY_DIM**-0.5
            end = jnp.exp(jnp.where(early, t0, t1) - within)
            decays[s, p, 0] = grow
            decays[s, p, 1] = jnp.exp(-within)
            decays[s, p, 2] = end
            decays[s, p, 3] = grow * jnp.where(early, 1.0, jnp.exp(t0))
            decays[s, p, 4] = end * jnp.where(early, jnp.exp(t1), 1.0)
            totals[s, p] = jnp.broadcast_to(jnp.exp(t0 + t1), totals.shape[2:])

        def window_maps(s, slices):
            total = nn(x_buf[s, :, columns(slices[0])], slice_rows(ww, slices[0])[...])
            for j in slices[1:]:
                total += nn(x_buf[s, :, columns(j)], slice_rows(ww, j)[...])
            return total

        def state_maps(s, slices):
            total = nn(x_buf[s, :, columns(slices[0])], slice_rows(wg, slices[0])[...])
            for j in slices[1:]:
                total += nn(x_buf[s, :, columns(j)], slice_rows(wg, j)[...])
            return total

        def place(s, p):
            q = p[:, :wq_cols].astype(BF).astype(F32) * HEAD_DIM**-0.5
            for h in range(heads):
                qh = jnp.where(left_all, q if h == 0 else roll_half(q), 0.0)
                qw[s, h] = qh.astype(BF)
            kvb[s + 1] = p[:, wq_cols:].astype(BF)

        left_all = lax.broadcasted_iota(jnp.int32, (fs * rows, pair), 1) < KEY_DIM
        tall = heads * WINDOW
        qi = lax.broadcasted_iota(jnp.int32, (tall, 2 * WINDOW), 0)
        ki = lax.broadcasted_iota(jnp.int32, (tall, 2 * WINDOW), 1)
        distance = lax.rem(qi, WINDOW) + WINDOW - ki
        inside = (distance >= 0) & (distance < WINDOW)
        sinks = sink_ref[:, :heads]
        for i in range(1, fs):
            sinks = jnp.where(f == i, sink_ref[:, i * heads : (i + 1) * heads], sinks)
        sink = sinks[:, :1]
        for h in range(1, heads):
            sink = jnp.where(qi < h * WINDOW, sink, sinks[:, h : h + 1])
        fill[...] = jnp.where(ki == 0, sink, -1e30)
        key_row = lax.broadcasted_iota(jnp.int32, (2 * WINDOW, pair), 0)
        key_lane = lax.broadcasted_iota(jnp.int32, (2 * WINDOW, pair), 1)

        @pl.when(me == 1)
        def _():
            kvb[0] = jnp.zeros(kvb.shape[1:], BF)
            state_in[...] = jnp.zeros_like(state_in)

        def far_rows(h):
            x_copy(far_slot, mine, h, SIB, 0).wait_recv()
            start(x_first(far_slot, h, True))

        arrive(LOW, buddy, True)
        w_copy(STATE, me).start()
        o_copy(0, me, 0, 0).start()
        arrive(LOW, third, False)
        arrive(KV, third, False)
        neighbours(slot, 0, False)
        far_rows(0)
        arrive(LOW, fourth, False)
        neighbours(slot, 1, False)
        far_rows(1)
        share_bulk(1).wait_recv()
        own_low()
        start(l_first())
        arrive(KV, buddy, True)
        neighbours(far_slot, 0, True)
        arrive(QUERY, buddy, True)
        o_copy(0, me, 0, 1).start()
        corner(slot)
        siblings(slot)
        arrive(QUERY, third, False)
        kv_share(third, 1 - side).wait_recv()
        acc[slot] = window_maps(slot, (me, third))
        neighbours(far_slot, 1, True)
        arrive(STATE, buddy, True)
        arrive(KV, fourth, False)
        l_bulk(3, 0).wait_recv()
        start(l_onward())
        l_bulk(4, 1).wait_recv()
        decay()
        w_copy(STATE, third).wait_recv()
        acc2[slot] = state_maps(slot, chunks[:3])
        o_relay(1, third, 0)
        corner(far_slot)
        arrive(QUERY, fourth, False)
        kv_share(buddy, 1 - side).wait_recv()
        kv_share(fourth, 1 - side).wait_recv()

        place(slot, acc[slot] + window_maps(slot, (buddy, fourth)))

        @pl.when(me == 1)
        def _():
            edge.start()

        for d in range(2):
            o_copy(0, me, 1, d).start()

        siblings(far_slot)
        place(far_slot, window_maps(far_slot, chunks))

        def window(s):
            valid = inside & ((ki >= WINDOW) | (me > 1) | (s > 0))
            bands = [jnp.concatenate([kvb[s, seq(b)], kvb[s + 1, seq(b)]], 0) for b in range(fs)]
            for b in range(fs):
                q = jnp.concatenate([qw[s, h, seq(b)] for h in range(heads)], 0)
                sc[b] = jnp.where(valid, nt(q, bands[b]), fill[...])
            for b in range(fs):
                near = sc[b]
                top = jnp.max(near, -1, keepdims=True)
                ew[b] = jnp.exp(near - top).astype(BF)
            for b in range(fs):
                band = jnp.concatenate([kvb[s, seq(b)], kvb[s + 1, seq(b)]], 0).astype(F32)
                values = jnp.where(
                    key_lane < HEAD_DIM, 1.0, jnp.where(key_row == 0, 0.0, band)
                ).astype(BF)
                both = nn(ew[b], values)
                turned = roll_half(both)
                first = turned[:WINDOW] / both[:WINDOW]
                second = both[WINDOW:] / turned[WINDOW:]
                hidden[s, seq(b), VALUE_DIM:] = jnp.where(left, first, second).astype(BF)

        window(far_slot)
        hid_copy(1, far_slot).start()

        @pl.when(me > 1)
        def _():
            for h in range(2):
                o_relay(0, buddy, h)

        acc2[far_slot] = state_maps(far_slot, chunks[:3])

        @pl.when(me > 1)
        def _():
            edge.wait_recv()
            edge_share(side).start()

        w_copy(STATE, fourth).wait_recv()

        for s in range(2):
            p = (acc2[s] + state_maps(s, chunks[3:])).astype(BF)
            gvb[s] = p[:, :VALUE_DIM]
            qkb[s] = p[:, VALUE_DIM:].astype(F32)

        def keys(s, p):
            return jnp.where(left, roll_half(qkb[s, seq(2 * p)]), qkb[s, seq(2 * p + 1)])

        def queries(s, p):
            return jnp.where(left, qkb[s, seq(2 * p)], roll_half(qkb[s, seq(2 * p + 1)]))

        for s in range(2):
            for p in range(fs // 2):
                k_far = (keys(s, p) * decays[s, p, 4]).astype(BF)
                states[s, p] = jnp.where(
                    left, tn(gvb[s, seq(2 * p)], k_far), tn(gvb[s, seq(2 * p + 1)], k_far)
                )
        for p in range(fs // 2):
            state_out[p] = (totals[1, p, :1] * states[0, p] + states[1, p]).astype(BF)

        @pl.when(me == 1)
        def _():
            state.start()
            o_relay(0, buddy, 0)

        for s in range(2):
            for p in range(fs // 2):
                k = keys(s, p)
                q = queries(s, p)
                qd = q * decays[s, p, 0]
                qf = q * decays[s, p, 3]
                kd = (k * decays[s, p, 1]).astype(BF)
                ke = (k * decays[s, p, 2]).astype(BF)
                for j in range(2):
                    here = left if j == 0 else jnp.logical_not(left)
                    qj = jnp.where(here, qd, 0.0).astype(BF)
                    scores = jnp.where(
                        diagonal, nt(qj, kd), jnp.where(below, nt(qj, ke), 0.0)
                    ).astype(BF)
                    local_out[s, seq(2 * p + j)] = nn(scores, gvb[s, seq(2 * p + j)])
                    q_far[s, seq(2 * p + j)] = jnp.where(here, qf, 0.0).astype(BF)
            if s == 0:
                @pl.when(me == 1)
                def _():
                    o_relay(1, third, 1)

        @pl.when(me == 1)
        def _():
            o_relay(0, buddy, 1)

        @pl.when(me > 1)
        def _():
            o_relay(1, third, 1)
            edge_share(1 - side).wait_recv()
            window(slot)
            state.wait_recv()

        def finish_state(s):
            for p in range(fs // 2):
                arrived = state_in[p].astype(F32)
                entering = jnp.where(s == 0, arrived, totals[0, p, :1] * arrived + states[0, p])
                entering = entering.astype(BF)
                for j in range(2):
                    b = 2 * p + j
                    o = local_out[s, seq(b)] + nt(q_far[s, seq(b)], entering)
                    hidden[s, seq(b), :VALUE_DIM] = rms_rows(o, hgain_ref[...]).astype(BF)

        finish_state(far_slot)
        hid_copy(0, far_slot).start()
        finish_state(slot)

        @pl.when(me == 1)
        def _():
            window(slot)

    def g_copy(k, j, g, h, target):
        ref = og.at[j, g, h]
        into = g_recv.at[j, h] if k == 0 else g_rest.at[0]
        return remote(ref, ref, g_send.at[0], into, target)

    def g_bulk(n, ssem):
        ref = og.at[:, pl.ds(0, n)]
        return remote(ref, ref, ssem.at[0], g_rest.at[0], SIB)

    corner_f = fs - 1 - f

    def g_first(j, h):
        return [g_copy(0, j, f, h, {"fs": n1}), g_copy(1, j, f, h, {"fs": n2})]

    def g_relay(j, h):
        return g_copy(2, j, n1, h, {"fs": n2})

    def a_part(g, i):
        return hidden.at[slot, seq(g), i * VALUE_DIM : (i + 1) * VALUE_DIM]

    def a_copy(k, i):
        g = (n1, n2, corner_f)[k]
        here = hall.at[f, :, i * VALUE_DIM : (i + 1) * VALUE_DIM]
        return remote(a_part(g, i), here, a_send.at[0], a_recv.at[0], {"fs": g})

    def a_bulk():
        ref = hall.at[pl.ds(0, fs - 1)]
        return remote(ref, ref, a_send.at[0], a_recv.at[0], {"fs": n1})

    @pl.when(outer)
    def _():
        for h in range(2):
            og[0, f, h] = o_buf[me, h]
            start(g_first(0, h))
        for h in range(2):
            for d in range(2):
                o_copy(0, buddy, h, d).wait_recv()
            og[1, f, h] = o_buf[buddy, h]
        for j in range(2):
            for h in range(2):
                g_copy(0, j, n1, h, SIB).wait_recv()
                g_relay(j, h).start()
                if j == 0:
                    start(g_first(1, h))
        g_bulk(2, g_send).wait_recv()
        for i in (1, 0):
            hid_copy(i, slot).wait_recv()
            for k in range(3):
                a_copy(k, i).start()
        hall[f] = hidden[slot, seq(f)]

    parts = [(s, h) for s in chunks for h in range(2)]

    def half_copy(s, h):
        return remote(
            half_out.at[s, h], half_in.at[s, h], half_send.at[0], half_recv.at[s, h], SIB
        )

    peers = (corner_f, n1, n2)

    def piece_copy(s, h, d):
        target = peers[d - 1]
        return remote(
            piece_out.at[s, h, d - 1], piece_in.at[s, h, d - 1],
            piece_send.at[0], piece_recv.at[s, h], {"fs": target},
        )

    def produce(t):
        s, h = parts[t]
        if 4 <= t < 6:
            @pl.when(outer)
            def _():
                for d in range(2):
                    o_copy(0, s, h, d).wait_recv()
        if t >= 6:
            @pl.when(outer)
            def _():
                for d in range(2):
                    o_copy(0, s, h, d).wait_recv()

        w = o_buf[s, h]
        for b in range(fs):
            partial = nn(hidden[slot, seq(b)], w)
            lo, hi = partial[:own], partial[own:]
            half_out[s, h, b] = jnp.where(c == 0, hi, lo).astype(BF)
            half_own[s, h, b] = jnp.where(c == 0, lo, hi)
        half_copy(s, h).start()

    def combine(t):
        s, h = parts[t]
        half_copy(s, h).wait_recv()
        for d in range(1, fs):
            to = peers[d - 1]
            piece_out[s, h, d - 1] = (half_own[s, h, to] + half_in[s, h, to].astype(F32)).astype(BF)
            piece_copy(s, h, d).start()
        piece_own[s, h] = half_own[s, h, f] + half_in[s, h, f].astype(F32)

    def store(t, total):
        s, h = parts[t]
        at = pl.ds(pl.multiple_of((2 * s + h) * nc, nc), nc)
        out_ref[:, at] = total.astype(BF)

    def finish(t):
        s, h = parts[t]
        total = piece_own[s, h]
        remote(
            piece_out.at[s, h], piece_in.at[s, h], piece_send.at[0], piece_recv.at[s, h], SIB
        ).wait_recv()
        for d in range(1, fs):
            total += piece_in[s, h, d - 1].astype(F32)
        store(t, total)

    def whole_copy(s, h):
        return remote(
            half_out.at[s, h, 0], half_in.at[s, h, 0], half_send.at[1], half_recv.at[s, h], SIB
        )

    def produce_whole(t):
        s, h = parts[t]
        total = nn(hall[0], og[t // 2, 0, h])
        for g in range(1, fs):
            total += nn(hall[g], og[t // 2, g, h])
        lo, hi = total[:own], total[own:]
        half_out[s, h, 0] = jnp.where(c == 0, hi, lo).astype(BF)
        half_own[s, h, 0] = jnp.where(c == 0, lo, hi)
        whole_copy(s, h).start()

    def finish_whole(t):
        s, h = parts[t]
        whole_copy(s, h).wait_recv()
        store(t, half_own[s, h, 0] + half_in[s, h, 0].astype(F32))

    def tail_sent(n):
        ref = half_out.at[pl.ds(0, n)]
        remote(ref, ref, half_send.at[0], half_recv.at[0, 0], SIB).wait_send()
        ref = piece_out.at[pl.ds(0, n)]
        remote(ref, ref, piece_send.at[0], piece_recv.at[0, 0], SIB).wait_send()

    @pl.when(inner)
    def _():
        produce(0)
        for t in range(1, 2 * sp):
            produce(t)
            combine(t - 1)
            for h, d in {2: quarters[:2], 4: quarters[2:3], 5: quarters[3:]}.get(t, ()):
                o_part(1, fourth, h, d)
        combine(2 * sp - 1)
        for t in range(2 * sp):
            finish(t)
        tail_sent(sp)

    @pl.when(outer)
    def _():
        produce(4)
        produce(5)
        combine(4)
        combine(5)
        produce(6)
        a_bulk().wait_recv()
        for t in range(4):
            produce_whole(t)
        combine(6)
        produce(7)
        combine(7)
        for t in range(4):
            finish_whole(t)
        for t in range(4, 2 * sp):
            finish(t)
        tail_sent(sp // 2)
        ref = half_out.at[0, 0]
        remote(ref, ref, half_send.at[1], half_recv.at[0, 0], SIB).wait_send()
        g_bulk(3, g_send).wait_send()
        a_bulk().wait_send()

    @pl.when(outer)
    def _():
        x_bulk(slot, 2).wait_send()
        for kind in range(4):
            w_bulk(kind, 1).wait_send()
        o_bulk(0, 1).wait_send()

    @pl.when(inner)
    def _():
        for s in range(2):
            x_bulk(s, 14).wait_send()
        l_bulk(7, 0).wait_send()
        for kind in range(4):
            w_bulk(kind, 2).wait_send()
        share_bulk(0).wait_send()
        share_bulk(1).wait_send()
        o_bulk(0, 2).wait_send()
        o_bulk(1, 3).wait_send()
        for i in range(2):
            hid_copy(i, far_slot).wait_send()

        @pl.when(me == 1)
        def _():
            edge.wait_send()
            state.wait_send()

        @pl.when(me > 1)
        def _():
            edge_share(side).wait_send()


def fold_call(sizes, operands):
    sp, fs, tp = sizes
    own, d = operands[0].shape
    rows = own * tp
    kc = operands[1].shape[0]
    rank = operands[7].shape[0]
    depth = (operands[8].shape[0] + operands[9].shape[0]) // fs
    nc = operands[8].shape[1]
    pair = 2 * KEY_DIM
    all_rows = fs * rows
    pairs = fs // 2
    vm = pltpu.VMEM
    dma = pltpu.SemaphoreType.DMA
    small = [(o.shape, o.dtype) for o in operands[10:]]
    scratch = [
        vm((own, d), BF),
        *(vm(shape, dtype) for shape, dtype in small),
        vm((2, all_rows, d), BF),
        vm((d, 2 * pair), BF),
        vm((d, VALUE_DIM + pair), BF),
        vm((sp, rank, kc), BF),
        vm((sp, 2, depth, nc // 2), BF),
        vm((4, kc, pair), BF),
        vm((2, 2, all_rows, pair), BF),
        vm((3, all_rows, pair), BF),
        vm((2, all_rows, VALUE_DIM), BF),
        vm((2, all_rows, pair), F32),
        vm((2, all_rows, 2 * pair), F32),
        vm((2, all_rows, VALUE_DIM + pair), F32),
        vm((2, fs, 2, depth, nc // 2), BF),
        vm((fs, rows, depth), BF),
        vm((fs * tp, rank, 2 * own), BF),
        vm((2 * WINDOW, 2 * WINDOW), F32),
        vm((fs, 2 * WINDOW, 2 * WINDOW), F32),
        vm((fs, 2 * WINDOW, 2 * WINDOW), BF),
        vm((2, pairs, 5, rows, pair), F32),
        vm((2, pairs, 8, pair), F32),
        vm((2, pairs, VALUE_DIM, pair), F32),
        vm((pairs, VALUE_DIM, pair), BF),
        vm((pairs, VALUE_DIM, pair), BF),
        vm((2, all_rows, VALUE_DIM), F32),
        vm((2, all_rows, pair), BF),
        vm((2, all_rows, depth), BF),
        vm((sp, 2, fs, own, nc // 2), BF),
        vm((sp, 2, fs, own, nc // 2), BF),
        vm((sp, 2, fs, own, nc // 2), F32),
        vm((sp, 2, fs - 1, own, nc // 2), BF),
        vm((sp, 2, fs - 1, own, nc // 2), BF),
        vm((sp, 2, own, nc // 2), F32),
        dma((11,)),
        dma((1,)),
        dma((2,)),
        dma((2,)),
        dma((2, 4, 2)),
        dma((2,)),
        dma((4,)),
        dma((4, sp)),
        dma((2,)),
        dma((sp + 1,)),
        dma((2,)),
        dma((sp, 2, 2)),
        dma((4,)),
        dma((2,)),
        dma((2,)),
        dma((2,)),
        dma((2,)),
        dma((sp, 2)),
        dma((1,)),
        dma((sp, 2)),
        dma((1,)),
        dma((2, 2)),
        dma((1,)),
        dma((1,)),
        dma((1,)),
    ]
    anywhere = pl.BlockSpec(memory_space=pl.ANY)
    return pl.pallas_call(
        functools.partial(fold_kernel, sizes),
        out_shape=pltpu.VMEM((own, sp * nc), BF),
        in_specs=[anywhere] * 15,
        out_specs=pl.BlockSpec(memory_space=pltpu.VMEM),
        scratch_shapes=scratch,
        compiler_params=pltpu.CompilerParams(
            has_side_effects=True, vmem_limit_bytes=60 * 1024 * 1024, collective_id=0
        ),
    )(*operands)


def folds(sp, fs, tp, shape, rows, kc, width, rank, nc, depth):
    whole_rows = rows == WINDOW == 2 * SPAN
    lanes_fit = nc % 256 == 0 and kc % 128 == 0 and depth == 2 * VALUE_DIM and 2 * HEAD_DIM == 2 * KEY_DIM
    return sp == 4 and fs == 4 and tp == 2 and whole_rows and lanes_fit and rank % 32 == 0


def per_device(
    tokens,
    norm_gain,
    gla_query_weight,
    gla_key_weight,
    gla_value_weight,
    decay_down,
    decay_up,
    decay_bias,
    head_gain,
    window_query_weight,
    window_key_weight,
    window_value_weight,
    sink_logit,
    gla_output_weight,
    window_output_weight,
):
    fs, tp, sp = (lax.axis_size(n) for n in ("fs", "tp", "sp"))
    low = decay_down.T
    own = tokens.shape[1]
    rows = own * tp
    kc = decay_down.shape[0]
    width = VALUE_DIM + 4 * HEAD_DIM + 2 * KEY_DIM
    rank = low.shape[0]
    depth = (gla_output_weight.shape[0] + window_output_weight.shape[0]) // fs
    nc = gla_output_weight.shape[1]
    flat = nc % 128 == 0
    operands = (
        tokens[0],
        gla_value_weight,
        window_query_weight,
        gla_query_weight,
        gla_key_weight,
        window_key_weight,
        window_value_weight,
        low,
        gla_output_weight,
        window_output_weight,
        norm_gain[None],
        decay_up,
        decay_bias[None],
        head_gain[None],
        sink_logit[None],
    )
    if folds(sp, fs, tp, tokens.shape, rows, kc, width, rank, nc, depth):
        return fold_call((sp, fs, tp), operands).reshape(1, own, sp * nc)
    vm = pltpu.VMEM
    dma = pltpu.SemaphoreType.DMA
    scratch = [
        vm((fs * rows, tokens.shape[2]), BF),
        vm((sp * kc, width), BF),
        vm((sp, rank, kc), BF),
        vm((sp, depth, nc), BF),
        vm((fs, rows, width + 128), BF),
        vm((fs, WINDOW, 2 * HEAD_DIM), BF),
        vm((fs, WINDOW, 2 * HEAD_DIM), BF),
        vm((fs // 2, VALUE_DIM + 16, 2 * KEY_DIM), BF),
        vm((sp, fs // 2, VALUE_DIM + 16, 2 * KEY_DIM), BF),
        vm((fs, rows, VALUE_DIM), F32),
        vm((fs, rows, KEY_DIM), BF),
        vm((fs, rows, depth), BF),
        vm((sp, fs, own, nc), BF),
        vm((sp, fs, own, nc), BF),
        vm((sp, fs, own, nc), F32),
        vm((sp, fs - 1, own, nc), BF),
        vm((sp, fs - 1, own, nc), BF),
        vm((sp, own, nc), F32),
        dma((6,)),
        dma((fs * tp - 1,)),
        dma((fs * tp - 1,)),
        dma((2, sp)),
        dma((sp,)),
        dma((2, sp)),
        dma((sp,)),
        dma((2, sp)),
        dma((sp,)),
        dma((sp,)),
        dma((sp,)),
        dma((sp,)),
        dma((sp,)),
        dma((2, sp)),
        dma((sp,)),
        dma((2,)),
        dma((sp,)),
        dma((sp,)),
        dma((sp,)),
        dma((sp,)),
        dma((sp, fs - 1)),
        dma((sp, fs - 1)),
    ]
    spec = pl.BlockSpec(memory_space=pltpu.VMEM)
    anywhere = pl.BlockSpec(memory_space=pl.ANY)
    mixed = pl.pallas_call(
        functools.partial(mixer_kernel, (sp, fs, tp)),
        out_shape=jax.ShapeDtypeStruct((own, sp * nc) if flat else (sp, own, nc), BF),
        in_specs=[
            anywhere if i in (1, 2, 8, 9) else spec for i in range(15)
        ],
        out_specs=spec,
        scratch_shapes=scratch,
        compiler_params=pltpu.CompilerParams(
            has_side_effects=True, vmem_limit_bytes=60 * 1024 * 1024
        ),
    )(*operands)
    return (mixed if flat else mixed.transpose(1, 0, 2)).reshape(1, own, sp * nc)


def solution(mesh):
    in_specs = (
        P("fs", ("sp", "tp"), None),
        P(),
        P("sp", "tp"),
        P("sp", "tp"),
        P("sp", "tp"),
        P("sp", None),
        P(None, "tp"),
        P("tp"),
        P(),
        P("sp", "tp"),
        P("sp", "tp"),
        P("sp", "tp"),
        P("tp"),
        P("tp", "sp"),
        P("tp", "sp"),
    )
    out_specs = P("fs", ("sp", "tp"), None)
    return jax.shard_map(
        per_device, mesh=mesh, in_specs=in_specs, out_specs=out_specs, check_vma=False
    )
```
